32 devices in a mesh: sp: 8 (over z, x), tp: 4 (over y, core).
Axes of the slice: x: 2, y: 2, z: 4, core: 2. Of those that a mesh axis runs over, the one named last changes fastest.
Arguments:
- layer_input: bfloat16 [1280, 4096], P('sp', 'tp'), may hold values from -24 to 24
- output_grad: bfloat16 [1280, 4096], P('sp', 'tp'), may hold values from -24 to 24
- query_weight: bfloat16 [4096, 2048], P(None, 'tp'), may hold values from -0.09375 to 0.09375
- key_weight: bfloat16 [4096, 1024], P(None, 'tp'), may hold values from -0.09375 to 0.09375
- value_weight: bfloat16 [4096, 1024], P(None, 'tp'), may hold values from -0.09375 to 0.09375
- out_weight: bfloat16 [2048, 4096], P('tp'), may hold values from -0.125 to 0.125
- sink_logit: float32 [16], P('tp'), may hold values from 3 to 7
Outputs:
- input_grad: bfloat16 [1280, 4096], P('sp', 'tp')
- query_weight_grad: float32 [4096, 2048], P('sp', 'tp')
- key_weight_grad: float32 [4096, 1024], P('sp', 'tp')
- value_weight_grad: float32 [4096, 1024], P('sp', 'tp')
- out_weight_grad: float32 [2048, 4096], P('tp', 'sp')
- sink_grad: float32 [16], P('tp')
The draws below stay inside these ranges and needn't reach their ends.
All inputs are finite; a program needn't handle non-finite values.
Results may differ from the reference program's by a relative error of at most 0.015.
Values may be sent and summed in bfloat16 or wider, within the bound.
A program may use at most 192 MiB of HBM per device.

```python
import jax
import jax.numpy as jnp
from jax import lax

D = 4096
HEADS = 16
KV_HEADS = 8
HEAD = 128
WINDOW = 128
TOK_DEV = 160
TOKENS = 1280


def draw_layer_input(key, part):
    key_normal = jax.random.fold_in(key, 11)
    key_pairing = jax.random.fold_in(key, 12)
    normal_part = jnp.clip(jax.random.normal(key_normal, (TOKENS, D), jnp.float32), -4.0, 4.0)
    blocks = TOKENS // TOK_DEV
    pairing = jax.random.permutation(key_pairing, blocks)
    row_block = jnp.arange(TOKENS, dtype=jnp.int32) // TOK_DEV
    col_block = jnp.arange(D, dtype=jnp.int32) * blocks // D
    spiked = pairing[row_block][:, None] == col_block[None, :]
    values = normal_part * jnp.where(spiked, 3.0, 1.0)
    return values.astype(jnp.bfloat16)


def strengthened(entries, own_key, source, target, parts, factor):
    owner, partner = [(jnp.arange(entries.shape[axis_at]) // (entries.shape[axis_at] // parts)).reshape([-1 if axis == axis_at else 1 for axis in range(entries.ndim)]) for axis_at in (source, target)]
    chosen = jax.random.permutation(own_key, parts)[partner]
    strong = (owner == chosen) | (owner == (partner + parts // 2) % parts)
    return jnp.where(strong, factor * entries, entries)


def block_levels(stream_key, shape, cuts, smallest, largest):
    def one(dim, shards_of):
        draws = jax.random.uniform(jax.random.fold_in(jax.random.fold_in(stream_key, 6), dim), (shards_of,), jnp.float32, smallest / len(cuts), largest / len(cuts))
        return jnp.repeat(jnp.exp(draws), shape[dim] // shards_of).reshape((-1,) + (1,) * (len(shape) - dim - 1))

    level = one(*cuts[0])
    for cut in cuts[1:]:
        level = level * one(*cut)
    return level


def scatter_about(key, shape, deviation, limit, pieces=(), kind=jnp.bfloat16):
    entries = jax.random.normal(key, shape, jnp.float32) * deviation
    if len(pieces) > 0:
        entries = block_levels(key, shape, pieces, -0.22, 0.18) * entries
    return jnp.clip(entries, min=-limit, max=limit).astype(kind)


def bell_draw_with(stream_key, shape, deviation, bound, pieces, heavy, kind=jnp.bfloat16):
    entries = deviation * jax.random.normal(stream_key, shape, jnp.float32)
    if pieces:
        entries = entries * block_levels(stream_key, shape, pieces, -0.22, 0.18)
    return jnp.clip(strengthened(entries, jax.random.fold_in(stream_key, 3), *heavy), -bound, bound).astype(kind)


def setup_inputs(seed: int = 0) -> dict:
    key_list = jax.random.split(jax.random.key(seed), 8)
    return {
        "layer_input": draw_layer_input(jax.random.fold_in(key_list[7], 71), 0),
        "output_grad": bell_draw_with(key_list[1], (TOKENS, D), 4.0, 24.0, ((0, 8), (1, 4)), (0, 1, 8, 2.0)),
        "query_weight": scatter_about(key_list[2], (D, HEADS * HEAD), D ** -0.5, 0.09375, ((1, 4),)),
        "key_weight": scatter_about(key_list[3], (D, KV_HEADS * HEAD), D ** -0.5, 0.09375, ((1, 4),)),
        "value_weight": scatter_about(key_list[4], (D, KV_HEADS * HEAD), D ** -0.5, 0.09375, ((1, 4),)),
        "out_weight": scatter_about(key_list[5], (HEADS * HEAD, D), (HEADS * HEAD) ** -0.5, 0.125, ((0, 4),)),
        "sink_logit": jnp.clip(3.0 + 4.0 * jax.random.uniform(key_list[6], (HEADS,), jnp.float32) ** block_levels(key_list[6], (HEADS,), ((0, 4),), -0.2, 0.2), 3.0, 7.0),
    }


masked_score = -1e30


def reference(layer_input, output_grad, query_weight, key_weight, value_weight, out_weight, sink_logit):
    seq_len = layer_input.shape[0]
    group_size = HEADS // KV_HEADS
    scaling = HEAD ** -0.5
    block_count = seq_len // WINDOW
    queries = jnp.dot(layer_input, query_weight, preferred_element_type=jnp.float32).astype(jnp.bfloat16)
    queries = queries.reshape(seq_len, KV_HEADS, group_size, HEAD)
    key_rows = jnp.dot(layer_input, key_weight, preferred_element_type=jnp.float32).astype(jnp.bfloat16)
    key_rows = key_rows.reshape(seq_len, KV_HEADS, HEAD)
    value_rows = jnp.dot(layer_input, value_weight, preferred_element_type=jnp.float32).astype(jnp.bfloat16)
    value_rows = value_rows.reshape(seq_len, KV_HEADS, HEAD)
    out_rows_grad = jnp.dot(output_grad, out_weight.T, preferred_element_type=jnp.float32).astype(jnp.bfloat16)
    out_rows_grad = out_rows_grad.reshape(seq_len, KV_HEADS, group_size, HEAD)
    sink_column = sink_logit.astype(jnp.float32).reshape(KV_HEADS, group_size)[:, :, None]
    edge_three = ((WINDOW, WINDOW), (0, 0), (0, 0))
    edge_four = ((WINDOW, WINDOW), (0, 0), (0, 0), (0, 0))
    padded_keys = jnp.pad(key_rows, edge_three)
    padded_values = jnp.pad(value_rows, edge_three)

    def forward_block(block):
        offset = block * WINDOW
        query_block = lax.dynamic_slice_in_dim(queries, offset, WINDOW, 0).astype(jnp.float32)
        grad_block = lax.dynamic_slice_in_dim(out_rows_grad, offset, WINDOW, 0).astype(jnp.float32)
        key_band = lax.dynamic_slice_in_dim(padded_keys, offset, 3 * WINDOW, 0).astype(jnp.float32)
        value_band = lax.dynamic_slice_in_dim(padded_values, offset, 3 * WINDOW, 0).astype(jnp.float32)
        query_pos = offset + jnp.arange(WINDOW, dtype=jnp.int32)
        key_pos = offset - WINDOW + jnp.arange(3 * WINDOW, dtype=jnp.int32)
        in_window = (jnp.abs(query_pos[:, None] - key_pos[None, :]) <= WINDOW) & (key_pos[None, :] >= 0) & (key_pos[None, :] < seq_len)
        scores = jnp.einsum("qkgd,skd->kgqs", query_block, key_band) * scaling
        scores = jnp.where(in_window[None, None], scores, masked_score)
        row_max = jnp.maximum(jnp.max(scores, axis=-1), sink_column)
        row_total = jnp.sum(jnp.exp(scores - row_max[..., None]), axis=-1) + jnp.exp(sink_column - row_max)
        log_total = row_max + jnp.log(row_total)
        soft_weights = jnp.exp(scores - log_total[..., None])
        soft_rounded = soft_weights.astype(jnp.bfloat16)
        attended = jnp.einsum("kgqs,skd->qkgd", soft_rounded.astype(jnp.float32), value_band).astype(jnp.bfloat16)
        row_dots = jnp.sum(grad_block * attended.astype(jnp.float32), axis=-1)
        dots_moved = row_dots.transpose(1, 2, 0)
        prob_grads = jnp.einsum("qkgd,skd->kgqs", grad_block, value_band)
        score_grads = (soft_weights * (prob_grads - dots_moved[..., None])).astype(jnp.bfloat16)
        query_grads = (jnp.einsum("kgqs,skd->qkgd", score_grads.astype(jnp.float32), key_band) * scaling).astype(jnp.bfloat16)
        sink_part = -jnp.sum(jnp.exp(sink_column - log_total) * dots_moved, axis=-1)
        return attended, log_total, row_dots, query_grads, sink_part

    attended, log_total, row_dots, query_grads, sink_parts = lax.map(forward_block, jnp.arange(block_count, dtype=jnp.int32))
    attended = attended.reshape(seq_len, HEADS * HEAD)
    log_total = log_total.transpose(0, 3, 1, 2).reshape(seq_len, KV_HEADS, group_size)
    row_dots = row_dots.reshape(seq_len, KV_HEADS, group_size)
    query_grads = query_grads.reshape(seq_len, HEADS * HEAD)
    sink_grad = jnp.sum(sink_parts, axis=0).reshape(HEADS)
    padded_queries = jnp.pad(queries, edge_four)
    padded_out_grad = jnp.pad(out_rows_grad, edge_four)
    padded_totals = jnp.pad(log_total, edge_three)
    padded_dots = jnp.pad(row_dots, edge_three)

    def key_block(block):
        offset = block * WINDOW
        key_own = lax.dynamic_slice_in_dim(key_rows, offset, WINDOW, 0).astype(jnp.float32)
        value_own = lax.dynamic_slice_in_dim(value_rows, offset, WINDOW, 0).astype(jnp.float32)
        query_band = lax.dynamic_slice_in_dim(padded_queries, offset, 3 * WINDOW, 0).astype(jnp.float32)
        grad_band = lax.dynamic_slice_in_dim(padded_out_grad, offset, 3 * WINDOW, 0).astype(jnp.float32)
        total_band = lax.dynamic_slice_in_dim(padded_totals, offset, 3 * WINDOW, 0).transpose(1, 2, 0)
        dots_band = lax.dynamic_slice_in_dim(padded_dots, offset, 3 * WINDOW, 0).transpose(1, 2, 0)
        query_pos = offset - WINDOW + jnp.arange(3 * WINDOW, dtype=jnp.int32)
        key_pos = offset + jnp.arange(WINDOW, dtype=jnp.int32)
        in_window = (jnp.abs(query_pos[:, None] - key_pos[None, :]) <= WINDOW) & (query_pos[:, None] >= 0) & (query_pos[:, None] < seq_len)
        scores = jnp.einsum("qkgd,skd->kgqs", query_band, key_own) * scaling
        scores = jnp.where(in_window[None, None], scores, masked_score)
        soft_weights = jnp.exp(scores - total_band[..., None])
        soft_rounded = soft_weights.astype(jnp.bfloat16)
        prob_grads = jnp.einsum("qkgd,skd->kgqs", grad_band, value_own)
        score_grads = (soft_weights * (prob_grads - dots_band[..., None])).astype(jnp.bfloat16)
        key_grads = (jnp.einsum("kgqs,qkgd->skd", score_grads.astype(jnp.float32), query_band) * scaling).astype(jnp.bfloat16)
        value_grads = jnp.einsum("kgqs,qkgd->skd", soft_rounded.astype(jnp.float32), grad_band).astype(jnp.bfloat16)
        return key_grads, value_grads

    key_grads, value_grads = lax.map(key_block, jnp.arange(block_count, dtype=jnp.int32))
    key_grads = key_grads.reshape(seq_len, KV_HEADS * HEAD)
    value_grads = value_grads.reshape(seq_len, KV_HEADS * HEAD)
    input_grad = (jnp.dot(query_grads, query_weight.T, preferred_element_type=jnp.float32)
                  + jnp.dot(key_grads, key_weight.T, preferred_element_type=jnp.float32)
                  + jnp.dot(value_grads, value_weight.T, preferred_element_type=jnp.float32)).astype(jnp.bfloat16)
    query_weight_grad = jnp.dot(layer_input.T, query_grads, preferred_element_type=jnp.float32)
    key_weight_grad = jnp.dot(layer_input.T, key_grads, preferred_element_type=jnp.float32)
    value_weight_grad = jnp.dot(layer_input.T, value_grads, preferred_element_type=jnp.float32)
    out_weight_grad = jnp.dot(attended.T, output_grad, preferred_element_type=jnp.float32)
    return (input_grad, query_weight_grad, key_weight_grad, value_weight_grad, out_weight_grad, sink_grad)
```

```python
import functools

import jax
import jax.numpy as jnp
from jax import lax
from jax.experimental import pallas as pl
from jax.experimental.pallas import tpu as pltpu
from jax.sharding import PartitionSpec as P

HEADS = 16
KV_HEADS = 8
HEAD = 128
WINDOW = 128


masked_score = -1e30


def extended(cells, sides, width):
    for axis, dim in sides:
        count = lax.axis_size(axis)
        ends = count - 1
        head = lax.slice_in_dim(cells, 0, width, axis=dim)
        tail = lax.slice_in_dim(cells, cells.shape[dim] - width, cells.shape[dim], axis=dim)
        cells = jnp.concatenate(
            [
                lax.ppermute(tail, axis, [(i, (i + 1) % count) for i in range(ends)]),
                cells,
                lax.ppermute(head, axis, [((i + 1) % count, i) for i in range(ends)]),
            ],
            axis=dim,
        )
    return cells


def passed_along(value, axis, steps):
    count = lax.axis_size(axis)
    initial, last = (max(0, -steps), min(count, count - steps))
    return lax.ppermute(value, axis, [(source, source + steps) for source in range(initial, last)])


def contract_rows(left, right):
    return lax.dot_general(
        left, right, (((0,), (0,)), ((), ())), preferred_element_type=jnp.float32
    )


def contract_cols(left, right):
    return lax.dot_general(
        left, right, (((1,), (1,)), ((), ())), preferred_element_type=jnp.float32
    )


def per_device(
    layer_input, output_grad, query_weight, key_weight, value_weight, out_weight, sink_logit
):
    whole_input, whole_grad = (
        lax.all_gather(layer_input, "tp", axis=1, tiled=True),
        lax.all_gather(output_grad, "tp", axis=1, tiled=True),
    )
    tok_rows = whole_input.shape[0]
    query_cols = query_weight.shape[1]
    key_cols = key_weight.shape[1]
    key_heads = key_cols // HEAD
    group_size = HEADS // KV_HEADS
    scaling = HEAD ** (-0.5)
    queries = jnp.dot(whole_input, query_weight, preferred_element_type=jnp.float32).astype(
        jnp.bfloat16
    )
    key_rows = jnp.dot(whole_input, key_weight, preferred_element_type=jnp.float32).astype(
        jnp.bfloat16
    )
    value_rows = jnp.dot(whole_input, value_weight, preferred_element_type=jnp.float32).astype(
        jnp.bfloat16
    )
    out_rows_grad = contract_cols(whole_grad, out_weight).astype(jnp.bfloat16)
    joined = jnp.concatenate([key_rows, value_rows], axis=1)
    band = extended(joined, (("sp", 0),), WINDOW)
    band_rows = band.shape[0]
    band_keys = band[:, :key_cols].reshape(band_rows, key_heads, HEAD)
    band_values = band[:, key_cols:].reshape(band_rows, key_heads, HEAD)
    shard_index = lax.axis_index("sp")
    seq_total = tok_rows * lax.axis_size("sp")
    query_pos = shard_index * tok_rows + jnp.arange(tok_rows, dtype=jnp.int32)
    key_pos = shard_index * tok_rows - WINDOW + jnp.arange(band_rows, dtype=jnp.int32)
    in_window = (
        (jnp.abs(query_pos[:, None] - key_pos[None, :]) <= WINDOW)
        & (key_pos[None, :] >= 0)
        & (key_pos[None, :] < seq_total)
    )
    query_heads = queries.reshape(tok_rows, key_heads, group_size, HEAD)
    grad_heads = out_rows_grad.reshape(tok_rows, key_heads, group_size, HEAD)
    scores = (
        jnp.einsum("qkgd,skd->kgqs", query_heads, band_keys, preferred_element_type=jnp.float32)
        * scaling
    )
    scores = jnp.where(in_window[None, None], scores, masked_score)
    sink_column = sink_logit.reshape(key_heads, group_size)[:, :, None]
    row_max = jnp.maximum(jnp.max(scores, axis=-1), sink_column)
    row_total = jnp.sum(jnp.exp(scores - row_max[..., None]), axis=-1) + jnp.exp(
        sink_column - row_max
    )
    log_total = row_max + jnp.log(row_total)
    soft_weights = jnp.exp(scores - log_total[..., None])
    soft_rounded = soft_weights.astype(jnp.bfloat16)
    attended = jnp.einsum(
        "kgqs,skd->qkgd", soft_rounded, band_values, preferred_element_type=jnp.float32
    ).astype(jnp.bfloat16)
    row_dots = jnp.sum(
        grad_heads.astype(jnp.float32) * attended.astype(jnp.float32), axis=-1
    ).transpose(1, 2, 0)
    prob_grads = jnp.einsum(
        "qkgd,skd->kgqs", grad_heads, band_values, preferred_element_type=jnp.float32
    )
    score_grads = (soft_weights * (prob_grads - row_dots[..., None])).astype(jnp.bfloat16)
    query_grads = (
        jnp.einsum("kgqs,skd->qkgd", score_grads, band_keys, preferred_element_type=jnp.float32)
        * scaling
    )
    query_grads = query_grads.astype(jnp.bfloat16).reshape(tok_rows, query_cols)
    band_key_grads = (
        jnp.einsum("kgqs,qkgd->skd", score_grads, query_heads, preferred_element_type=jnp.float32)
        * scaling
    )
    band_value_grads = jnp.einsum(
        "kgqs,qkgd->skd", soft_rounded, grad_heads, preferred_element_type=jnp.float32
    )
    band_grads = jnp.concatenate(
        [
            band_key_grads.reshape(band_rows, key_cols),
            band_value_grads.reshape(band_rows, key_cols),
        ],
        axis=1,
    )
    sink_part = -jnp.sum(jnp.exp(sink_column - log_total) * row_dots, axis=-1).reshape(-1)
    sink_grad = lax.psum(sink_part, "sp")
    attended_rows = attended.reshape(tok_rows, query_cols)
    input_block = lax.all_to_all(whole_input, "sp", 1, 0, tiled=True)
    grad_block = lax.all_to_all(whole_grad, "sp", 1, 0, tiled=True)
    early_rows = lax.all_gather(
        jnp.concatenate([query_grads, attended_rows], axis=1), "sp", axis=0, tiled=True
    )
    query_part = contract_rows(input_block, early_rows[:, :query_cols])
    out_part = contract_rows(early_rows[:, query_cols:], grad_block)
    returned_low = passed_along(band_grads[:WINDOW].astype(jnp.bfloat16), "sp", -1).astype(
        jnp.float32
    )
    returned_high = passed_along(
        band_grads[band_rows - WINDOW :].astype(jnp.bfloat16), "sp", 1
    ).astype(jnp.float32)
    own_rows = band_grads[WINDOW : WINDOW + tok_rows]
    own_rows = own_rows.at[tok_rows - WINDOW :].add(returned_low)
    own_rows = own_rows.at[:WINDOW].add(returned_high)
    key_grads = own_rows[:, :key_cols].astype(jnp.bfloat16)
    value_grads = own_rows[:, key_cols:].astype(jnp.bfloat16)
    late_rows = lax.all_gather(
        jnp.concatenate([key_grads, value_grads], axis=1), "sp", axis=0, tiled=True
    )
    key_part = contract_rows(input_block, late_rows[:, :key_cols])
    value_part = contract_rows(input_block, late_rows[:, key_cols:])
    partials = (
        contract_cols(query_grads, query_weight)
        + contract_cols(key_grads, key_weight)
        + contract_cols(value_grads, value_weight)
    )
    input_grad = lax.psum_scatter(
        partials.astype(jnp.bfloat16), "tp", scatter_dimension=1, tiled=True
    )
    return (input_grad, query_part, key_part, value_part, out_part, sink_grad)


LANES = 128
MESH = pl.DeviceIdType.MESH
VMEM_BYTES = 60 * 1024 * 1024


def dot_nn(a, b):
    return jnp.dot(a, b, preferred_element_type=jnp.float32)


def layer_kernel(
    x_ref, g_ref, wq_hbm, wk_hbm, wv_hbm, wo_hbm, sink_ref,
    ig_ref, gq_ref, gk_ref, gv_ref, go_ref, sg_ref,
    wq, wk, wv, wo, xg, acc, kvs, acts, att, dqs, dkv, cols,
    soft, sink_soft, sinks, part, rs_in,
    w_sem, ag_send, ag_recv, col_send, col_recv, y_send, y_recv, chip_send, chip_recv,
    z_sem, cross_sem, acts_recv, rs_send, rs_recv,
):
    bf16, f32 = jnp.bfloat16, jnp.float32
    count, tps = lax.axis_size("sp"), lax.axis_size("tp")
    depth = count // 2
    s, t = lax.axis_index("sp"), lax.axis_index("tp")
    z, x = s // 2, s % 2
    y, core = t // 2, t % 2
    partner = y * 2 + (1 - core)
    across = (1 - y) * 2 + core
    diag = (1 - y) * 2 + (1 - core)
    rows, feats = x_ref.shape
    q_cols, k_cols = wq.shape[1], wk.shape[1]
    block_cols = gq_ref.shape[0]
    per_slot = feats // block_cols
    key_heads = k_cols // HEAD
    group = q_cols // k_cols
    scaling = HEAD**-0.5

    def remote(src, dst, send, recv, dev_s, dev_t):
        return pltpu.make_async_remote_copy(
            src_ref=src, dst_ref=dst, send_sem=send, recv_sem=recv,
            device_id=(dev_s, dev_t), device_id_type=MESH,
        )

    weights = [
        pltpu.make_async_copy(src, dst, w_sem.at[i])
        for i, (src, dst) in enumerate(((wq_hbm, wq), (wk_hbm, wk), (wv_hbm, wv), (wo_hbm, wo)))
    ]
    for copy in weights:
        copy.start()

    barrier = pltpu.get_barrier_semaphore()
    for peer in (partner, across, diag):
        pl.semaphore_signal(barrier, inc=1, device_id=(s, peer), device_id_type=MESH)
    for d in range(1, count):
        pl.semaphore_signal(
            barrier, inc=1, device_id=((s + d) % count, t), device_id_type=MESH
        )
    pl.semaphore_wait(barrier, 3 + count - 1)

    sources = (x_ref, g_ref)
    to_across = [
        remote(sources[a], xg.at[t, a], ag_send.at[0, a], ag_recv.at[0, a], s, across)
        for a in range(2)
    ]
    to_partner = [
        remote(sources[a], xg.at[t, a], ag_send.at[1, a], ag_recv.at[1, a], s, partner)
        for a in range(2)
    ]
    relay = [
        remote(xg.at[across, a], xg.at[across, a], ag_send.at[2, a], ag_recv.at[2, a], s, partner)
        for a in range(2)
    ]
    for copy in to_across + to_partner:
        copy.start()

    is_home = s // per_slot == t
    is_across = s // per_slot == across
    is_last = jnp.logical_not(is_home | is_across)

    turn = [(s + d) % count for d in range(count)]

    def column_copy(a, b):
        span = pl.ds(b * block_cols, block_cols)
        source, slot = (g_ref.at[:, span], t) if a else (xg.at[across, 0, :, span], across)
        return remote(
            source, cols.at[a, s], col_send.at[a, b], col_recv.at[a, s], slot * per_slot + b, t
        )

    def column_arrival(a, source):
        ref = cols.at[a, source]
        return remote(ref, ref, col_send.at[a, 0], col_recv.at[a, source], turn[1], t)

    def y_copy(a, source):
        ref = cols.at[a, source]
        return remote(ref, ref, y_send.at[a, source], y_recv.at[a, source], s, across)

    def chip_copy(a, source):
        ref = cols.at[a, source]
        return remote(ref, ref, chip_send.at[a, source], chip_recv.at[a, source], s, partner)

    def each_column(a, act):
        slot = t if a else across
        for b in range(per_slot):

            @pl.when(slot * per_slot + b != s)
            def _():
                act(column_copy(a, b))

    def send_columns(a):
        each_column(a, lambda copy: copy.start())

    send_columns(1)

    def project_input(slot, first=False):
        cells = x_ref[...] if first else xg[slot, 0]
        span = pl.ds(pl.multiple_of(slot * feats, feats), feats)
        at = 0
        for w in (wq, wk, wv):
            wide = w.shape[1]
            term = dot_nn(cells, w[span, :])
            acc[:, at : at + wide] = term if first else acc[:, at : at + wide] + term
            at += wide

    def project_grad(slot, first=False):
        cells = g_ref[...] if first else xg[slot, 1]
        span = pl.ds(pl.multiple_of(slot * feats, feats), feats)
        term = contract_cols(cells, wo[:, span])
        lo = q_cols + 2 * k_cols
        acc[:, lo:] = term if first else acc[:, lo:] + term

    for edge in (0, WINDOW + count * rows):
        kvs[edge : edge + WINDOW] = jnp.zeros((WINDOW, 2 * k_cols), bf16)
    dkv[...] = jnp.zeros_like(dkv)
    sinks[...] = jnp.zeros_like(sinks)

    for copy in weights:
        copy.wait()
    project_input(t, True)
    project_grad(t, True)
    to_partner[0].wait_recv()
    project_input(partner)
    to_partner[1].wait_recv()
    project_grad(partner)
    to_across[0].wait_recv()
    relay[0].start()
    send_columns(0)
    project_input(across)
    relay[0].wait_recv()
    project_input(diag)
    for b in range(per_slot):
        span = slice(b * block_cols, (b + 1) * block_cols)

        @pl.when(t * per_slot + b == s)
        def _():
            cols[1, s] = g_ref[:, span]

        @pl.when(across * per_slot + b == s)
        def _():
            cols[0, s] = xg[across, 0, :, span]

    band_rows = rows + 2 * WINDOW
    tall = group * rows
    side_first = 1 - x

    def own_rows(block):
        return pl.ds(pl.multiple_of(WINDOW + block * rows, 32), rows)

    def band_at(block):
        return pl.ds(pl.multiple_of(block * rows, 32), band_rows)

    def item(i, block):
        return acts.at[i - 1, block] if i else kvs.at[own_rows(block)]

    def z_copy(i, block, way):
        dev = (z + 1 - 2 * way + depth) % depth * 2 + x
        ref = item(i, block)
        return remote(ref, ref, z_sem.at[way, i, block], acts_recv.at[i, block], dev, t)

    def cross_copy(i, block):
        ref = item(i, block)
        return remote(
            ref, ref, cross_sem.at[i, block], acts_recv.at[i, block], z * 2 + (1 - x), t
        )

    def goes_on(way):
        return jnp.where(way == 0, z < depth - 1, z > 0)

    def send_own(i):
        cross_copy(i, s).start()
        for way in range(2):

            @pl.when(goes_on(way))
            def _():
                z_copy(i, s, way).start()

    def level_at(d, way):
        level = z - d * (1 - 2 * way)
        return level, (level >= 0) & (level < depth)

    def forward(i, d):
        def one(k, _):
            way = lax.rem(side_first + k, 2)
            level, there = level_at(d, way)

            @pl.when(there)
            def _():
                block = level * 2 + x
                z_copy(i, block, way).wait_recv()
                cross_copy(i, block).start()

                @pl.when(goes_on(way))
                def _():
                    z_copy(i, block, way).start()

            return 0

        lax.fori_loop(0, 2, one, 0)

    kvs[own_rows(s)] = acc[:, q_cols : q_cols + 2 * k_cols].astype(bf16)
    send_own(0)
    acts[0, s] = acc[:, :q_cols].astype(bf16)
    send_own(1)

    to_across[1].wait_recv()
    relay[1].start()
    project_grad(across)
    relay[1].wait_recv()
    project_grad(diag)
    acts[1, s] = acc[:, q_cols + 2 * k_cols :].astype(bf16)
    send_own(2)

    def pass_direct(here, a):
        @pl.when(here)
        def _():
            for d, source in enumerate(turn):
                if d:
                    column_arrival(a, source).wait_recv()
                y_copy(a, source).start()
                chip_copy(a, source).start()

    def pass_second(here, a):
        @pl.when(here)
        def _():
            for source in turn:
                y_copy(a, source).wait_recv()
                chip_copy(a, source).start()

    def soften(block):
        row_at = lax.broadcasted_iota(jnp.int32, (tall, 1), 0)
        head_at = row_at // rows
        q_at = lax.broadcasted_iota(jnp.int32, (tall, band_rows), 0) - head_at * rows
        k_at = lax.broadcasted_iota(jnp.int32, (tall, band_rows), 1) - WINDOW
        k_pos = k_at + block * rows
        in_window = (
            (jnp.abs(q_at - k_at) <= WINDOW) & (k_pos >= 0) & (k_pos < rows * count)
        )
        for kh in range(key_heads):
            keys = kvs[band_at(block), kh * HEAD : (kh + 1) * HEAD]
            values = kvs[band_at(block), k_cols + kh * HEAD : k_cols + (kh + 1) * HEAD]
            heads = [kh * group + g for g in range(group)]
            q = jnp.concatenate(
                [acts[0, block, :, h * HEAD : (h + 1) * HEAD] for h in heads], axis=0
            )
            scores = jnp.where(in_window, contract_cols(q, keys) * scaling, masked_score)
            sink = jnp.full((tall, 1), sink_ref[0, kh * group], f32)
            for g in range(1, group):
                sink = jnp.where(head_at == g, sink_ref[0, kh * group + g], sink)
            top = jnp.maximum(jnp.max(scores, axis=1, keepdims=True), sink)
            e = jnp.exp(scores - top)
            sink_e = jnp.exp(sink - top)
            inverse = 1.0 / (jnp.sum(e, axis=1, keepdims=True) + sink_e)
            p = e * inverse
            soft[kh] = p
            sink_soft[kh] = jnp.broadcast_to(sink_e * inverse, (tall, LANES))
            attended = dot_nn(p.astype(bf16), values).astype(bf16)
            for g, h in enumerate(heads):
                att[block, :, h * HEAD : (h + 1) * HEAD] = attended[g * rows : (g + 1) * rows]

    def differentiate(block):
        lane_at = lax.broadcasted_iota(jnp.int32, (8, LANES), 1)
        sink_row = jnp.zeros((8, LANES), f32)
        for kh in range(key_heads):
            k_at = slice(kh * HEAD, (kh + 1) * HEAD)
            v_at = slice(k_cols + kh * HEAD, k_cols + (kh + 1) * HEAD)
            keys, values = kvs[band_at(block), k_at], kvs[band_at(block), v_at]
            heads = [kh * group + g for g in range(group)]
            q, do = (
                jnp.concatenate(
                    [acts[i, block, :, h * HEAD : (h + 1) * HEAD] for h in heads], axis=0
                )
                for i in range(2)
            )
            attended = jnp.concatenate(
                [att[block, :, h * HEAD : (h + 1) * HEAD] for h in heads], axis=0
            )
            dots = jnp.sum(do.astype(f32) * attended.astype(f32), axis=1, keepdims=True)
            p = soft[kh]
            ds = (p * (contract_cols(do, values) - dots)).astype(bf16)
            dq = (dot_nn(ds, keys) * scaling).astype(bf16)
            sink_terms = sink_soft[kh] * dots
            for g, h in enumerate(heads):
                dqs[block, :, h * HEAD : (h + 1) * HEAD] = dq[g * rows : (g + 1) * rows]
                total = -jnp.sum(sink_terms[g * rows : (g + 1) * rows], axis=0, keepdims=True)
                sink_row = jnp.where(lane_at == h, total, sink_row)
            dkv[band_at(block), k_at] += contract_rows(ds, q)
            dkv[band_at(block), v_at] += contract_rows(p.astype(bf16), do)
        sinks[...] += sink_row

    def cross_arrived(i, level):
        cross_copy(i, level * 2 + (1 - x)).wait_recv()

    def attend_own():
        for i in range(3):
            cross_arrived(i, z)

        @pl.when((z == 0) | (z == depth - 1))
        def _():
            block = jnp.where(z == 0, 0, count - 1)
            soften(block)
            differentiate(block)

    def attend(d, way, begin=0, end=None):
        level, there = level_at(d, way)
        cross = level * 2 + (1 - x)
        extra = jnp.where(jnp.where(way == 0, level == 0, level == depth - 1), 1, 0)
        stop = 2 + extra
        nearest = jnp.where(way == 0, 2 * level + 2, 2 * level - 1)
        step = jnp.where(way == 0, -1, 1)
        inside = (x == way) | (extra == 1)
        key_at = jnp.where(x == way, 0, 1)

        def one(k, _):
            is_end = k == stop - 1
            block = nearest + step * k
            passed = jnp.where(way == 0, block <= cross, block >= cross)
            block = jnp.where(inside & passed, block + step, block)
            block = jnp.where(inside & is_end, cross, block)

            @pl.when(k == key_at)
            def _():
                cross_arrived(0, level)

            @pl.when(is_end)
            def _():
                cross_arrived(1, level)

            soften(block)

            @pl.when(is_end)
            def _():
                cross_arrived(2, level)

            differentiate(block)
            return 0

        last = stop if end is None else jnp.minimum(stop, end)
        lax.fori_loop(begin, jnp.where(there, last, begin), one, 0)

    def attend_both(d):
        lax.fori_loop(0, 2, lambda k, _: attend(d, lax.rem(x + k, 2)) or 0, 0)

    def attended_range(d):
        first = jnp.where(z <= d, 0, 2 * (z - d) + 1)
        last = jnp.where(z + d >= depth - 1, count - 1, 2 * (z + d))
        return first, last + 1

    def consume(block, first=False):
        pieces = (
            (go_ref, contract_rows(att[block], cols[1, block])),
            (gq_ref, contract_rows(cols[0, block], dqs[block])),
        )
        for ref, value in pieces:
            ref[...] += value

    def consume_range(begin, end):
        lax.fori_loop(begin, end, lambda block, _: consume(block) or 0, 0)

    def consume_since(d):
        before, now = attended_range(d - 1), attended_range(d)
        consume_range(now[0], before[0])
        consume_range(before[1], now[1])

    pass_direct(is_home, 1)
    forward(0, 1)
    forward(1, 1)
    attend_own()
    forward(2, 1)
    pass_direct(is_across, 0)
    forward(0, 2)
    forward(1, 2)
    attend(1, x)
    attend(1, 1 - x, 0, 1)
    forward(2, 2)
    pass_second(is_across, 1)
    own_dkv = dkv[own_rows(s)]
    own_dk = (own_dkv[:, :k_cols] * scaling).astype(bf16)
    own_dv = own_dkv[:, k_cols:].astype(bf16)

    def partial_for(slot):
        span = pl.ds(pl.multiple_of(slot * feats, feats), feats)
        return (
            contract_cols(dqs[s], wq[span, :])
            + contract_cols(own_dk, wk[span, :])
            + contract_cols(own_dv, wv[span, :])
        )

    rs_copies = [
        remote(part.at[i], rs_in.at[i], rs_send.at[i], rs_recv.at[i], s, peer)
        for i, peer in enumerate((partner, partner, across))
    ]
    for i, slot in enumerate((diag, partner)):
        part[i] = partial_for(slot).astype(bf16)
        rs_copies[i].start()
    far = partial_for(across)
    rs_copies[0].wait_recv()
    part[2] = (far + rs_in[0].astype(f32)).astype(bf16)
    rs_copies[2].start()
    ig_acc = acc.at[:, :feats]
    ig_acc[...] = partial_for(t)
    go_ref[...] = jnp.zeros_like(go_ref)
    gq_ref[...] = jnp.zeros_like(gq_ref)

    for d in range(3, depth):
        forward(0, d)
        forward(1, d)
    attend(1, 1 - x, 1)
    pass_second(is_home, 0)
    @pl.when(is_last)
    def _():
        for source in range(count):
            for a in range(2):
                chip_copy(a, source).wait_recv()

    consume_range(*attended_range(1))
    attend_both(2)
    for d in range(3, depth):
        forward(2, d)
    consume_since(2)
    for copy in rs_copies[1:]:
        copy.wait_recv()
    ig_ref[...] = (
        ig_acc[...] + rs_in[1].astype(f32) + rs_in[2].astype(f32)
    ).astype(bf16)
    for d in range(3, depth):
        attend_both(d)
        consume_since(d)
    sg_ref[...] = sinks[...]
    seq = pl.ds(WINDOW, count * rows)
    left = cols[0].reshape(count * rows, block_cols)
    gk_ref[...] = contract_rows(left, (dkv[seq, :k_cols] * scaling).astype(bf16))
    gv_ref[...] = contract_rows(left, dkv[seq, k_cols:].astype(bf16))

    for copy in to_across + to_partner + relay + rs_copies:
        copy.wait_send()
    for a in range(2):
        each_column(a, lambda copy: copy.wait_send())
        for source in range(count):

            @pl.when(is_home if a else is_across)
            def _():
                y_copy(a, source).wait_send()

            @pl.when(jnp.logical_not(is_last))
            def _():
                chip_copy(a, source).wait_send()

    for i in range(3):
        for level in range(depth):
            block = level * 2 + x
            for way in range(2):
                came = jnp.where(way == 0, level <= z, level >= z)

                @pl.when(came & goes_on(way))
                def _():
                    z_copy(i, block, way).wait_send()

            cross_copy(i, block).wait_send()


def store_kernel(*refs):
    ins, sink_in, outs, sink_out = refs[:5], refs[5], refs[6:11], refs[11]
    held, in_sem, out_sem = refs[12:17], refs[17], refs[18]
    loads = [pltpu.make_async_copy(ins[i], held[i], in_sem.at[i]) for i in range(5)]
    stores = [pltpu.make_async_copy(held[i], outs[i], out_sem.at[i]) for i in range(5)]
    for load in loads:
        load.start()
    sink_out[...] = sink_in[0:1, : sink_out.shape[1]]
    for load, store in zip(loads, stores):
        load.wait()
        store.start()
    for store in stores:
        store.wait()


def fused_device(
    layer_input, output_grad, query_weight, key_weight, value_weight, out_weight, sink_logit
):
    bf16, f32 = jnp.bfloat16, jnp.float32
    count, tps = lax.axis_size("sp"), lax.axis_size("tp")
    rows, feats = layer_input.shape
    width = query_weight.shape[0]
    q_cols, k_cols = query_weight.shape[1], key_weight.shape[1]
    block_cols = width // count
    vmem = pl.BlockSpec(memory_space=pltpu.VMEM)
    hbm = pl.BlockSpec(memory_space=pl.ANY)
    dma = pltpu.SemaphoreType.DMA
    outs = pl.pallas_call(
        layer_kernel,
        out_shape=(
            jax.ShapeDtypeStruct((rows, feats), bf16),
            jax.ShapeDtypeStruct((block_cols, q_cols), f32),
            jax.ShapeDtypeStruct((block_cols, k_cols), f32),
            jax.ShapeDtypeStruct((block_cols, k_cols), f32),
            jax.ShapeDtypeStruct((q_cols, block_cols), f32),
            jax.ShapeDtypeStruct((8, LANES), f32),
        ),
        in_specs=[vmem, vmem, hbm, hbm, hbm, hbm, pl.BlockSpec(memory_space=pltpu.SMEM)],
        out_specs=(vmem,) * 6,
        scratch_shapes=[
            pltpu.VMEM(query_weight.shape, bf16),
            pltpu.VMEM(key_weight.shape, bf16),
            pltpu.VMEM(value_weight.shape, bf16),
            pltpu.VMEM(out_weight.shape, bf16),
            pltpu.VMEM((tps, 2, rows, feats), bf16),
            pltpu.VMEM((rows, 2 * q_cols + 2 * k_cols), f32),
            pltpu.VMEM((count * rows + 2 * WINDOW, 2 * k_cols), bf16),
            pltpu.VMEM((2, count, rows, q_cols), bf16),
            pltpu.VMEM((count, rows, q_cols), bf16),
            pltpu.VMEM((count, rows, q_cols), bf16),
            pltpu.VMEM((count * rows + 2 * WINDOW, 2 * k_cols), f32),
            pltpu.VMEM((2, count, rows, block_cols), bf16),
            pltpu.VMEM((k_cols // HEAD, q_cols // k_cols * rows, rows + 2 * WINDOW), f32),
            pltpu.VMEM((k_cols // HEAD, q_cols // k_cols * rows, LANES), f32),
            pltpu.VMEM((8, LANES), f32),
            pltpu.VMEM((3, rows, feats), bf16),
            pltpu.VMEM((3, rows, feats), bf16),
            dma((4,)), dma((3, 2)), dma((3, 2)),
            dma((2, feats // block_cols)), dma((2, count)),
            dma((2, count)), dma((2, count)), dma((2, count)), dma((2, count)),
            dma((2, 3, count)), dma((3, count)), dma((3, count)), dma((3,)), dma((3,)),
        ],
        compiler_params=pltpu.CompilerParams(
            collective_id=0, has_side_effects=True, vmem_limit_bytes=VMEM_BYTES
        ),
        name="layer",
    )(
        layer_input, output_grad, query_weight, key_weight, value_weight, out_weight,
        sink_logit.reshape(1, -1),
    )
    kept = [jax.ShapeDtypeStruct(out.shape, out.dtype) for out in outs[:5]]
    stored = pl.pallas_call(
        store_kernel,
        out_shape=(*kept, jax.ShapeDtypeStruct((1, sink_logit.shape[0]), f32)),
        in_specs=[hbm] * 5 + [vmem],
        out_specs=(hbm,) * 5 + (vmem,),
        scratch_shapes=[pltpu.VMEM(out.shape, out.dtype) for out in kept]
        + [dma((5,)), dma((5,))],
        compiler_params=pltpu.CompilerParams(vmem_limit_bytes=VMEM_BYTES),
        name="store",
    )(*outs)
    return tuple(stored[:5]) + (stored[5].reshape(-1),)


def fits_kernel(mesh, layer_width):
    count, tps = mesh.shape["sp"], mesh.shape["tp"]
    return tps == 4 and count % 8 == 0 and layer_width == count * tps * LANES and HEADS == 2 * KV_HEADS


def solution(mesh):
    placed = (
        P("sp", "tp"),
        P("sp", "tp"),
        P(None, "tp"),
        P(None, "tp"),
        P(None, "tp"),
        P("tp", None),
        P("tp"),
    )

    def sharded(*arrays):
        width = arrays[0].shape[1]
        body = fused_device if fits_kernel(mesh, width) else per_device
        return jax.shard_map(
            body,
            mesh=mesh,
            in_specs=placed,
            out_specs=(
                P("sp", "tp"),
                P("sp", "tp"),
                P("sp", "tp"),
                P("sp", "tp"),
                P("tp", "sp"),
                P("tp"),
            ),
            check_vma=False,
        )(*arrays)

    return sharded
```

```python
import functools

import jax
import jax.numpy as jnp
from jax import lax
from jax.experimental import pallas as pl
from jax.experimental.pallas import tpu as pltpu
from jax.sharding import PartitionSpec as P

HEADS = 16
KV_HEADS = 8
HEAD = 128
WINDOW = 128


masked_score = -1e30


def extended(cells, sides, width):
    for axis, dim in sides:
        count = lax.axis_size(axis)
        ends = count - 1
        head = lax.slice_in_dim(cells, 0, width, axis=dim)
        tail = lax.slice_in_dim(cells, cells.shape[dim] - width, cells.shape[dim], axis=dim)
        cells = jnp.concatenate(
            [
                lax.ppermute(tail, axis, [(i, (i + 1) % count) for i in range(ends)]),
                cells,
                lax.ppermute(head, axis, [((i + 1) % count, i) for i in range(ends)]),
            ],
            axis=dim,
        )
    return cells


def passed_along(value, axis, steps):
    count = lax.axis_size(axis)
    initial, last = (max(0, -steps), min(count, count - steps))
    return lax.ppermute(value, axis, [(source, source + steps) for source in range(initial, last)])


def contract_rows(left, right):
    return lax.dot_general(
        left, right, (((0,), (0,)), ((), ())), preferred_element_type=jnp.float32
    )


def contract_cols(left, right):
    return lax.dot_general(
        left, right, (((1,), (1,)), ((), ())), preferred_element_type=jnp.float32
    )


def per_device(
    layer_input, output_grad, query_weight, key_weight, value_weight, out_weight, sink_logit
):
    whole_input, whole_grad = (
        lax.all_gather(layer_input, "tp", axis=1, tiled=True),
        lax.all_gather(output_grad, "tp", axis=1, tiled=True),
    )
    tok_rows = whole_input.shape[0]
    query_cols = query_weight.shape[1]
    key_cols = key_weight.shape[1]
    key_heads = key_cols // HEAD
    group_size = HEADS // KV_HEADS
    scaling = HEAD ** (-0.5)
    queries = jnp.dot(whole_input, query_weight, preferred_element_type=jnp.float32).astype(
        jnp.bfloat16
    )
    key_rows = jnp.dot(whole_input, key_weight, preferred_element_type=jnp.float32).astype(
        jnp.bfloat16
    )
    value_rows = jnp.dot(whole_input, value_weight, preferred_element_type=jnp.float32).astype(
        jnp.bfloat16
    )
    out_rows_grad = contract_cols(whole_grad, out_weight).astype(jnp.bfloat16)
    joined = jnp.concatenate([key_rows, value_rows], axis=1)
    band = extended(joined, (("sp", 0),), WINDOW)
    band_rows = band.shape[0]
    band_keys = band[:, :key_cols].reshape(band_rows, key_heads, HEAD)
    band_values = band[:, key_cols:].reshape(band_rows, key_heads, HEAD)
    shard_index = lax.axis_index("sp")
    seq_total = tok_rows * lax.axis_size("sp")
    query_pos = shard_index * tok_rows + jnp.arange(tok_rows, dtype=jnp.int32)
    key_pos = shard_index * tok_rows - WINDOW + jnp.arange(band_rows, dtype=jnp.int32)
    in_window = (
        (jnp.abs(query_pos[:, None] - key_pos[None, :]) <= WINDOW)
        & (key_pos[None, :] >= 0)
        & (key_pos[None, :] < seq_total)
    )
    query_heads = queries.reshape(tok_rows, key_heads, group_size, HEAD)
    grad_heads = out_rows_grad.reshape(tok_rows, key_heads, group_size, HEAD)
    scores = (
        jnp.einsum("qkgd,skd->kgqs", query_heads, band_keys, preferred_element_type=jnp.float32)
        * scaling
    )
    scores = jnp.where(in_window[None, None], scores, masked_score)
    sink_column = sink_logit.reshape(key_heads, group_size)[:, :, None]
    row_max = jnp.maximum(jnp.max(scores, axis=-1), sink_column)
    row_total = jnp.sum(jnp.exp(scores - row_max[..., None]), axis=-1) + jnp.exp(
        sink_column - row_max
    )
    log_total = row_max + jnp.log(row_total)
    soft_weights = jnp.exp(scores - log_total[..., None])
    soft_rounded = soft_weights.astype(jnp.bfloat16)
    attended = jnp.einsum(
        "kgqs,skd->qkgd", soft_rounded, band_values, preferred_element_type=jnp.float32
    ).astype(jnp.bfloat16)
    row_dots = jnp.sum(
        grad_heads.astype(jnp.float32) * attended.astype(jnp.float32), axis=-1
    ).transpose(1, 2, 0)
    prob_grads = jnp.einsum(
        "qkgd,skd->kgqs", grad_heads, band_values, preferred_element_type=jnp.float32
    )
    score_grads = (soft_weights * (prob_grads - row_dots[..., None])).astype(jnp.bfloat16)
    query_grads = (
        jnp.einsum("kgqs,skd->qkgd", score_grads, band_keys, preferred_element_type=jnp.float32)
        * scaling
    )
    query_grads = query_grads.astype(jnp.bfloat16).reshape(tok_rows, query_cols)
    band_key_grads = (
        jnp.einsum("kgqs,qkgd->skd", score_grads, query_heads, preferred_element_type=jnp.float32)
        * scaling
    )
    band_value_grads = jnp.einsum(
        "kgqs,qkgd->skd", soft_rounded, grad_heads, preferred_element_type=jnp.float32
    )
    band_grads = jnp.concatenate(
        [
            band_key_grads.reshape(band_rows, key_cols),
            band_value_grads.reshape(band_rows, key_cols),
        ],
        axis=1,
    )
    sink_part = -jnp.sum(jnp.exp(sink_column - log_total) * row_dots, axis=-1).reshape(-1)
    sink_grad = lax.psum(sink_part, "sp")
    attended_rows = attended.reshape(tok_rows, query_cols)
    input_block = lax.all_to_all(whole_input, "sp", 1, 0, tiled=True)
    grad_block = lax.all_to_all(whole_grad, "sp", 1, 0, tiled=True)
    early_rows = lax.all_gather(
        jnp.concatenate([query_grads, attended_rows], axis=1), "sp", axis=0, tiled=True
    )
    query_part = contract_rows(input_block, early_rows[:, :query_cols])
    out_part = contract_rows(early_rows[:, query_cols:], grad_block)
    returned_low = passed_along(band_grads[:WINDOW].astype(jnp.bfloat16), "sp", -1).astype(
        jnp.float32
    )
    returned_high = passed_along(
        band_grads[band_rows - WINDOW :].astype(jnp.bfloat16), "sp", 1
    ).astype(jnp.float32)
    own_rows = band_grads[WINDOW : WINDOW + tok_rows]
    own_rows = own_rows.at[tok_rows - WINDOW :].add(returned_low)
    own_rows = own_rows.at[:WINDOW].add(returned_high)
    key_grads = own_rows[:, :key_cols].astype(jnp.bfloat16)
    value_grads = own_rows[:, key_cols:].astype(jnp.bfloat16)
    late_rows = lax.all_gather(
        jnp.concatenate([key_grads, value_grads], axis=1), "sp", axis=0, tiled=True
    )
    key_part = contract_rows(input_block, late_rows[:, :key_cols])
    value_part = contract_rows(input_block, late_rows[:, key_cols:])
    partials = (
        contract_cols(query_grads, query_weight)
        + contract_cols(key_grads, key_weight)
        + contract_cols(value_grads, value_weight)
    )
    input_grad = lax.psum_scatter(
        partials.astype(jnp.bfloat16), "tp", scatter_dimension=1, tiled=True
    )
    return (input_grad, query_part, key_part, value_part, out_part, sink_grad)


LANES = 128
LOG2E = 1.4426950408889634
MESH = pl.DeviceIdType.MESH
VMEM_BYTES = 46 * 1024 * 1024
STORE_BYTES = 8 * 1024 * 1024


def dot_nn(a, b):
    return jnp.dot(a, b, preferred_element_type=jnp.float32)


def layer_kernel(
    x_hbm, g_hbm, wq_hbm, wk_hbm, wv_hbm, wo_hbm, sink_hbm,
    ig_ref, gq_ref, gk_ref, gv_ref, go_ref, sg_ref,
    w_in, wo, xg, acc, kvs, acts, att, dqs, dkv, cols, bias, sinks, part, rs_in, sink_ref,
    w_sem, ag_send, ag_recv, col_send, col_recv, y_send, y_recv, chip_send, chip_recv,
    z_sem, cross_sem, acts_recv, rs_send, rs_recv,
):
    bf16, f32 = jnp.bfloat16, jnp.float32
    count, tps = lax.axis_size("sp"), lax.axis_size("tp")
    depth = count // 2
    s, t = lax.axis_index("sp"), lax.axis_index("tp")
    z, x = s // 2, s % 2
    y, core = t // 2, t % 2
    partner = y * 2 + (1 - core)
    across = (1 - y) * 2 + core
    diag = (1 - y) * 2 + (1 - core)
    rows, feats = x_hbm.shape
    q_cols, k_cols = wq_hbm.shape[1], wk_hbm.shape[1]
    in_cols = q_cols + 2 * k_cols
    block_cols = gq_ref.shape[0]
    per_slot = feats // block_cols
    key_heads = k_cols // HEAD
    group = q_cols // k_cols
    scaling = HEAD**-0.5

    def remote(src, dst, send, recv, dev_s, dev_t):
        return pltpu.make_async_remote_copy(
            src_ref=src, dst_ref=dst, send_sem=send, recv_sem=recv,
            device_id=(dev_s, dev_t), device_id_type=MESH,
        )

    own = [
        pltpu.make_async_copy(src, xg.at[t, a], w_sem.at[4 + a])
        for a, src in enumerate((x_hbm, g_hbm))
    ]
    for copy in own:
        copy.start()
    weights, at = [], 0
    for i, src in enumerate((wq_hbm, wk_hbm, wv_hbm)):
        span = pl.ds(at, src.shape[1])
        weights.append(pltpu.make_async_copy(src, w_in.at[:, span], w_sem.at[i]))
        at += src.shape[1]
    weights.append(pltpu.make_async_copy(wo_hbm, wo, w_sem.at[3]))
    weights.append(pltpu.make_async_copy(sink_hbm, sink_ref, w_sem.at[6]))
    for copy in weights:
        copy.start()

    barrier = pltpu.get_barrier_semaphore()
    for peer in (partner, across, diag):
        pl.semaphore_signal(barrier, inc=1, device_id=(s, peer), device_id_type=MESH)
    for d in range(1, count):
        pl.semaphore_signal(
            barrier, inc=1, device_id=((s + d) % count, t), device_id_type=MESH
        )
    pl.semaphore_wait(barrier, 3 + count - 1)

    sources = (xg.at[t, 0], xg.at[t, 1])
    for copy in own:
        copy.wait()
    to_across = [
        remote(sources[a], xg.at[t, a], ag_send.at[0, a], ag_recv.at[0, a], s, across)
        for a in range(2)
    ]
    to_partner = [
        remote(sources[a], xg.at[t, a], ag_send.at[1, a], ag_recv.at[1, a], s, partner)
        for a in range(2)
    ]
    relay = [
        remote(xg.at[across, a], xg.at[across, a], ag_send.at[2, a], ag_recv.at[2, a], s, partner)
        for a in range(2)
    ]
    for copy in to_across + to_partner:
        copy.start()

    is_home = s // per_slot == t
    is_across = s // per_slot == across
    is_last = jnp.logical_not(is_home | is_across)

    turn = [(s + d) % count for d in range(count)]

    def column_copy(a, b):
        span = pl.ds(b * block_cols, block_cols)
        source, slot = (xg.at[t, 1, :, span], t) if a else (xg.at[across, 0, :, span], across)
        return remote(
            source, cols.at[a, s], col_send.at[a, b], col_recv.at[a, s], slot * per_slot + b, t
        )

    def column_arrival(a, source):
        ref = cols.at[a, source]
        return remote(ref, ref, col_send.at[a, 0], col_recv.at[a, source], turn[1], t)

    def y_copy(a, source):
        ref = cols.at[a, source]
        return remote(ref, ref, y_send.at[a, source], y_recv.at[a, source], s, across)

    def chip_copy(a, source):
        ref = cols.at[a, source]
        return remote(ref, ref, chip_send.at[a, source], chip_recv.at[a, source], s, partner)

    def each_column(a, act):
        slot = t if a else across
        for b in range(per_slot):

            @pl.when(slot * per_slot + b != s)
            def _():
                act(column_copy(a, b))

    def send_columns(a):
        each_column(a, lambda copy: copy.start())

    send_columns(1)

    def project_input(slot, first=False):
        cells = xg[slot, 0]
        span = pl.ds(pl.multiple_of(slot * feats, feats), feats)
        term = dot_nn(cells, w_in[span, :])
        acc[:, :in_cols] = term if first else acc[:, :in_cols] + term

    def project_grad(slot, first=False):
        cells = xg[slot, 1]
        span = pl.ds(pl.multiple_of(slot * feats, feats), feats)
        term = contract_cols(cells, wo[:, span])
        acc[:, in_cols:] = term if first else acc[:, in_cols:] + term

    for edge in (0, WINDOW + count * rows):
        kvs[edge : edge + WINDOW] = jnp.zeros((WINDOW, 2 * k_cols), bf16)
    dkv[...] = jnp.zeros_like(dkv)
    sinks[...] = jnp.zeros_like(sinks)
    part_rows = rows // 2
    part_keys = part_rows + 2 * WINDOW
    tall = group * part_rows
    edges = -(-WINDOW // part_rows)
    parts = rows * count // part_rows
    q_at = lax.rem(lax.broadcasted_iota(jnp.int32, (tall, part_keys), 0), part_rows)
    k_at = lax.broadcasted_iota(jnp.int32, (tall, part_keys), 1)
    band = (k_at >= q_at) & (k_at - q_at <= 2 * WINDOW)
    starts = [edges] + list(range(edges)) + [parts - edges + i for i in range(edges)]
    for i, start in enumerate(starts):
        pos = k_at + (start * part_rows - WINDOW)
        inside = band & (pos >= 0) & (pos < rows * count) if i else band
        bias[i] = jnp.where(inside, 0.0, masked_score)

    for copy in weights:
        copy.wait()
    project_input(t, True)
    project_grad(t, True)
    to_partner[0].wait_recv()
    project_input(partner)
    to_partner[1].wait_recv()
    project_grad(partner)
    to_across[0].wait_recv()
    relay[0].start()
    send_columns(0)
    project_input(across)
    relay[0].wait_recv()
    project_input(diag)
    for b in range(per_slot):
        span = slice(b * block_cols, (b + 1) * block_cols)

        @pl.when(t * per_slot + b == s)
        def _():
            cols[1, s] = xg[t, 1, :, span]

        @pl.when(across * per_slot + b == s)
        def _():
            cols[0, s] = xg[across, 0, :, span]

    side_first = 1 - x

    def own_rows(block):
        return pl.ds(pl.multiple_of(WINDOW + block * rows, 32), rows)

    def item(i, block):
        return acts.at[i - 1, block] if i else kvs.at[own_rows(block)]

    def z_copy(i, block, way):
        dev = (z + 1 - 2 * way + depth) % depth * 2 + x
        ref = item(i, block)
        return remote(ref, ref, z_sem.at[way, i, block], acts_recv.at[i, block], dev, t)

    def cross_copy(i, block):
        ref = item(i, block)
        return remote(
            ref, ref, cross_sem.at[i, block], acts_recv.at[i, block], z * 2 + (1 - x), t
        )

    def goes_on(way):
        return jnp.where(way == 0, z < depth - 1, z > 0)

    def send_own(i):
        cross_copy(i, s).start()
        for way in range(2):

            @pl.when(goes_on(way))
            def _():
                z_copy(i, s, way).start()

    def level_at(d, way):
        level = z - d * (1 - 2 * way)
        return level, (level >= 0) & (level < depth)

    def forward(i, d):
        def one(k, _):
            way = lax.rem(side_first + k, 2)
            level, there = level_at(d, way)

            @pl.when(there)
            def _():
                block = level * 2 + x
                z_copy(i, block, way).wait_recv()
                cross_copy(i, block).start()

                @pl.when(goes_on(way))
                def _():
                    z_copy(i, block, way).start()

            return 0

        lax.fori_loop(0, 2, one, 0)

    kvs[own_rows(s)] = acc[:, q_cols:in_cols].astype(bf16)
    send_own(0)
    acts[0, s] = acc[:, :q_cols].astype(bf16)
    send_own(1)

    to_across[1].wait_recv()
    relay[1].start()
    project_grad(across)
    relay[1].wait_recv()
    project_grad(diag)
    acts[1, s] = acc[:, in_cols:].astype(bf16)
    send_own(2)

    def pass_direct(here, a):
        @pl.when(here)
        def _():
            for d, source in enumerate(turn):
                if d:
                    column_arrival(a, source).wait_recv()
                y_copy(a, source).start()
                chip_copy(a, source).start()

    def pass_second(here, a):
        @pl.when(here)
        def _():
            for source in turn:
                y_copy(a, source).wait_recv()
                chip_copy(a, source).start()

    def attend_block(block):
        jobs = [(half_at, kh) for half_at in range(2) for kh in range(key_heads)]
        each = range(len(jobs))
        head_at = lax.broadcasted_iota(jnp.int32, (tall, 1), 0) // part_rows

        def at(half_at):
            start = block * rows + half_at * part_rows
            return pl.ds(pl.multiple_of(start, 16), part_keys)

        def stacked(i, half_at, kh):
            span = slice(half_at * part_rows, (half_at + 1) * part_rows)
            heads = [kh * group + g for g in range(group)]
            return jnp.concatenate(
                [acts[i, block, span, h * HEAD : (h + 1) * HEAD] for h in heads], axis=0
            )

        def k_lanes(kh):
            return slice(kh * HEAD, (kh + 1) * HEAD)

        def v_lanes(kh):
            return slice(k_cols + kh * HEAD, k_cols + (kh + 1) * HEAD)

        which = []
        for half_at, _ in jobs:
            part_at = block * 2 + half_at
            late = part_at - (parts - edges)
            which.append(
                jnp.where(part_at < edges, 1 + part_at, jnp.where(late >= 0, 1 + edges + late, 0))
            )
        q = [stacked(0, *job) for job in jobs]
        do = [stacked(1, *job) for job in jobs]
        keys = [kvs[at(half_at), k_lanes(kh)] for half_at, kh in jobs]
        values = [kvs[at(half_at), v_lanes(kh)] for half_at, kh in jobs]
        scores = [contract_cols(q[i], keys[i]) for i in each]
        prob_grads = [contract_cols(do[i], values[i]) for i in each]
        scores = [scores[i] * (scaling * LOG2E) + bias[which[i]] for i in each]
        sink = []
        for _, kh in jobs:
            column = jnp.full((tall, 1), sink_ref[0, kh * group], f32)
            for g in range(1, group):
                column = jnp.where(head_at == g, sink_ref[0, kh * group + g], column)
            sink.append(column * LOG2E)
        top = [jnp.maximum(jnp.max(scores[i], axis=1, keepdims=True), sink[i]) for i in each]
        e = [jnp.exp2(scores[i] - top[i]) for i in each]
        sink_e = [jnp.exp2(sink[i] - top[i]) for i in each]
        inverse = [1.0 / (jnp.sum(e[i], axis=1, keepdims=True) + sink_e[i]) for i in each]
        p = [e[i] * inverse[i] for i in each]
        p_low = [p[i].astype(bf16) for i in each]
        attended = [dot_nn(p_low[i], values[i]).astype(bf16) for i in each]
        dots = [
            jnp.sum(do[i].astype(f32) * attended[i].astype(f32), axis=1, keepdims=True)
            for i in each
        ]
        dv = [contract_rows(p_low[i], do[i]) for i in each]
        ds = [(p[i] * (prob_grads[i] - dots[i])).astype(bf16) for i in each]
        dq = [(dot_nn(ds[i], keys[i]) * scaling).astype(bf16) for i in each]
        dk = [contract_rows(ds[i], q[i]) for i in each]
        lane_at = lax.broadcasted_iota(jnp.int32, (8, LANES), 1)
        sink_row = sinks[...]
        for i, (half_at, kh) in enumerate(jobs):
            span = slice(half_at * part_rows, (half_at + 1) * part_rows)
            sink_terms = sink_e[i] * inverse[i] * dots[i]
            for g in range(group):
                h = kh * group + g
                lanes, piece = slice(h * HEAD, (h + 1) * HEAD), slice(g * part_rows, (g + 1) * part_rows)
                att[block, span, lanes] = attended[i][piece]
                dqs[block, span, lanes] = dq[i][piece]
                total = jnp.sum(sink_terms[piece], axis=0, keepdims=True)
                sink_row = jnp.where(lane_at == h, sink_row - total, sink_row)
            dkv[at(half_at), k_lanes(kh)] += dk[i]
            dkv[at(half_at), v_lanes(kh)] += dv[i]
        sinks[...] = sink_row

    def cross_arrived(i, level):
        cross_copy(i, level * 2 + (1 - x)).wait_recv()

    def attend_own():
        for i in range(3):
            cross_arrived(i, z)

        @pl.when((z == 0) | (z == depth - 1))
        def _():
            block = jnp.where(z == 0, 0, count - 1)
            attend_block(block)

    def attend(d, way, begin=0, end=None):
        level, there = level_at(d, way)
        cross = level * 2 + (1 - x)
        extra = jnp.where(jnp.where(way == 0, level == 0, level == depth - 1), 1, 0)
        stop = 2 + extra
        nearest = jnp.where(way == 0, 2 * level + 2, 2 * level - 1)
        step = jnp.where(way == 0, -1, 1)
        inside = (x == way) | (extra == 1)
        key_at = jnp.where(x == way, 0, 1)

        def one(k, _):
            is_end = k == stop - 1
            block = nearest + step * k
            passed = jnp.where(way == 0, block <= cross, block >= cross)
            block = jnp.where(inside & passed, block + step, block)
            block = jnp.where(inside & is_end, cross, block)

            @pl.when(k == key_at)
            def _():
                cross_arrived(0, level)

            @pl.when(is_end)
            def _():
                cross_arrived(1, level)
                cross_arrived(2, level)

            attend_block(block)
            return 0

        last = stop if end is None else jnp.minimum(stop, end)
        lax.fori_loop(begin, jnp.where(there, last, begin), one, 0)

    def attend_both(d):
        lax.fori_loop(0, 2, lambda k, _: attend(d, lax.rem(x + k, 2)) or 0, 0)

    pass_direct(is_home, 1)
    forward(0, 1)
    forward(1, 1)
    attend_own()
    forward(2, 1)
    pass_direct(is_across, 0)
    forward(0, 2)
    forward(1, 2)
    attend(1, x)
    attend(1, 1 - x, 0, 1)
    forward(2, 2)
    pass_second(is_across, 1)
    own_dkv = dkv[own_rows(s)]
    own_grads = jnp.concatenate(
        [
            dqs[s],
            (own_dkv[:, :k_cols] * scaling).astype(bf16),
            own_dkv[:, k_cols:].astype(bf16),
        ],
        axis=1,
    )

    def partial_for(slot):
        span = pl.ds(pl.multiple_of(slot * feats, feats), feats)
        return contract_cols(own_grads, w_in[span, :])

    rs_copies = [
        remote(part.at[i], rs_in.at[i], rs_send.at[i], rs_recv.at[i], s, peer)
        for i, peer in enumerate((partner, partner, across))
    ]
    for i, slot in enumerate((diag, partner)):
        part[i] = partial_for(slot).astype(bf16)
        rs_copies[i].start()
    far = partial_for(across)
    rs_copies[0].wait_recv()
    part[2] = (far + rs_in[0].astype(f32)).astype(bf16)
    rs_copies[2].start()
    ig_acc = acc.at[:, :feats]
    ig_acc[...] = partial_for(t)

    for d in range(3, depth):
        forward(0, d)
        forward(1, d)
    attend(1, 1 - x, 1)
    pass_second(is_home, 0)
    @pl.when(is_last)
    def _():
        for source in range(count):
            for a in range(2):
                chip_copy(a, source).wait_recv()

    attend_both(2)
    for d in range(3, depth):
        forward(2, d)
    for copy in rs_copies[1:]:
        copy.wait_recv()
    ig_ref[...] = (
        ig_acc[...] + rs_in[1].astype(f32) + rs_in[2].astype(f32)
    ).astype(bf16)
    for d in range(3, depth):
        attend_both(d)
    sg_ref[...] = sinks[...]
    seq = pl.ds(WINDOW, count * rows)
    left = cols[0].reshape(count * rows, block_cols)
    go_ref[...] = contract_rows(
        att[...].reshape(count * rows, q_cols), cols[1].reshape(count * rows, block_cols)
    )
    gq_ref[...] = contract_rows(left, dqs[...].reshape(count * rows, q_cols))
    gk_ref[...] = contract_rows(left, (dkv[seq, :k_cols] * scaling).astype(bf16))
    gv_ref[...] = contract_rows(left, dkv[seq, k_cols:].astype(bf16))

    for copy in to_across + to_partner + relay + rs_copies:
        copy.wait_send()
    for a in range(2):
        each_column(a, lambda copy: copy.wait_send())
        for source in range(count):

            @pl.when(is_home if a else is_across)
            def _():
                y_copy(a, source).wait_send()

            @pl.when(jnp.logical_not(is_last))
            def _():
                chip_copy(a, source).wait_send()

    for i in range(3):
        for level in range(depth):
            block = level * 2 + x
            for way in range(2):
                came = jnp.where(way == 0, level <= z, level >= z)

                @pl.when(came & goes_on(way))
                def _():
                    z_copy(i, block, way).wait_send()

            cross_copy(i, block).wait_send()


def store_kernel(*refs):
    ins, sink_in, outs, sink_out, sem = refs[:5], refs[5], refs[6:11], refs[11], refs[12]
    stores = [pltpu.make_async_copy(ins[i], outs[i], sem.at[i]) for i in range(5)]
    for store in stores:
        store.start()
    sink_out[...] = sink_in[0:1, : sink_out.shape[1]]
    for store in stores:
        store.wait()


def fused_device(
    layer_input, output_grad, query_weight, key_weight, value_weight, out_weight, sink_logit
):
    bf16, f32 = jnp.bfloat16, jnp.float32
    count, tps = lax.axis_size("sp"), lax.axis_size("tp")
    rows, feats = layer_input.shape
    width = query_weight.shape[0]
    q_cols, k_cols = query_weight.shape[1], key_weight.shape[1]
    block_cols = width // count
    vmem = pl.BlockSpec(memory_space=pltpu.VMEM)
    hbm = pl.BlockSpec(memory_space=pltpu.HBM)
    dma = pltpu.SemaphoreType.DMA
    outs = pl.pallas_call(
        layer_kernel,
        out_shape=(
            jax.ShapeDtypeStruct((rows, feats), bf16),
            jax.ShapeDtypeStruct((block_cols, q_cols), f32),
            jax.ShapeDtypeStruct((block_cols, k_cols), f32),
            jax.ShapeDtypeStruct((block_cols, k_cols), f32),
            jax.ShapeDtypeStruct((q_cols, block_cols), f32),
            jax.ShapeDtypeStruct((8, LANES), f32),
        ),
        in_specs=[hbm] * 7,
        out_specs=(vmem,) * 6,
        scratch_shapes=[
            pltpu.VMEM((width, q_cols + 2 * k_cols), bf16),
            pltpu.VMEM(out_weight.shape, bf16),
            pltpu.VMEM((tps, 2, rows, feats), bf16),
            pltpu.VMEM((rows, 2 * q_cols + 2 * k_cols), f32),
            pltpu.VMEM((count * rows + 2 * WINDOW, 2 * k_cols), bf16),
            pltpu.VMEM((2, count, rows, q_cols), bf16),
            pltpu.VMEM((count, rows, q_cols), bf16),
            pltpu.VMEM((count, rows, q_cols), bf16),
            pltpu.VMEM((count * rows + 2 * WINDOW, 2 * k_cols), f32),
            pltpu.VMEM((2, count, rows, block_cols), bf16),
            pltpu.VMEM((1 + 2 * (-(-2 * WINDOW // rows)), q_cols // k_cols * rows // 2, rows // 2 + 2 * WINDOW), f32),
            pltpu.VMEM((8, LANES), f32),
            pltpu.VMEM((3, rows, feats), bf16),
            pltpu.VMEM((3, rows, feats), bf16),
            pltpu.SMEM((1, sink_logit.shape[0]), f32),
            dma((7,)), dma((3, 2)), dma((3, 2)),
            dma((2, feats // block_cols)), dma((2, count)),
            dma((2, count)), dma((2, count)), dma((2, count)), dma((2, count)),
            dma((2, 3, count)), dma((3, count)), dma((3, count)), dma((3,)), dma((3,)),
        ],
        compiler_params=pltpu.CompilerParams(
            collective_id=0, has_side_effects=True, vmem_limit_bytes=VMEM_BYTES
        ),
        name="layer",
    )(
        *(
            pltpu.with_memory_space_constraint(array, pltpu.HBM)
            for array in (
                layer_input, output_grad, query_weight, key_weight, value_weight, out_weight,
                sink_logit.reshape(1, -1),
            )
        ),
    )
    kept = [jax.ShapeDtypeStruct(out.shape, out.dtype) for out in outs[:5]]
    stored = pl.pallas_call(
        store_kernel,
        out_shape=(*kept, jax.ShapeDtypeStruct((1, sink_logit.shape[0]), f32)),
        in_specs=[vmem] * 6,
        out_specs=(hbm,) * 5 + (vmem,),
        scratch_shapes=[dma((5,))],
        compiler_params=pltpu.CompilerParams(vmem_limit_bytes=STORE_BYTES),
        name="store",
    )(*outs)
    return tuple(stored[:5]) + (stored[5].reshape(-1),)


def fits_kernel(mesh, layer_width):
    count, tps = mesh.shape["sp"], mesh.shape["tp"]
    return tps == 4 and count % 8 == 0 and layer_width == count * tps * LANES and HEADS == 2 * KV_HEADS


def solution(mesh):
    placed = (
        P("sp", "tp"),
        P("sp", "tp"),
        P(None, "tp"),
        P(None, "tp"),
        P(None, "tp"),
        P("tp", None),
        P("tp"),
    )

    def sharded(*arrays):
        width = arrays[0].shape[1]
        body = fused_device if fits_kernel(mesh, width) else per_device
        return jax.shard_map(
            body,
            mesh=mesh,
            in_specs=placed,
            out_specs=(
                P("sp", "tp"),
                P("sp", "tp"),
                P("sp", "tp"),
                P("sp", "tp"),
                P("tp", "sp"),
                P("tp"),
            ),
            check_vma=False,
        )(*arrays)

    return sharded
```

```python
import functools

import jax
import jax.numpy as jnp
from jax import lax
from jax.experimental import pallas as pl
from jax.experimental.pallas import tpu as pltpu
from jax.sharding import PartitionSpec as P

HEADS = 16
KV_HEADS = 8
HEAD = 128
WINDOW = 128


masked_score = -1e30


def extended(cells, sides, width):
    for axis, dim in sides:
        count = lax.axis_size(axis)
        ends = count - 1
        head = lax.slice_in_dim(cells, 0, width, axis=dim)
        tail = lax.slice_in_dim(cells, cells.shape[dim] - width, cells.shape[dim], axis=dim)
        cells = jnp.concatenate(
            [
                lax.ppermute(tail, axis, [(i, (i + 1) % count) for i in range(ends)]),
                cells,
                lax.ppermute(head, axis, [((i + 1) % count, i) for i in range(ends)]),
            ],
            axis=dim,
        )
    return cells


def passed_along(value, axis, steps):
    count = lax.axis_size(axis)
    initial, last = (max(0, -steps), min(count, count - steps))
    return lax.ppermute(value, axis, [(source, source + steps) for source in range(initial, last)])


def contract_rows(left, right):
    return lax.dot_general(
        left, right, (((0,), (0,)), ((), ())), preferred_element_type=jnp.float32
    )


def contract_cols(left, right):
    return lax.dot_general(
        left, right, (((1,), (1,)), ((), ())), preferred_element_type=jnp.float32
    )


def per_device(
    layer_input, output_grad, query_weight, key_weight, value_weight, out_weight, sink_logit
):
    whole_input, whole_grad = (
        lax.all_gather(layer_input, "tp", axis=1, tiled=True),
        lax.all_gather(output_grad, "tp", axis=1, tiled=True),
    )
    tok_rows = whole_input.shape[0]
    query_cols = query_weight.shape[1]
    key_cols = key_weight.shape[1]
    key_heads = key_cols // HEAD
    group_size = HEADS // KV_HEADS
    scaling = HEAD ** (-0.5)
    queries = jnp.dot(whole_input, query_weight, preferred_element_type=jnp.float32).astype(
        jnp.bfloat16
    )
    key_rows = jnp.dot(whole_input, key_weight, preferred_element_type=jnp.float32).astype(
        jnp.bfloat16
    )
    value_rows = jnp.dot(whole_input, value_weight, preferred_element_type=jnp.float32).astype(
        jnp.bfloat16
    )
    out_rows_grad = contract_cols(whole_grad, out_weight).astype(jnp.bfloat16)
    joined = jnp.concatenate([key_rows, value_rows], axis=1)
    band = extended(joined, (("sp", 0),), WINDOW)
    band_rows = band.shape[0]
    band_keys = band[:, :key_cols].reshape(band_rows, key_heads, HEAD)
    band_values = band[:, key_cols:].reshape(band_rows, key_heads, HEAD)
    shard_index = lax.axis_index("sp")
    seq_total = tok_rows * lax.axis_size("sp")
    query_pos = shard_index * tok_rows + jnp.arange(tok_rows, dtype=jnp.int32)
    key_pos = shard_index * tok_rows - WINDOW + jnp.arange(band_rows, dtype=jnp.int32)
    in_window = (
        (jnp.abs(query_pos[:, None] - key_pos[None, :]) <= WINDOW)
        & (key_pos[None, :] >= 0)
        & (key_pos[None, :] < seq_total)
    )
    query_heads = queries.reshape(tok_rows, key_heads, group_size, HEAD)
    grad_heads = out_rows_grad.reshape(tok_rows, key_heads, group_size, HEAD)
    scores = (
        jnp.einsum("qkgd,skd->kgqs", query_heads, band_keys, preferred_element_type=jnp.float32)
        * scaling
    )
    scores = jnp.where(in_window[None, None], scores, masked_score)
    sink_column = sink_logit.reshape(key_heads, group_size)[:, :, None]
    row_max = jnp.maximum(jnp.max(scores, axis=-1), sink_column)
    row_total = jnp.sum(jnp.exp(scores - row_max[..., None]), axis=-1) + jnp.exp(
        sink_column - row_max
    )
    log_total = row_max + jnp.log(row_total)
    soft_weights = jnp.exp(scores - log_total[..., None])
    soft_rounded = soft_weights.astype(jnp.bfloat16)
    attended = jnp.einsum(
        "kgqs,skd->qkgd", soft_rounded, band_values, preferred_element_type=jnp.float32
    ).astype(jnp.bfloat16)
    row_dots = jnp.sum(
        grad_heads.astype(jnp.float32) * attended.astype(jnp.float32), axis=-1
    ).transpose(1, 2, 0)
    prob_grads = jnp.einsum(
        "qkgd,skd->kgqs", grad_heads, band_values, preferred_element_type=jnp.float32
    )
    score_grads = (soft_weights * (prob_grads - row_dots[..., None])).astype(jnp.bfloat16)
    query_grads = (
        jnp.einsum("kgqs,skd->qkgd", score_grads, band_keys, preferred_element_type=jnp.float32)
        * scaling
    )
    query_grads = query_grads.astype(jnp.bfloat16).reshape(tok_rows, query_cols)
    band_key_grads = (
        jnp.einsum("kgqs,qkgd->skd", score_grads, query_heads, preferred_element_type=jnp.float32)
        * scaling
    )
    band_value_grads = jnp.einsum(
        "kgqs,qkgd->skd", soft_rounded, grad_heads, preferred_element_type=jnp.float32
    )
    band_grads = jnp.concatenate(
        [
            band_key_grads.reshape(band_rows, key_cols),
            band_value_grads.reshape(band_rows, key_cols),
        ],
        axis=1,
    )
    sink_part = -jnp.sum(jnp.exp(sink_column - log_total) * row_dots, axis=-1).reshape(-1)
    sink_grad = lax.psum(sink_part, "sp")
    attended_rows = attended.reshape(tok_rows, query_cols)
    input_block = lax.all_to_all(whole_input, "sp", 1, 0, tiled=True)
    grad_block = lax.all_to_all(whole_grad, "sp", 1, 0, tiled=True)
    early_rows = lax.all_gather(
        jnp.concatenate([query_grads, attended_rows], axis=1), "sp", axis=0, tiled=True
    )
    query_part = contract_rows(input_block, early_rows[:, :query_cols])
    out_part = contract_rows(early_rows[:, query_cols:], grad_block)
    returned_low = passed_along(band_grads[:WINDOW].astype(jnp.bfloat16), "sp", -1).astype(
        jnp.float32
    )
    returned_high = passed_along(
        band_grads[band_rows - WINDOW :].astype(jnp.bfloat16), "sp", 1
    ).astype(jnp.float32)
    own_rows = band_grads[WINDOW : WINDOW + tok_rows]
    own_rows = own_rows.at[tok_rows - WINDOW :].add(returned_low)
    own_rows = own_rows.at[:WINDOW].add(returned_high)
    key_grads = own_rows[:, :key_cols].astype(jnp.bfloat16)
    value_grads = own_rows[:, key_cols:].astype(jnp.bfloat16)
    late_rows = lax.all_gather(
        jnp.concatenate([key_grads, value_grads], axis=1), "sp", axis=0, tiled=True
    )
    key_part = contract_rows(input_block, late_rows[:, :key_cols])
    value_part = contract_rows(input_block, late_rows[:, key_cols:])
    partials = (
        contract_cols(query_grads, query_weight)
        + contract_cols(key_grads, key_weight)
        + contract_cols(value_grads, value_weight)
    )
    input_grad = lax.psum_scatter(
        partials.astype(jnp.bfloat16), "tp", scatter_dimension=1, tiled=True
    )
    return (input_grad, query_part, key_part, value_part, out_part, sink_grad)


LANES = 128
LOG2E = 1.4426950408889634
MESH = pl.DeviceIdType.MESH
VMEM_BYTES = 46 * 1024 * 1024
STORE_BYTES = 8 * 1024 * 1024


def dot_nn(a, b):
    return jnp.dot(a, b, preferred_element_type=jnp.float32)


def layer_kernel(
    x_hbm, g_hbm, wq_hbm, wk_hbm, wv_hbm, wo_hbm, sink_hbm,
    ig_ref, gq_ref, gk_ref, gv_ref, go_ref, sg_ref,
    w_in, wo, xg, acc, kvs, acts, att, dqs, dkv, cols, bias, sinks, part, rs_in, sink_ref,
    w_sem, ag_send, ag_recv, col_send, col_recv, y_send, y_recv, chip_send, chip_recv,
    z_sem, cross_sem, acts_recv, rs_send, rs_recv,
):
    bf16, f32 = jnp.bfloat16, jnp.float32
    count, tps = lax.axis_size("sp"), lax.axis_size("tp")
    depth = count // 2
    s, t = lax.axis_index("sp"), lax.axis_index("tp")
    z, x = s // 2, s % 2
    y, core = t // 2, t % 2
    partner = y * 2 + (1 - core)
    across = (1 - y) * 2 + core
    diag = (1 - y) * 2 + (1 - core)
    rows, feats = x_hbm.shape
    q_cols, k_cols = wq_hbm.shape[1], wk_hbm.shape[1]
    in_cols = q_cols + 2 * k_cols
    block_cols = gq_ref.shape[0]
    per_slot = feats // block_cols
    key_heads = k_cols // HEAD
    group = q_cols // k_cols
    scaling = HEAD**-0.5

    def remote(src, dst, send, recv, dev_s, dev_t):
        return pltpu.make_async_remote_copy(
            src_ref=src, dst_ref=dst, send_sem=send, recv_sem=recv,
            device_id=(dev_s, dev_t), device_id_type=MESH,
        )

    own = [
        pltpu.make_async_copy(src, xg.at[t, a], w_sem.at[4 + a])
        for a, src in enumerate((x_hbm, g_hbm))
    ]
    for copy in own:
        copy.start()
    weights, at = [], 0
    for i, src in enumerate((wq_hbm, wk_hbm, wv_hbm)):
        span = pl.ds(at, src.shape[1])
        weights.append(pltpu.make_async_copy(src, w_in.at[:, span], w_sem.at[i]))
        at += src.shape[1]
    weights.append(pltpu.make_async_copy(wo_hbm, wo, w_sem.at[3]))
    weights.append(pltpu.make_async_copy(sink_hbm, sink_ref, w_sem.at[6]))
    for copy in weights:
        copy.start()

    barrier = pltpu.get_barrier_semaphore()
    for peer in (partner, across, diag):
        pl.semaphore_signal(barrier, inc=1, device_id=(s, peer), device_id_type=MESH)
    for d in range(1, count):
        pl.semaphore_signal(
            barrier, inc=1, device_id=((s + d) % count, t), device_id_type=MESH
        )
    pl.semaphore_wait(barrier, 3 + count - 1)

    sources = (xg.at[t, 0], xg.at[t, 1])
    for copy in own:
        copy.wait()
    to_across = [
        remote(sources[a], xg.at[t, a], ag_send.at[0, a], ag_recv.at[0, a], s, across)
        for a in range(2)
    ]
    to_partner = [
        remote(sources[a], xg.at[t, a], ag_send.at[1, a], ag_recv.at[1, a], s, partner)
        for a in range(2)
    ]
    relay = [
        remote(xg.at[across, a], xg.at[across, a], ag_send.at[2, a], ag_recv.at[2, a], s, partner)
        for a in range(2)
    ]
    for copy in to_across + to_partner:
        copy.start()

    is_home = s // per_slot == t
    is_across = s // per_slot == across
    is_last = jnp.logical_not(is_home | is_across)

    half = count // 2
    here_half = s // half * half
    near = [here_half + i for i in range(half)]
    far = [half - here_half + i for i in range(half)]
    sends_near = s // half == t * per_slot // half

    def column_copy(kind, b):
        a, slot = kind % 2, t if kind else across
        return remote(
            xg.at[slot, a, :, pl.ds(b * block_cols, block_cols)], cols.at[a, s],
            col_send.at[kind, b], col_recv.at[a, s], slot * per_slot + b, t,
        )

    def column_arrival(a, source):
        ref = cols.at[a, source]
        return remote(ref, ref, col_send.at[a, 0], col_recv.at[a, source], (s + 1) % count, t)

    def y_copy(a, source):
        ref = cols.at[a, source]
        return remote(ref, ref, y_send.at[a, source], y_recv.at[a, source], s, across)

    def chip_copy(a, source):
        ref = cols.at[a, source]
        return remote(ref, ref, chip_send.at[a, source], chip_recv.at[a, source], s, partner)

    def each_column(kind, act):
        slot = t if kind else across
        for b in range(per_slot):
            sent = slot * per_slot + b != s

            @pl.when(sent if kind == 1 else sent & sends_near)
            def _():
                act(column_copy(kind, b))

    def send_columns(kind):
        each_column(kind, lambda copy: copy.start())

    send_columns(1)
    send_columns(2)

    def project_input(slot, first=False):
        cells = xg[slot, 0]
        span = pl.ds(pl.multiple_of(slot * feats, feats), feats)
        term = dot_nn(cells, w_in[span, :])
        acc[:, :in_cols] = term if first else acc[:, :in_cols] + term

    def project_grad(slot, first=False):
        cells = xg[slot, 1]
        span = pl.ds(pl.multiple_of(slot * feats, feats), feats)
        term = contract_cols(cells, wo[:, span])
        acc[:, in_cols:] = term if first else acc[:, in_cols:] + term

    for edge in (0, WINDOW + count * rows):
        kvs[edge : edge + WINDOW] = jnp.zeros((WINDOW, 2 * k_cols), bf16)
    dkv[...] = jnp.zeros_like(dkv)
    sinks[...] = jnp.zeros_like(sinks)
    part_rows = rows // 2
    part_keys = part_rows + 2 * WINDOW
    tall = group * part_rows
    edges = -(-WINDOW // part_rows)
    parts = rows * count // part_rows
    q_at = lax.rem(lax.broadcasted_iota(jnp.int32, (tall, part_keys), 0), part_rows)
    k_at = lax.broadcasted_iota(jnp.int32, (tall, part_keys), 1)
    band = (k_at >= q_at) & (k_at - q_at <= 2 * WINDOW)
    starts = [edges] + list(range(edges)) + [parts - edges + i for i in range(edges)]
    for i, start in enumerate(starts):
        pos = k_at + (start * part_rows - WINDOW)
        inside = band & (pos >= 0) & (pos < rows * count) if i else band
        bias[i] = jnp.where(inside, 0.0, masked_score)

    for copy in weights:
        copy.wait()
    project_input(t, True)
    project_grad(t, True)
    to_partner[0].wait_recv()
    project_input(partner)
    to_partner[1].wait_recv()
    project_grad(partner)
    to_across[0].wait_recv()
    relay[0].start()
    send_columns(0)
    project_input(across)
    relay[0].wait_recv()
    project_input(diag)
    for b in range(per_slot):
        span = slice(b * block_cols, (b + 1) * block_cols)

        @pl.when(t * per_slot + b == s)
        def _():
            for a in range(2):
                cols[a, s] = xg[t, a, :, span]

    side_first = 1 - y

    def own_rows(block):
        return pl.ds(pl.multiple_of(WINDOW + block * rows, 32), rows)

    def item(i, block):
        return acts.at[i - 1, block] if i else kvs.at[own_rows(block)]

    def z_copy(i, block, way):
        dev = (z + 1 - 2 * way + depth) % depth * 2 + x
        ref = item(i, block)
        return remote(ref, ref, z_sem.at[way, i, block], acts_recv.at[i, block], dev, t)

    def cross_copy(i, block):
        ref = item(i, block)
        return remote(
            ref, ref, cross_sem.at[i, block], acts_recv.at[i, block], z * 2 + (1 - x), t
        )

    def goes_on(way):
        return jnp.where(way == 0, z < depth - 1, z > 0)

    def send_own(i):
        cross_copy(i, s).start()
        for way in range(2):

            @pl.when(goes_on(way))
            def _():
                z_copy(i, s, way).start()

    def level_at(d, way):
        level = z - d * (1 - 2 * way)
        return level, (level >= 0) & (level < depth)

    def crosses(i, level):
        return (i > 0) | ((level > 0) & (level < depth - 1)) | (level == z)

    def end_copy(way):
        return z_copy(0, (depth - 1) * way * 2 + (1 - x), way)

    def forward_end(d):
        for way in range(2):
            level, there = level_at(d, way)

            @pl.when(there & (level == (depth - 1) * way))
            def _():
                end_copy(way).wait_recv()

                @pl.when(goes_on(way))
                def _():
                    end_copy(way).start()

    def forward(i, d):
        def one(k, _):
            way = lax.rem(side_first + k, 2)
            level, there = level_at(d, way)

            @pl.when(there)
            def _():
                block = level * 2 + x
                z_copy(i, block, way).wait_recv()

                @pl.when(crosses(i, level))
                def _():
                    cross_copy(i, block).start()

                @pl.when(goes_on(way))
                def _():
                    z_copy(i, block, way).start()

            return 0

        lax.fori_loop(0, 2, one, 0)

    kvs[own_rows(s)] = acc[:, q_cols:in_cols].astype(bf16)
    send_own(0)
    acts[0, s] = acc[:, :q_cols].astype(bf16)
    send_own(1)

    to_across[1].wait_recv()
    relay[1].start()
    project_grad(across)
    relay[1].wait_recv()
    project_grad(diag)
    acts[1, s] = acc[:, in_cols:].astype(bf16)
    send_own(2)

    straight = [(source, a) for source in near for a in range(2)] + [(source, 1) for source in far]
    around = [(source, 0) for source in far]

    def pass_direct(here, items):
        @pl.when(here)
        def _():
            for source, a in items:

                @pl.when(source != s)
                def _():
                    column_arrival(a, source).wait_recv()

                y_copy(a, source).start()
                chip_copy(a, source).start()

    def pass_second(here, items):
        @pl.when(here)
        def _():
            for source, a in items:
                y_copy(a, source).wait_recv()
                chip_copy(a, source).start()

    def last_arrivals(sources):
        @pl.when(is_last)
        def _():
            for source in sources:
                for a in range(2):
                    chip_copy(a, source).wait_recv()

    def attend_block(block):
        jobs = [(half_at, kh) for half_at in range(2) for kh in range(key_heads)]
        each = range(len(jobs))
        head_at = lax.broadcasted_iota(jnp.int32, (tall, 1), 0) // part_rows

        def at(half_at):
            start = block * rows + half_at * part_rows
            return pl.ds(pl.multiple_of(start, 16), part_keys)

        def stacked(i, half_at, kh):
            span = slice(half_at * part_rows, (half_at + 1) * part_rows)
            heads = [kh * group + g for g in range(group)]
            return jnp.concatenate(
                [acts[i, block, span, h * HEAD : (h + 1) * HEAD] for h in heads], axis=0
            )

        def k_lanes(kh):
            return slice(kh * HEAD, (kh + 1) * HEAD)

        def v_lanes(kh):
            return slice(k_cols + kh * HEAD, k_cols + (kh + 1) * HEAD)

        which = []
        for half_at, _ in jobs:
            part_at = block * 2 + half_at
            late = part_at - (parts - edges)
            which.append(
                jnp.where(part_at < edges, 1 + part_at, jnp.where(late >= 0, 1 + edges + late, 0))
            )
        q = [stacked(0, *job) for job in jobs]
        do = [stacked(1, *job) for job in jobs]
        keys = [kvs[at(half_at), k_lanes(kh)] for half_at, kh in jobs]
        values = [kvs[at(half_at), v_lanes(kh)] for half_at, kh in jobs]
        scores = [contract_cols(q[i], keys[i]) for i in each]
        prob_grads = [contract_cols(do[i], values[i]) for i in each]
        scores = [scores[i] * (scaling * LOG2E) + bias[which[i]] for i in each]
        sink = []
        for _, kh in jobs:
            column = jnp.full((tall, 1), sink_ref[0, kh * group], f32)
            for g in range(1, group):
                column = jnp.where(head_at == g, sink_ref[0, kh * group + g], column)
            sink.append(column * LOG2E)
        top = [jnp.maximum(jnp.max(scores[i], axis=1, keepdims=True), sink[i]) for i in each]
        e = [jnp.exp2(scores[i] - top[i]) for i in each]
        sink_e = [jnp.exp2(sink[i] - top[i]) for i in each]
        inverse = [1.0 / (jnp.sum(e[i], axis=1, keepdims=True) + sink_e[i]) for i in each]
        p = [e[i] * inverse[i] for i in each]
        p_low = [p[i].astype(bf16) for i in each]
        attended = [dot_nn(p_low[i], values[i]).astype(bf16) for i in each]
        dots = [
            jnp.sum(do[i].astype(f32) * attended[i].astype(f32), axis=1, keepdims=True)
            for i in each
        ]
        dv = [contract_rows(p_low[i], do[i]) for i in each]
        ds = [(p[i] * (prob_grads[i] - dots[i])).astype(bf16) for i in each]
        dq = [(dot_nn(ds[i], keys[i]) * scaling).astype(bf16) for i in each]
        dk = [contract_rows(ds[i], q[i]) for i in each]
        lane_at = lax.broadcasted_iota(jnp.int32, (8, LANES), 1)
        sink_row = sinks[...]
        for i, (half_at, kh) in enumerate(jobs):
            span = slice(half_at * part_rows, (half_at + 1) * part_rows)
            sink_terms = sink_e[i] * inverse[i] * dots[i]
            for g in range(group):
                h = kh * group + g
                lanes, piece = slice(h * HEAD, (h + 1) * HEAD), slice(g * part_rows, (g + 1) * part_rows)
                att[block, span, lanes] = attended[i][piece]
                dqs[block, span, lanes] = dq[i][piece]
                total = jnp.sum(sink_terms[piece], axis=0, keepdims=True)
                sink_row = jnp.where(lane_at == h, sink_row - total, sink_row)
            dkv[at(half_at), k_lanes(kh)] += dk[i]
            dkv[at(half_at), v_lanes(kh)] += dv[i]
        sinks[...] = sink_row

    def cross_arrived(i, level):
        cross_copy(i, level * 2 + (1 - x)).wait_recv()

    def attend_own():
        cross_arrived(0, z)
        for way in range(2):

            @pl.when(z == (depth - 1) * way)
            def _():
                end_copy(way).start()

        for i in range(1, 3):
            cross_arrived(i, z)

        @pl.when((z == 0) | (z == depth - 1))
        def _():
            block = jnp.where(z == 0, 0, count - 1)
            attend_block(block)

    def attend(d, way, span=None):
        level, there = level_at(d, way)
        cross = level * 2 + (1 - x)
        extra = jnp.where(jnp.where(way == 0, level == 0, level == depth - 1), 1, 0)
        stop = 2 + extra
        nearest = jnp.where(way == 0, 2 * level + 2, 2 * level - 1)
        step = jnp.where(way == 0, -1, 1)
        inside = (x == way) | (extra == 1)
        key_at = jnp.where(x == way, 0, 1)

        def one(k, _):
            is_end = k == stop - 1
            block = nearest + step * k
            passed = jnp.where(way == 0, block <= cross, block >= cross)
            block = jnp.where(inside & passed, block + step, block)
            block = jnp.where(inside & is_end, cross, block)

            @pl.when((k == key_at) & (extra == 0))
            def _():
                cross_arrived(0, level)

            @pl.when(is_end)
            def _():
                cross_arrived(1, level)
                cross_arrived(2, level)

            attend_block(block)
            return 0

        begin, end = (0, stop) if span is None else span(stop)
        lax.fori_loop(begin, jnp.where(there, end, begin), one, 0)

    def attend_both(d):
        lax.fori_loop(0, 2, lambda k, _: attend(d, k) or 0, 0)

    pass_direct(is_home, straight)
    forward(0, 1)
    forward(1, 1)
    attend_own()
    forward(2, 1)
    forward_end(1)
    pass_direct(is_across, around)
    is_end = (z == 0) | (z == depth - 1)
    waits_late = jnp.logical_not(is_end) & ((2 * z < depth) == (y == 1))
    attend(1, 1 - y, lambda stop: (0, jnp.where(waits_late, stop - 1, 0)))
    forward(0, 2)
    forward(1, 2)
    attend(1, 1 - y, lambda stop: (jnp.where(waits_late, stop - 1, 0), stop))
    attend(1, y)
    forward(2, 2)
    forward_end(2)
    pass_second(is_across, straight)
    own_dkv = dkv[own_rows(s)]
    own_grads = jnp.concatenate(
        [
            dqs[s],
            (own_dkv[:, :k_cols] * scaling).astype(bf16),
            own_dkv[:, k_cols:].astype(bf16),
        ],
        axis=1,
    )

    def partial_for(slot):
        span = pl.ds(pl.multiple_of(slot * feats, feats), feats)
        return contract_cols(own_grads, w_in[span, :])

    rs_copies = [
        remote(part.at[i], rs_in.at[i], rs_send.at[i], rs_recv.at[i], s, peer)
        for i, peer in enumerate((partner, partner, across))
    ]
    part[0] = partial_for(diag).astype(bf16)
    rs_copies[0].start()
    acc[:, :feats] = partial_for(across)
    for d in range(3, depth):
        forward(0, d)
        forward(1, d)
    def weight_grads(begin, sources, first):
        last_arrivals(sources)
        blocks = pl.ds(begin, half)
        seq = pl.ds(pl.multiple_of(WINDOW + begin * rows, WINDOW), half * rows)

        def flat(value):
            return value.reshape(half * rows, value.shape[-1])

        left = flat(cols[0, blocks])
        pieces = (
            (go_ref, contract_rows(flat(att[blocks]), flat(cols[1, blocks]))),
            (gq_ref, contract_rows(left, flat(dqs[blocks]))),
            (gk_ref, contract_rows(left, (dkv[seq, :k_cols] * scaling).astype(bf16))),
            (gv_ref, contract_rows(left, dkv[seq, k_cols:].astype(bf16))),
        )
        for ref, value in pieces:
            ref[...] = value if first else ref[...] + value

    @pl.when(jnp.logical_not(is_end) & (core == 1))
    def _():
        weight_grads(here_half, near, True)

    rs_copies[0].wait_recv()
    part[2] = (acc[:, :feats] + rs_in[0].astype(f32)).astype(bf16)
    rs_copies[2].start()
    part[1] = partial_for(partner).astype(bf16)
    rs_copies[1].start()
    acc[:, :feats] = partial_for(t)

    @pl.when(jnp.logical_not(is_end) & (core == 0))
    def _():
        weight_grads(here_half, near, True)

    attend_both(2)
    for d in range(3, depth):
        forward(2, d)
        forward_end(d)
    pass_second(is_home, around)
    @pl.when(is_end)
    def _():
        weight_grads(here_half, near, True)

    for d in range(3, depth):
        attend_both(d)
    weight_grads(half - here_half, far, False)
    sg_ref[...] = sinks[...]
    for copy in rs_copies[1:]:
        copy.wait_recv()
    ig_ref[...] = (
        acc[:, :feats] + rs_in[1].astype(f32) + rs_in[2].astype(f32)
    ).astype(bf16)

    for copy in to_across + to_partner + relay + rs_copies:
        copy.wait_send()
    for kind in range(3):
        each_column(kind, lambda copy: copy.wait_send())
    for here, items in ((is_home, straight), (is_across, around)):

        @pl.when(here)
        def _():
            for source, a in items:
                y_copy(a, source).wait_send()

    @pl.when(jnp.logical_not(is_last))
    def _():
        for source in near + far:
            for a in range(2):
                chip_copy(a, source).wait_send()

    for way in range(2):

        @pl.when(goes_on(way))
        def _():
            end_copy(way).wait_send()

    for i in range(3):
        for level in range(depth):
            block = level * 2 + x
            for way in range(2):
                came = jnp.where(way == 0, level <= z, level >= z)

                @pl.when(came & goes_on(way))
                def _():
                    z_copy(i, block, way).wait_send()

            @pl.when(crosses(i, level))
            def _():
                cross_copy(i, block).wait_send()


def store_kernel(*refs):
    ins, sink_in, outs, sink_out, sem = refs[:5], refs[5], refs[6:11], refs[11], refs[12]
    stores = [pltpu.make_async_copy(ins[i], outs[i], sem.at[i]) for i in range(5)]
    for store in stores:
        store.start()
    sink_out[...] = sink_in[0:1, : sink_out.shape[1]]
    for store in stores:
        store.wait()


def fused_device(
    layer_input, output_grad, query_weight, key_weight, value_weight, out_weight, sink_logit
):
    bf16, f32 = jnp.bfloat16, jnp.float32
    count, tps = lax.axis_size("sp"), lax.axis_size("tp")
    rows, feats = layer_input.shape
    width = query_weight.shape[0]
    q_cols, k_cols = query_weight.shape[1], key_weight.shape[1]
    block_cols = width // count
    vmem = pl.BlockSpec(memory_space=pltpu.VMEM)
    hbm = pl.BlockSpec(memory_space=pltpu.HBM)
    dma = pltpu.SemaphoreType.DMA
    outs = pl.pallas_call(
        layer_kernel,
        out_shape=(
            jax.ShapeDtypeStruct((rows, feats), bf16),
            jax.ShapeDtypeStruct((block_cols, q_cols), f32),
            jax.ShapeDtypeStruct((block_cols, k_cols), f32),
            jax.ShapeDtypeStruct((block_cols, k_cols), f32),
            jax.ShapeDtypeStruct((q_cols, block_cols), f32),
            jax.ShapeDtypeStruct((8, LANES), f32),
        ),
        in_specs=[hbm] * 7,
        out_specs=(vmem,) * 6,
        scratch_shapes=[
            pltpu.VMEM((width, q_cols + 2 * k_cols), bf16),
            pltpu.VMEM(out_weight.shape, bf16),
            pltpu.VMEM((tps, 2, rows, feats), bf16),
            pltpu.VMEM((rows, 2 * q_cols + 2 * k_cols), f32),
            pltpu.VMEM((count * rows + 2 * WINDOW, 2 * k_cols), bf16),
            pltpu.VMEM((2, count, rows, q_cols), bf16),
            pltpu.VMEM((count, rows, q_cols), bf16),
            pltpu.VMEM((count, rows, q_cols), bf16),
            pltpu.VMEM((count * rows + 2 * WINDOW, 2 * k_cols), f32),
            pltpu.VMEM((2, count, rows, block_cols), bf16),
            pltpu.VMEM((1 + 2 * (-(-2 * WINDOW // rows)), q_cols // k_cols * rows // 2, rows // 2 + 2 * WINDOW), f32),
            pltpu.VMEM((8, LANES), f32),
            pltpu.VMEM((3, rows, feats), bf16),
            pltpu.VMEM((3, rows, feats), bf16),
            pltpu.SMEM((1, sink_logit.shape[0]), f32),
            dma((7,)), dma((3, 2)), dma((3, 2)),
            dma((3, feats // block_cols)), dma((2, count)),
            dma((2, count)), dma((2, count)), dma((2, count)), dma((2, count)),
            dma((2, 3, count)), dma((3, count)), dma((3, count)), dma((3,)), dma((3,)),
        ],
        compiler_params=pltpu.CompilerParams(
            collective_id=0, has_side_effects=True, vmem_limit_bytes=VMEM_BYTES
        ),
        name="layer",
    )(
        *(
            pltpu.with_memory_space_constraint(array, pltpu.HBM)
            for array in (
                layer_input, output_grad, query_weight, key_weight, value_weight, out_weight,
                sink_logit.reshape(1, -1),
            )
        ),
    )
    kept = [jax.ShapeDtypeStruct(out.shape, out.dtype) for out in outs[:5]]
    stored = pl.pallas_call(
        store_kernel,
        out_shape=(*kept, jax.ShapeDtypeStruct((1, sink_logit.shape[0]), f32)),
        in_specs=[vmem] * 6,
        out_specs=(hbm,) * 5 + (vmem,),
        scratch_shapes=[dma((5,))],
        compiler_params=pltpu.CompilerParams(vmem_limit_bytes=STORE_BYTES),
        name="store",
    )(*outs)
    return tuple(stored[:5]) + (stored[5].reshape(-1),)


def fits_kernel(mesh, layer_width):
    count, tps = mesh.shape["sp"], mesh.shape["tp"]
    return tps == 4 and count == 8 and layer_width == count * tps * LANES and HEADS == 2 * KV_HEADS


def solution(mesh):
    placed = (
        P("sp", "tp"),
        P("sp", "tp"),
        P(None, "tp"),
        P(None, "tp"),
        P(None, "tp"),
        P("tp", None),
        P("tp"),
    )

    def sharded(*arrays):
        width = arrays[0].shape[1]
        body = fused_device if fits_kernel(mesh, width) else per_device
        return jax.shard_map(
            body,
            mesh=mesh,
            in_specs=placed,
            out_specs=(
                P("sp", "tp"),
                P("sp", "tp"),
                P("sp", "tp"),
                P("sp", "tp"),
                P("tp", "sp"),
                P("tp"),
            ),
            check_vma=False,
        )(*arrays)

    return sharded
```

```python
import functools

import jax
import jax.numpy as jnp
from jax import lax
from jax.experimental import pallas as pl
from jax.experimental.pallas import tpu as pltpu
from jax.sharding import PartitionSpec as P

HEADS = 16
KV_HEADS = 8
HEAD = 128
WINDOW = 128


masked_score = -1e30


def extended(cells, sides, width):
    for axis, dim in sides:
        count = lax.axis_size(axis)
        ends = count - 1
        head = lax.slice_in_dim(cells, 0, width, axis=dim)
        tail = lax.slice_in_dim(cells, cells.shape[dim] - width, cells.shape[dim], axis=dim)
        cells = jnp.concatenate(
            [
                lax.ppermute(tail, axis, [(i, (i + 1) % count) for i in range(ends)]),
                cells,
                lax.ppermute(head, axis, [((i + 1) % count, i) for i in range(ends)]),
            ],
            axis=dim,
        )
    return cells


def passed_along(value, axis, steps):
    count = lax.axis_size(axis)
    initial, last = (max(0, -steps), min(count, count - steps))
    return lax.ppermute(value, axis, [(source, source + steps) for source in range(initial, last)])


def contract_rows(left, right):
    return lax.dot_general(
        left, right, (((0,), (0,)), ((), ())), preferred_element_type=jnp.float32
    )


def contract_cols(left, right):
    return lax.dot_general(
        left, right, (((1,), (1,)), ((), ())), preferred_element_type=jnp.float32
    )


def per_device(
    layer_input, output_grad, query_weight, key_weight, value_weight, out_weight, sink_logit
):
    whole_input, whole_grad = (
        lax.all_gather(layer_input, "tp", axis=1, tiled=True),
        lax.all_gather(output_grad, "tp", axis=1, tiled=True),
    )
    tok_rows = whole_input.shape[0]
    query_cols = query_weight.shape[1]
    key_cols = key_weight.shape[1]
    key_heads = key_cols // HEAD
    group_size = HEADS // KV_HEADS
    scaling = HEAD ** (-0.5)
    queries = jnp.dot(whole_input, query_weight, preferred_element_type=jnp.float32).astype(
        jnp.bfloat16
    )
    key_rows = jnp.dot(whole_input, key_weight, preferred_element_type=jnp.float32).astype(
        jnp.bfloat16
    )
    value_rows = jnp.dot(whole_input, value_weight, preferred_element_type=jnp.float32).astype(
        jnp.bfloat16
    )
    out_rows_grad = contract_cols(whole_grad, out_weight).astype(jnp.bfloat16)
    joined = jnp.concatenate([key_rows, value_rows], axis=1)
    band = extended(joined, (("sp", 0),), WINDOW)
    band_rows = band.shape[0]
    band_keys = band[:, :key_cols].reshape(band_rows, key_heads, HEAD)
    band_values = band[:, key_cols:].reshape(band_rows, key_heads, HEAD)
    shard_index = lax.axis_index("sp")
    seq_total = tok_rows * lax.axis_size("sp")
    query_pos = shard_index * tok_rows + jnp.arange(tok_rows, dtype=jnp.int32)
    key_pos = shard_index * tok_rows - WINDOW + jnp.arange(band_rows, dtype=jnp.int32)
    in_window = (
        (jnp.abs(query_pos[:, None] - key_pos[None, :]) <= WINDOW)
        & (key_pos[None, :] >= 0)
        & (key_pos[None, :] < seq_total)
    )
    query_heads = queries.reshape(tok_rows, key_heads, group_size, HEAD)
    grad_heads = out_rows_grad.reshape(tok_rows, key_heads, group_size, HEAD)
    scores = (
        jnp.einsum("qkgd,skd->kgqs", query_heads, band_keys, preferred_element_type=jnp.float32)
        * scaling
    )
    scores = jnp.where(in_window[None, None], scores, masked_score)
    sink_column = sink_logit.reshape(key_heads, group_size)[:, :, None]
    row_max = jnp.maximum(jnp.max(scores, axis=-1), sink_column)
    row_total = jnp.sum(jnp.exp(scores - row_max[..., None]), axis=-1) + jnp.exp(
        sink_column - row_max
    )
    log_total = row_max + jnp.log(row_total)
    soft_weights = jnp.exp(scores - log_total[..., None])
    soft_rounded = soft_weights.astype(jnp.bfloat16)
    attended = jnp.einsum(
        "kgqs,skd->qkgd", soft_rounded, band_values, preferred_element_type=jnp.float32
    ).astype(jnp.bfloat16)
    row_dots = jnp.sum(
        grad_heads.astype(jnp.float32) * attended.astype(jnp.float32), axis=-1
    ).transpose(1, 2, 0)
    prob_grads = jnp.einsum(
        "qkgd,skd->kgqs", grad_heads, band_values, preferred_element_type=jnp.float32
    )
    score_grads = (soft_weights * (prob_grads - row_dots[..., None])).astype(jnp.bfloat16)
    query_grads = (
        jnp.einsum("kgqs,skd->qkgd", score_grads, band_keys, preferred_element_type=jnp.float32)
        * scaling
    )
    query_grads = query_grads.astype(jnp.bfloat16).reshape(tok_rows, query_cols)
    band_key_grads = (
        jnp.einsum("kgqs,qkgd->skd", score_grads, query_heads, preferred_element_type=jnp.float32)
        * scaling
    )
    band_value_grads = jnp.einsum(
        "kgqs,qkgd->skd", soft_rounded, grad_heads, preferred_element_type=jnp.float32
    )
    band_grads = jnp.concatenate(
        [
            band_key_grads.reshape(band_rows, key_cols),
            band_value_grads.reshape(band_rows, key_cols),
        ],
        axis=1,
    )
    sink_part = -jnp.sum(jnp.exp(sink_column - log_total) * row_dots, axis=-1).reshape(-1)
    sink_grad = lax.psum(sink_part, "sp")
    attended_rows = attended.reshape(tok_rows, query_cols)
    input_block = lax.all_to_all(whole_input, "sp", 1, 0, tiled=True)
    grad_block = lax.all_to_all(whole_grad, "sp", 1, 0, tiled=True)
    early_rows = lax.all_gather(
        jnp.concatenate([query_grads, attended_rows], axis=1), "sp", axis=0, tiled=True
    )
    query_part = contract_rows(input_block, early_rows[:, :query_cols])
    out_part = contract_rows(early_rows[:, query_cols:], grad_block)
    returned_low = passed_along(band_grads[:WINDOW].astype(jnp.bfloat16), "sp", -1).astype(
        jnp.float32
    )
    returned_high = passed_along(
        band_grads[band_rows - WINDOW :].astype(jnp.bfloat16), "sp", 1
    ).astype(jnp.float32)
    own_rows = band_grads[WINDOW : WINDOW + tok_rows]
    own_rows = own_rows.at[tok_rows - WINDOW :].add(returned_low)
    own_rows = own_rows.at[:WINDOW].add(returned_high)
    key_grads = own_rows[:, :key_cols].astype(jnp.bfloat16)
    value_grads = own_rows[:, key_cols:].astype(jnp.bfloat16)
    late_rows = lax.all_gather(
        jnp.concatenate([key_grads, value_grads], axis=1), "sp", axis=0, tiled=True
    )
    key_part = contract_rows(input_block, late_rows[:, :key_cols])
    value_part = contract_rows(input_block, late_rows[:, key_cols:])
    partials = (
        contract_cols(query_grads, query_weight)
        + contract_cols(key_grads, key_weight)
        + contract_cols(value_grads, value_weight)
    )
    input_grad = lax.psum_scatter(
        partials.astype(jnp.bfloat16), "tp", scatter_dimension=1, tiled=True
    )
    return (input_grad, query_part, key_part, value_part, out_part, sink_grad)


LANES = 128
LOG2E = 1.4426950408889634
MESH = pl.DeviceIdType.MESH
VMEM_BYTES = 46 * 1024 * 1024
STORE_BYTES = 8 * 1024 * 1024


def dot_nn(a, b):
    return jnp.dot(a, b, preferred_element_type=jnp.float32)


def layer_kernel(
    x_hbm, g_hbm, wq_hbm, wk_hbm, wv_hbm, wo_hbm, sink_hbm,
    ig_ref, gq_ref, gk_ref, gv_ref, go_ref, sg_ref,
    w_in, wo, xg, acc, kvs, acts, att, dqs, dkv, cols, bias, sinks, part, rs_in, sink_ref,
    w_sem, ag_send, ag_recv, col_send, col_recv, y_send, chip_send,
    z_sem, cross_sem, end_sem, acts_recv, rs_send, rs_recv,
):
    bf16, f32 = jnp.bfloat16, jnp.float32
    count, tps = lax.axis_size("sp"), lax.axis_size("tp")
    depth = count // 2
    s, t = lax.axis_index("sp"), lax.axis_index("tp")
    z, x = s // 2, s % 2
    y, core = t // 2, t % 2
    partner = y * 2 + (1 - core)
    across = (1 - y) * 2 + core
    diag = (1 - y) * 2 + (1 - core)
    rows, feats = x_hbm.shape
    q_cols, k_cols = wq_hbm.shape[1], wk_hbm.shape[1]
    in_cols = q_cols + 2 * k_cols
    block_cols = gq_ref.shape[0]
    per_slot = feats // block_cols
    key_heads = k_cols // HEAD
    group = q_cols // k_cols
    scaling = HEAD**-0.5

    def remote(src, dst, send, recv, dev_s, dev_t):
        return pltpu.make_async_remote_copy(
            src_ref=src, dst_ref=dst, send_sem=send, recv_sem=recv,
            device_id=(dev_s, dev_t), device_id_type=MESH,
        )

    own = [
        pltpu.make_async_copy(src, xg.at[t, a], w_sem.at[3 + a])
        for a, src in enumerate((x_hbm, g_hbm))
    ]
    for copy in own:
        copy.start()
    weights, at = [], 0
    for src in (wq_hbm, wk_hbm, wv_hbm):
        span = pl.ds(at, src.shape[1])
        weights.append(pltpu.make_async_copy(src, w_in.at[:, span], w_sem.at[0]))
        at += src.shape[1]
    weights.append(pltpu.make_async_copy(wo_hbm, wo, w_sem.at[1]))
    weights.append(pltpu.make_async_copy(sink_hbm, sink_ref, w_sem.at[2]))
    for copy in weights:
        copy.start()

    barrier = pltpu.get_barrier_semaphore()
    for peer in (partner, across, diag):
        pl.semaphore_signal(barrier, inc=1, device_id=(s, peer), device_id_type=MESH)
    for d in range(1, count):
        pl.semaphore_signal(
            barrier, inc=1, device_id=((s + d) % count, t), device_id_type=MESH
        )
    pl.semaphore_wait(barrier, 3 + count - 1)

    sources = (xg.at[t, 0], xg.at[t, 1])
    for copy in own:
        copy.wait()
    to_across = [
        remote(sources[a], xg.at[t, a], ag_send.at[0], ag_recv.at[0, a], s, across)
        for a in range(2)
    ]
    to_partner = [
        remote(sources[a], xg.at[t, a], ag_send.at[1], ag_recv.at[1, a], s, partner)
        for a in range(2)
    ]
    relay = [
        remote(xg.at[across, a], xg.at[across, a], ag_send.at[2], ag_recv.at[2, a], s, partner)
        for a in range(2)
    ]
    for copy in to_across + to_partner:
        copy.start()

    is_home = s // per_slot == t
    is_across = s // per_slot == across
    is_last = jnp.logical_not(is_home | is_across)

    half = count // 2
    here_half = s // half * half
    near = [here_half + i for i in range(half)]
    far = [half - here_half + i for i in range(half)]
    sends_near = s // half == t * per_slot // half

    def column_copy(kind, b):
        a, slot = kind % 2, t if kind else across
        return remote(
            xg.at[slot, a, :, pl.ds(b * block_cols, block_cols)], cols.at[a, s],
            col_send.at[kind, b], col_recv.at[a, s], slot * per_slot + b, t,
        )

    def column_arrival(a, source):
        ref = cols.at[a, source]
        return remote(ref, ref, col_send.at[a, 0], col_recv.at[a, source], (s + 1) % count, t)

    def y_copy(a, source):
        ref = cols.at[a, source]
        return remote(ref, ref, y_send.at[a], col_recv.at[a, source], s, across)

    def chip_copy(a, source):
        ref = cols.at[a, source]
        return remote(ref, ref, chip_send.at[0], col_recv.at[a, source], s, partner)

    def each_column(kind, act, which=None):
        slot = t if kind else across
        for b in range(per_slot) if which is None else which:
            sent = slot * per_slot + b != s

            @pl.when(sent if kind == 1 else sent & sends_near)
            def _():
                act(column_copy(kind, b))

    def send_columns(kind, which=None):
        each_column(kind, lambda copy: copy.start(), which)

    send_columns(1)
    send_columns(2)

    def project_input(slot, first=False):
        cells = xg[slot, 0]
        span = pl.ds(pl.multiple_of(slot * feats, feats), feats)
        term = dot_nn(cells, w_in[span, :])
        acc[:, :in_cols] = term if first else acc[:, :in_cols] + term

    def project_grad(slot, first=False):
        cells = xg[slot, 1]
        span = pl.ds(pl.multiple_of(slot * feats, feats), feats)
        term = contract_cols(cells, wo[:, span])
        acc[:, in_cols:] = term if first else acc[:, in_cols:] + term

    for edge in (0, WINDOW + count * rows):
        kvs[edge : edge + WINDOW] = jnp.zeros((WINDOW, 2 * k_cols), bf16)
    dkv[...] = jnp.zeros_like(dkv)
    sinks[...] = jnp.zeros_like(sinks)
    part_rows = rows // 2
    part_keys = part_rows + 2 * WINDOW
    tall = group * part_rows
    edges = -(-WINDOW // part_rows)
    parts = rows * count // part_rows
    q_at = lax.rem(lax.broadcasted_iota(jnp.int32, (tall, part_keys), 0), part_rows)
    k_at = lax.broadcasted_iota(jnp.int32, (tall, part_keys), 1)
    band = (k_at >= q_at) & (k_at - q_at <= 2 * WINDOW)
    starts = [edges] + list(range(edges)) + [parts - edges + i for i in range(edges)]
    for i, start in enumerate(starts):
        pos = k_at + (start * part_rows - WINDOW)
        inside = band & (pos >= 0) & (pos < rows * count) if i else band
        bias[i] = jnp.where(inside, 0.0, masked_score)

    pltpu.make_async_copy(w_in, w_in, w_sem.at[0]).wait()
    for copy in weights[3:]:
        copy.wait()
    project_input(t, True)
    project_grad(t, True)
    to_partner[0].wait_recv()
    project_input(partner)
    to_partner[1].wait_recv()
    project_grad(partner)
    to_across[0].wait_recv()
    relay[0].start()
    send_columns(0, (0,))
    project_input(across)
    relay[0].wait_recv()
    project_input(diag)
    for b in range(per_slot):
        span = slice(b * block_cols, (b + 1) * block_cols)

        @pl.when(t * per_slot + b == s)
        def _():
            for a in range(2):
                cols[a, s] = xg[t, a, :, span]


    def own_rows(block):
        return pl.ds(pl.multiple_of(WINDOW + block * rows, 32), rows)

    def item(i, block):
        return acts.at[i - 1, block] if i else kvs.at[own_rows(block)]

    def z_copy(i, block, way):
        dev = (z + 1 - 2 * way + depth) % depth * 2 + x
        ref = item(i, block)
        return remote(ref, ref, z_sem.at[way, block // 2], acts_recv.at[i, block], dev, t)

    def cross_copy(i, block):
        ref = item(i, block)
        return remote(
            ref, ref, cross_sem.at[block // 2], acts_recv.at[i, block], z * 2 + (1 - x), t
        )

    def goes_on(way):
        return jnp.where(way == 0, z < depth - 1, z > 0)

    def send_own(i):
        cross_copy(i, s).start()
        for way in range(2):

            @pl.when(goes_on(way))
            def _():
                z_copy(i, s, way).start()

    def level_at(d, way):
        level = z - d * (1 - 2 * way)
        return level, (level >= 0) & (level < depth)

    def crosses(i, level):
        return (i < 2) | ((level > 0) & (level < depth - 1)) | (level == z)

    def end_copy(way):
        block = (depth - 1) * way * 2 + (1 - x)
        dev = (z + 1 - 2 * way + depth) % depth * 2 + x
        ref = item(2, block)
        return remote(ref, ref, end_sem.at[way], acts_recv.at[2, block], dev, t)

    def forward_end(d, allowed=True):
        for way in range(2):
            level, there = level_at(d, way)
            there = there & allowed

            @pl.when(there & (level == (depth - 1) * way))
            def _():
                end_copy(way).wait_recv()

                @pl.when(goes_on(way))
                def _():
                    end_copy(way).start()

    def forward_way(i, d, way, allowed=True):
        level, there = level_at(d, way)

        @pl.when(there & allowed)
        def _():
            block = level * 2 + x
            z_copy(i, block, way).wait_recv()

            @pl.when(crosses(i, level))
            def _():
                cross_copy(i, block).start()

            @pl.when(goes_on(way))
            def _():
                z_copy(i, block, way).start()

    early, late = 1 - y, y

    def forward(i, d, allowed=True):
        forward_way(i, d, early, allowed)
        forward_way(i, d, late, allowed)

    kvs[own_rows(s)] = acc[:, q_cols:in_cols].astype(bf16)
    send_own(0)
    acts[0, s] = acc[:, :q_cols].astype(bf16)
    send_own(1)
    send_columns(0, (1,))

    to_across[1].wait_recv()
    relay[1].start()
    project_grad(across)
    relay[1].wait_recv()
    project_grad(diag)
    acts[1, s] = acc[:, in_cols:].astype(bf16)
    send_own(2)

    straight = [(source, a) for source in near for a in range(2)] + [(source, 1) for source in far]
    around = [(source, 0) for source in far]

    def pass_direct(here, items):
        @pl.when(here)
        def _():
            for source, a in items:

                @pl.when(source != s)
                def _():
                    column_arrival(a, source).wait_recv()

                y_copy(a, source).start()
                chip_copy(a, source).start()

    def pass_second(here, items):
        @pl.when(here)
        def _():
            for source, a in items:
                y_copy(a, source).wait_recv()
                chip_copy(a, source).start()

    def last_arrivals(sources):
        @pl.when(is_last)
        def _():
            for source in sources:
                for a in range(2):
                    chip_copy(a, source).wait_recv()

    def attend_block(block):
        jobs = [(half_at, kh) for half_at in range(2) for kh in range(key_heads)]
        each = range(len(jobs))
        head_at = lax.broadcasted_iota(jnp.int32, (tall, 1), 0) // part_rows

        def at(half_at):
            start = block * rows + half_at * part_rows
            return pl.ds(pl.multiple_of(start, 16), part_keys)

        def stacked(i, half_at, kh):
            span = slice(half_at * part_rows, (half_at + 1) * part_rows)
            heads = [kh * group + g for g in range(group)]
            return jnp.concatenate(
                [acts[i, block, span, h * HEAD : (h + 1) * HEAD] for h in heads], axis=0
            )

        def k_lanes(kh):
            return slice(kh * HEAD, (kh + 1) * HEAD)

        def v_lanes(kh):
            return slice(k_cols + kh * HEAD, k_cols + (kh + 1) * HEAD)

        which = []
        for half_at, _ in jobs:
            part_at = block * 2 + half_at
            late = part_at - (parts - edges)
            which.append(
                jnp.where(part_at < edges, 1 + part_at, jnp.where(late >= 0, 1 + edges + late, 0))
            )
        q = [stacked(0, *job) for job in jobs]
        do = [stacked(1, *job) for job in jobs]
        keys = [kvs[at(half_at), k_lanes(kh)] for half_at, kh in jobs]
        values = [kvs[at(half_at), v_lanes(kh)] for half_at, kh in jobs]
        scores = [contract_cols(q[i], keys[i]) for i in each]
        prob_grads = [contract_cols(do[i], values[i]) for i in each]
        scores = [scores[i] * (scaling * LOG2E) + bias[which[i]] for i in each]
        sink = []
        for _, kh in jobs:
            column = jnp.full((tall, 1), sink_ref[0, kh * group], f32)
            for g in range(1, group):
                column = jnp.where(head_at == g, sink_ref[0, kh * group + g], column)
            sink.append(column * LOG2E)
        top = [jnp.maximum(jnp.max(scores[i], axis=1, keepdims=True), sink[i]) for i in each]
        e = [jnp.exp2(scores[i] - top[i]) for i in each]
        sink_e = [jnp.exp2(sink[i] - top[i]) for i in each]
        inverse = [1.0 / (jnp.sum(e[i], axis=1, keepdims=True) + sink_e[i]) for i in each]
        p = [e[i] * inverse[i] for i in each]
        p_low = [p[i].astype(bf16) for i in each]
        attended = [dot_nn(p_low[i], values[i]).astype(bf16) for i in each]
        dots = [
            jnp.sum(do[i].astype(f32) * attended[i].astype(f32), axis=1, keepdims=True)
            for i in each
        ]
        dv = [contract_rows(p_low[i], do[i]) for i in each]
        ds = [(p[i] * (prob_grads[i] - dots[i])).astype(bf16) for i in each]
        dq = [(dot_nn(ds[i], keys[i]) * scaling).astype(bf16) for i in each]
        dk = [contract_rows(ds[i], q[i]) for i in each]
        lane_at = lax.broadcasted_iota(jnp.int32, (8, LANES), 1)
        sink_row = sinks[...]
        for i, (half_at, kh) in enumerate(jobs):
            span = slice(half_at * part_rows, (half_at + 1) * part_rows)
            sink_terms = sink_e[i] * inverse[i] * dots[i]
            for g in range(group):
                h = kh * group + g
                lanes, piece = slice(h * HEAD, (h + 1) * HEAD), slice(g * part_rows, (g + 1) * part_rows)
                att[block, span, lanes] = attended[i][piece]
                dqs[block, span, lanes] = dq[i][piece]
                total = jnp.sum(sink_terms[piece], axis=0, keepdims=True)
                sink_row = jnp.where(lane_at == h, sink_row - total, sink_row)
            dkv[at(half_at), k_lanes(kh)] += dk[i]
            dkv[at(half_at), v_lanes(kh)] += dv[i]
        sinks[...] = sink_row

    def cross_arrived(i, level):
        cross_copy(i, level * 2 + (1 - x)).wait_recv()

    def attend_own():
        for i in range(3):
            cross_arrived(i, z)
        for way in range(2):

            @pl.when(z == (depth - 1) * way)
            def _():
                end_copy(way).start()

        @pl.when((z == 0) | (z == depth - 1))
        def _():
            block = jnp.where(z == 0, 0, count - 1)
            attend_block(block)

    def attend(d, way, span=None):
        level, there = level_at(d, way)
        cross = level * 2 + (1 - x)
        extra = jnp.where(jnp.where(way == 0, level == 0, level == depth - 1), 1, 0)
        stop = 2 + extra
        nearest = jnp.where(way == 0, 2 * level + 2, 2 * level - 1)
        step = jnp.where(way == 0, -1, 1)
        inside = (x == way) | (extra == 1)
        key_at = jnp.where(x == way, 0, 1)

        def one(k, _):
            is_end = k == stop - 1
            block = nearest + step * k
            passed = jnp.where(way == 0, block <= cross, block >= cross)
            block = jnp.where(inside & passed, block + step, block)
            block = jnp.where(inside & is_end, cross, block)

            @pl.when(k == key_at)
            def _():
                cross_arrived(0, level)

            @pl.when(is_end)
            def _():
                cross_arrived(1, level)

            @pl.when(is_end & (extra == 0))
            def _():
                cross_arrived(2, level)

            attend_block(block)
            return 0

        begin, end = (0, stop) if span is None else span(stop)
        lax.fori_loop(begin, jnp.where(there, end, begin), one, 0)

    def attend_both(d, span=None):
        def one(way, _):
            attend(d, way, None if span is None else functools.partial(span, way))
            return 0

        lax.fori_loop(0, 2, one, 0)

    is_end = (z == 0) | (z == depth - 1)
    is_mid = jnp.logical_not(is_end)
    waits_late = is_mid & ((2 * z < depth) == (y == 1))
    waits_little = is_mid & jnp.logical_not(waits_late)
    pass_direct(is_home, straight)
    forward_way(0, 1, early)
    forward_way(1, 1, early)
    forward_way(0, 1, late)
    forward_way(2, 1, early, is_mid)
    forward_way(1, 1, late)
    attend_own()
    forward_way(2, 1, early, is_end)
    forward_way(2, 1, late)
    forward_end(1)
    pass_direct(is_across, around)
    attend(1, 1 - y, lambda stop: (0, jnp.where(waits_late, stop - 1, 0)))
    forward(0, 2)
    forward(1, 2)
    forward(2, 2, waits_little)
    forward_end(2, waits_little)
    attend(1, 1 - y, lambda stop: (jnp.where(waits_late, stop - 1, 0), stop))
    pass_second(is_across, straight)
    attend(1, y)
    forward(2, 2, jnp.logical_not(waits_little))
    forward_end(2, jnp.logical_not(waits_little))
    own_dkv = dkv[own_rows(s)]
    own_grads = jnp.concatenate(
        [
            dqs[s],
            (own_dkv[:, :k_cols] * scaling).astype(bf16),
            own_dkv[:, k_cols:].astype(bf16),
        ],
        axis=1,
    )

    def partial_for(slot):
        span = pl.ds(pl.multiple_of(slot * feats, feats), feats)
        return contract_cols(own_grads, w_in[span, :])

    rs_copies = [
        remote(part.at[i], rs_in.at[i], rs_send.at[i], rs_recv.at[i], s, peer)
        for i, peer in enumerate((partner, partner, across))
    ]
    part[0] = partial_for(diag).astype(bf16)
    rs_copies[0].start()
    acc[:, :feats] = partial_for(across)
    def weight_grads(begin, sources, first):
        last_arrivals(sources)
        blocks = pl.ds(begin, half)
        seq = pl.ds(pl.multiple_of(WINDOW + begin * rows, WINDOW), half * rows)

        def flat(value):
            return value.reshape(half * rows, value.shape[-1])

        left = flat(cols[0, blocks])
        pieces = (
            (go_ref, contract_rows(flat(att[blocks]), flat(cols[1, blocks]))),
            (gq_ref, contract_rows(left, flat(dqs[blocks]))),
            (gk_ref, contract_rows(left, (dkv[seq, :k_cols] * scaling).astype(bf16))),
            (gv_ref, contract_rows(left, dkv[seq, k_cols:].astype(bf16))),
        )
        for ref, value in pieces:
            ref[...] = value if first else ref[...] + value

    @pl.when(jnp.logical_not(is_end) & (core == 1))
    def _():
        weight_grads(here_half, near, True)

    rs_copies[0].wait_recv()
    part[2] = (acc[:, :feats] + rs_in[0].astype(f32)).astype(bf16)
    rs_copies[2].start()
    part[1] = partial_for(partner).astype(bf16)
    rs_copies[1].start()
    acc[:, :feats] = partial_for(t)

    @pl.when(jnp.logical_not(is_end) & (core == 0))
    def _():
        weight_grads(here_half, near, True)

    for d in range(3, depth):
        forward(0, d)
        forward(1, d)
    attend_both(2)
    @pl.when(is_end)
    def _():
        weight_grads(here_half, near, True)

    for d in range(3, depth):
        attend_both(d, lambda way, stop: (0, 1))
    for d in range(3, depth):
        forward(2, d)
        forward_end(d)
    pass_second(is_home, around)
    for d in range(3, depth):
        attend_both(d, lambda way, stop: (1, stop))
    weight_grads(half - here_half, far, False)
    sg_ref[...] = sinks[...]
    for copy in rs_copies[1:]:
        copy.wait_recv()
    ig_ref[...] = (
        acc[:, :feats] + rs_in[1].astype(f32) + rs_in[2].astype(f32)
    ).astype(bf16)

    def sent(ref, sem):
        remote(ref, ref, sem, rs_recv.at[0], (s + 1) % count, t).wait_send()

    for i in range(3):
        sent(xg.at[t], ag_send.at[i])
    for copy in rs_copies:
        copy.wait_send()
    for kind in range(3):
        each_column(kind, lambda copy: copy.wait_send())

    @pl.when(is_home)
    def _():
        sent(cols.at[0, pl.ds(here_half, half)], y_send.at[0])
        sent(cols.at[1], y_send.at[1])

    @pl.when(is_across)
    def _():
        sent(cols.at[0, pl.ds(half - here_half, half)], y_send.at[0])

    @pl.when(jnp.logical_not(is_last))
    def _():
        sent(cols, chip_send.at[0])

    for level in range(depth):
        for way in range(2):
            came = jnp.where(way == 0, level <= z, level >= z)

            @pl.when(came & goes_on(way))
            def _():
                sent(acts.at[0, pl.ds(0, 3)], z_sem.at[way, level])

        all_cross = crosses(2, level)

        @pl.when(all_cross)
        def _():
            sent(acts.at[0, pl.ds(0, 3)], cross_sem.at[level])

        @pl.when(jnp.logical_not(all_cross))
        def _():
            sent(acts.at[0, pl.ds(0, 2)], cross_sem.at[level])

    for way in range(2):

        @pl.when(goes_on(way))
        def _():
            end_copy(way).wait_send()


def store_kernel(*refs):
    ins, sink_in, outs, sink_out, sem = refs[:5], refs[5], refs[6:11], refs[11], refs[12]
    stores = [pltpu.make_async_copy(ins[i], outs[i], sem.at[i]) for i in range(5)]
    for store in stores:
        store.start()
    sink_out[...] = sink_in[0:1, : sink_out.shape[1]]
    for store in stores:
        store.wait()


def fused_device(
    layer_input, output_grad, query_weight, key_weight, value_weight, out_weight, sink_logit
):
    bf16, f32 = jnp.bfloat16, jnp.float32
    count, tps = lax.axis_size("sp"), lax.axis_size("tp")
    rows, feats = layer_input.shape
    width = query_weight.shape[0]
    q_cols, k_cols = query_weight.shape[1], key_weight.shape[1]
    block_cols = width // count
    vmem = pl.BlockSpec(memory_space=pltpu.VMEM)
    hbm = pl.BlockSpec(memory_space=pltpu.HBM)
    dma = pltpu.SemaphoreType.DMA
    outs = pl.pallas_call(
        layer_kernel,
        out_shape=(
            jax.ShapeDtypeStruct((rows, feats), bf16),
            jax.ShapeDtypeStruct((block_cols, q_cols), f32),
            jax.ShapeDtypeStruct((block_cols, k_cols), f32),
            jax.ShapeDtypeStruct((block_cols, k_cols), f32),
            jax.ShapeDtypeStruct((q_cols, block_cols), f32),
            jax.ShapeDtypeStruct((8, LANES), f32),
        ),
        in_specs=[hbm] * 7,
        out_specs=(vmem,) * 6,
        scratch_shapes=[
            pltpu.VMEM((width, q_cols + 2 * k_cols), bf16),
            pltpu.VMEM(out_weight.shape, bf16),
            pltpu.VMEM((tps, 2, rows, feats), bf16),
            pltpu.VMEM((rows, 2 * q_cols + 2 * k_cols), f32),
            pltpu.VMEM((count * rows + 2 * WINDOW, 2 * k_cols), bf16),
            pltpu.VMEM((2, count, rows, q_cols), bf16),
            pltpu.VMEM((count, rows, q_cols), bf16),
            pltpu.VMEM((count, rows, q_cols), bf16),
            pltpu.VMEM((count * rows + 2 * WINDOW, 2 * k_cols), f32),
            pltpu.VMEM((2, count, rows, block_cols), bf16),
            pltpu.VMEM((1 + 2 * (-(-2 * WINDOW // rows)), q_cols // k_cols * rows // 2, rows // 2 + 2 * WINDOW), f32),
            pltpu.VMEM((8, LANES), f32),
            pltpu.VMEM((3, rows, feats), bf16),
            pltpu.VMEM((3, rows, feats), bf16),
            pltpu.SMEM((1, sink_logit.shape[0]), f32),
            dma((5,)), dma((3,)), dma((3, 2)),
            dma((3, feats // block_cols)), dma((2, count)), dma((2,)), dma((1,)),
            dma((2, count // 2)), dma((count // 2,)), dma((2,)), dma((3, count)), dma((3,)), dma((3,)),
        ],
        compiler_params=pltpu.CompilerParams(
            collective_id=0, has_side_effects=True, vmem_limit_bytes=VMEM_BYTES
        ),
        name="layer",
    )(
        *(
            pltpu.with_memory_space_constraint(array, pltpu.HBM)
            for array in (
                layer_input, output_grad, query_weight, key_weight, value_weight, out_weight,
                sink_logit.reshape(1, -1),
            )
        ),
    )
    kept = [jax.ShapeDtypeStruct(out.shape, out.dtype) for out in outs[:5]]
    stored = pl.pallas_call(
        store_kernel,
        out_shape=(*kept, jax.ShapeDtypeStruct((1, sink_logit.shape[0]), f32)),
        in_specs=[vmem] * 6,
        out_specs=(hbm,) * 5 + (vmem,),
        scratch_shapes=[dma((5,))],
        compiler_params=pltpu.CompilerParams(vmem_limit_bytes=STORE_BYTES),
        name="store",
    )(*outs)
    return tuple(stored[:5]) + (stored[5].reshape(-1),)


def fits_kernel(mesh, layer_width):
    count, tps = mesh.shape["sp"], mesh.shape["tp"]
    return tps == 4 and count == 8 and layer_width == count * tps * LANES and HEADS == 2 * KV_HEADS


def solution(mesh):
    placed = (
        P("sp", "tp"),
        P("sp", "tp"),
        P(None, "tp"),
        P(None, "tp"),
        P(None, "tp"),
        P("tp", None),
        P("tp"),
    )

    def sharded(*arrays):
        width = arrays[0].shape[1]
        body = fused_device if fits_kernel(mesh, width) else per_device
        return jax.shard_map(
            body,
            mesh=mesh,
            in_specs=placed,
            out_specs=(
                P("sp", "tp"),
                P("sp", "tp"),
                P("sp", "tp"),
                P("sp", "tp"),
                P("tp", "sp"),
                P("tp"),
            ),
            check_vma=False,
        )(*arrays)

    return sharded
```

```python
import functools

import jax
import jax.numpy as jnp
from jax import lax
from jax.experimental import pallas as pl
from jax.experimental.pallas import tpu as pltpu
from jax.sharding import PartitionSpec as P

HEADS = 16
KV_HEADS = 8
HEAD = 128
WINDOW = 128


masked_score = -1e30


def extended(cells, sides, width):
    for axis, dim in sides:
        count = lax.axis_size(axis)
        ends = count - 1
        head = lax.slice_in_dim(cells, 0, width, axis=dim)
        tail = lax.slice_in_dim(cells, cells.shape[dim] - width, cells.shape[dim], axis=dim)
        cells = jnp.concatenate(
            [
                lax.ppermute(tail, axis, [(i, (i + 1) % count) for i in range(ends)]),
                cells,
                lax.ppermute(head, axis, [((i + 1) % count, i) for i in range(ends)]),
            ],
            axis=dim,
        )
    return cells


def passed_along(value, axis, steps):
    count = lax.axis_size(axis)
    initial, last = (max(0, -steps), min(count, count - steps))
    return lax.ppermute(value, axis, [(source, source + steps) for source in range(initial, last)])


def contract_rows(left, right):
    return lax.dot_general(
        left, right, (((0,), (0,)), ((), ())), preferred_element_type=jnp.float32
    )


def contract_cols(left, right):
    return lax.dot_general(
        left, right, (((1,), (1,)), ((), ())), preferred_element_type=jnp.float32
    )


def per_device(
    layer_input, output_grad, query_weight, key_weight, value_weight, out_weight, sink_logit
):
    whole_input, whole_grad = (
        lax.all_gather(layer_input, "tp", axis=1, tiled=True),
        lax.all_gather(output_grad, "tp", axis=1, tiled=True),
    )
    tok_rows = whole_input.shape[0]
    query_cols = query_weight.shape[1]
    key_cols = key_weight.shape[1]
    key_heads = key_cols // HEAD
    group_size = HEADS // KV_HEADS
    scaling = HEAD ** (-0.5)
    queries = jnp.dot(whole_input, query_weight, preferred_element_type=jnp.float32).astype(
        jnp.bfloat16
    )
    key_rows = jnp.dot(whole_input, key_weight, preferred_element_type=jnp.float32).astype(
        jnp.bfloat16
    )
    value_rows = jnp.dot(whole_input, value_weight, preferred_element_type=jnp.float32).astype(
        jnp.bfloat16
    )
    out_rows_grad = contract_cols(whole_grad, out_weight).astype(jnp.bfloat16)
    joined = jnp.concatenate([key_rows, value_rows], axis=1)
    band = extended(joined, (("sp", 0),), WINDOW)
    band_rows = band.shape[0]
    band_keys = band[:, :key_cols].reshape(band_rows, key_heads, HEAD)
    band_values = band[:, key_cols:].reshape(band_rows, key_heads, HEAD)
    shard_index = lax.axis_index("sp")
    seq_total = tok_rows * lax.axis_size("sp")
    query_pos = shard_index * tok_rows + jnp.arange(tok_rows, dtype=jnp.int32)
    key_pos = shard_index * tok_rows - WINDOW + jnp.arange(band_rows, dtype=jnp.int32)
    in_window = (
        (jnp.abs(query_pos[:, None] - key_pos[None, :]) <= WINDOW)
        & (key_pos[None, :] >= 0)
        & (key_pos[None, :] < seq_total)
    )
    query_heads = queries.reshape(tok_rows, key_heads, group_size, HEAD)
    grad_heads = out_rows_grad.reshape(tok_rows, key_heads, group_size, HEAD)
    scores = (
        jnp.einsum("qkgd,skd->kgqs", query_heads, band_keys, preferred_element_type=jnp.float32)
        * scaling
    )
    scores = jnp.where(in_window[None, None], scores, masked_score)
    sink_column = sink_logit.reshape(key_heads, group_size)[:, :, None]
    row_max = jnp.maximum(jnp.max(scores, axis=-1), sink_column)
    row_total = jnp.sum(jnp.exp(scores - row_max[..., None]), axis=-1) + jnp.exp(
        sink_column - row_max
    )
    log_total = row_max + jnp.log(row_total)
    soft_weights = jnp.exp(scores - log_total[..., None])
    soft_rounded = soft_weights.astype(jnp.bfloat16)
    attended = jnp.einsum(
        "kgqs,skd->qkgd", soft_rounded, band_values, preferred_element_type=jnp.float32
    ).astype(jnp.bfloat16)
    row_dots = jnp.sum(
        grad_heads.astype(jnp.float32) * attended.astype(jnp.float32), axis=-1
    ).transpose(1, 2, 0)
    prob_grads = jnp.einsum(
        "qkgd,skd->kgqs", grad_heads, band_values, preferred_element_type=jnp.float32
    )
    score_grads = (soft_weights * (prob_grads - row_dots[..., None])).astype(jnp.bfloat16)
    query_grads = (
        jnp.einsum("kgqs,skd->qkgd", score_grads, band_keys, preferred_element_type=jnp.float32)
        * scaling
    )
    query_grads = query_grads.astype(jnp.bfloat16).reshape(tok_rows, query_cols)
    band_key_grads = (
        jnp.einsum("kgqs,qkgd->skd", score_grads, query_heads, preferred_element_type=jnp.float32)
        * scaling
    )
    band_value_grads = jnp.einsum(
        "kgqs,qkgd->skd", soft_rounded, grad_heads, preferred_element_type=jnp.float32
    )
    band_grads = jnp.concatenate(
        [
            band_key_grads.reshape(band_rows, key_cols),
            band_value_grads.reshape(band_rows, key_cols),
        ],
        axis=1,
    )
    sink_part = -jnp.sum(jnp.exp(sink_column - log_total) * row_dots, axis=-1).reshape(-1)
    sink_grad = lax.psum(sink_part, "sp")
    attended_rows = attended.reshape(tok_rows, query_cols)
    input_block = lax.all_to_all(whole_input, "sp", 1, 0, tiled=True)
    grad_block = lax.all_to_all(whole_grad, "sp", 1, 0, tiled=True)
    early_rows = lax.all_gather(
        jnp.concatenate([query_grads, attended_rows], axis=1), "sp", axis=0, tiled=True
    )
    query_part = contract_rows(input_block, early_rows[:, :query_cols])
    out_part = contract_rows(early_rows[:, query_cols:], grad_block)
    returned_low = passed_along(band_grads[:WINDOW].astype(jnp.bfloat16), "sp", -1).astype(
        jnp.float32
    )
    returned_high = passed_along(
        band_grads[band_rows - WINDOW :].astype(jnp.bfloat16), "sp", 1
    ).astype(jnp.float32)
    own_rows = band_grads[WINDOW : WINDOW + tok_rows]
    own_rows = own_rows.at[tok_rows - WINDOW :].add(returned_low)
    own_rows = own_rows.at[:WINDOW].add(returned_high)
    key_grads = own_rows[:, :key_cols].astype(jnp.bfloat16)
    value_grads = own_rows[:, key_cols:].astype(jnp.bfloat16)
    late_rows = lax.all_gather(
        jnp.concatenate([key_grads, value_grads], axis=1), "sp", axis=0, tiled=True
    )
    key_part = contract_rows(input_block, late_rows[:, :key_cols])
    value_part = contract_rows(input_block, late_rows[:, key_cols:])
    partials = (
        contract_cols(query_grads, query_weight)
        + contract_cols(key_grads, key_weight)
        + contract_cols(value_grads, value_weight)
    )
    input_grad = lax.psum_scatter(
        partials.astype(jnp.bfloat16), "tp", scatter_dimension=1, tiled=True
    )
    return (input_grad, query_part, key_part, value_part, out_part, sink_grad)


LANES = 128
LOG2E = 1.4426950408889634
MESH = pl.DeviceIdType.MESH
VMEM_BYTES = 40 * 1024 * 1024
STORE_BYTES = 12 * 1024 * 1024


def dot_nn(a, b):
    return jnp.dot(a, b, preferred_element_type=jnp.float32)


def layer_kernel(
    x_hbm, g_hbm, wq_hbm, wk_hbm, wv_hbm, wo_hbm, sink_hbm,
    ig_ref, gq_ref, gk_ref, gv_ref, go_ref, sg_ref, att, dqs, dkv, far_cols,
    w_in, wo, xg, acc, kvs, acts, cols, bias, sinks, part, rs_in, sink_ref,
    w_sem, ag_send, ag_recv, col_send, col_recv, y_send, chip_send,
    z_sem, cross_sem, end_sem, acts_recv, rs_send, rs_recv,
):
    bf16, f32 = jnp.bfloat16, jnp.float32
    count, tps = lax.axis_size("sp"), lax.axis_size("tp")
    depth = count // 2
    s, t = lax.axis_index("sp"), lax.axis_index("tp")
    z, x = s // 2, s % 2
    y, core = t // 2, t % 2
    partner = y * 2 + (1 - core)
    across = (1 - y) * 2 + core
    diag = (1 - y) * 2 + (1 - core)
    rows, feats = x_hbm.shape
    q_cols, k_cols = wq_hbm.shape[1], wk_hbm.shape[1]
    in_cols = q_cols + 2 * k_cols
    block_cols = gq_ref.shape[0]
    per_slot = feats // block_cols
    key_heads = k_cols // HEAD
    group = q_cols // k_cols
    scaling = HEAD**-0.5

    def remote(src, dst, send, recv, dev_s, dev_t):
        return pltpu.make_async_remote_copy(
            src_ref=src, dst_ref=dst, send_sem=send, recv_sem=recv,
            device_id=(dev_s, dev_t), device_id_type=MESH,
        )

    own = [
        pltpu.make_async_copy(src, xg.at[t, a], w_sem.at[3 + a])
        for a, src in enumerate((x_hbm, g_hbm))
    ]
    for copy in own:
        copy.start()
    weights, at = [], 0
    for src in (wq_hbm, wk_hbm, wv_hbm):
        span = pl.ds(at, src.shape[1])
        weights.append(pltpu.make_async_copy(src, w_in.at[:, span], w_sem.at[0]))
        at += src.shape[1]
    weights.append(pltpu.make_async_copy(wo_hbm, wo, w_sem.at[1]))
    weights.append(pltpu.make_async_copy(sink_hbm, sink_ref, w_sem.at[2]))
    for copy in weights:
        copy.start()

    barrier = pltpu.get_barrier_semaphore()
    for peer in (partner, across, diag):
        pl.semaphore_signal(barrier, inc=1, device_id=(s, peer), device_id_type=MESH)
    for d in range(1, count):
        pl.semaphore_signal(
            barrier, inc=1, device_id=((s + d) % count, t), device_id_type=MESH
        )
    pl.semaphore_wait(barrier, 3 + count - 1)

    sources = (xg.at[t, 0], xg.at[t, 1])
    for copy in own:
        copy.wait()
    to_across = [
        remote(sources[a], xg.at[t, a], ag_send.at[0], ag_recv.at[0, a], s, across)
        for a in range(2)
    ]
    to_partner = [
        remote(sources[a], xg.at[t, a], ag_send.at[1], ag_recv.at[1, a], s, partner)
        for a in range(2)
    ]
    relay = [
        remote(xg.at[across, a], xg.at[across, a], ag_send.at[2], ag_recv.at[2, a], s, partner)
        for a in range(2)
    ]
    for copy in to_across + to_partner:
        copy.start()

    is_home = s // per_slot == t
    is_across = s // per_slot == across
    is_last = jnp.logical_not(is_home | is_across)

    half = count // 2
    here_half = s // half * half
    near = [here_half + i for i in range(half)]
    far = [half - here_half + i for i in range(half)]
    sends_near = s // half == t * per_slot // half

    def column_copy(kind, b):
        a, slot = kind % 2, t if kind else across
        return remote(
            xg.at[slot, a, :, pl.ds(b * block_cols, block_cols)], cols.at[a, s],
            col_send.at[kind, b], col_recv.at[a, s], slot * per_slot + b, t,
        )

    def column_arrival(a, source):
        ref = cols.at[a, source]
        return remote(ref, ref, col_send.at[a, 0], col_recv.at[a, source], (s + 1) % count, t)

    def y_copy(a, source):
        ref = cols.at[a, source]
        return remote(ref, ref, y_send.at[a], col_recv.at[a, source], s, across)

    def chip_copy(a, source):
        ref = cols.at[a, source]
        return remote(ref, ref, chip_send.at[0], col_recv.at[a, source], s, partner)

    def each_column(kind, act, which=None):
        slot = t if kind else across
        for b in range(per_slot) if which is None else which:
            sent = slot * per_slot + b != s

            @pl.when(sent if kind == 1 else sent & sends_near)
            def _():
                act(column_copy(kind, b))

    def send_columns(kind, which=None):
        each_column(kind, lambda copy: copy.start(), which)

    send_columns(1)
    send_columns(2)

    def project_input(slot, first=False):
        cells = xg[slot, 0]
        span = pl.ds(pl.multiple_of(slot * feats, feats), feats)
        term = dot_nn(cells, w_in[span, :])
        acc[:, :in_cols] = term if first else acc[:, :in_cols] + term

    def project_grad(slot, first=False):
        cells = xg[slot, 1]
        span = pl.ds(pl.multiple_of(slot * feats, feats), feats)
        term = contract_cols(cells, wo[:, span])
        acc[:, in_cols:] = term if first else acc[:, in_cols:] + term

    for edge in (0, WINDOW + count * rows):
        kvs[edge : edge + WINDOW] = jnp.zeros((WINDOW, 2 * k_cols), bf16)
    dkv[...] = jnp.zeros_like(dkv)
    sinks[...] = jnp.zeros_like(sinks)
    part_rows = rows // 2
    part_keys = part_rows + 2 * WINDOW
    tall = group * part_rows
    edges = -(-WINDOW // part_rows)
    parts = rows * count // part_rows
    q_at = lax.rem(lax.broadcasted_iota(jnp.int32, (tall, part_keys), 0), part_rows)
    k_at = lax.broadcasted_iota(jnp.int32, (tall, part_keys), 1)
    band = (k_at >= q_at) & (k_at - q_at <= 2 * WINDOW)
    starts = [edges] + list(range(edges)) + [parts - edges + i for i in range(edges)]
    for i, start in enumerate(starts):
        pos = k_at + (start * part_rows - WINDOW)
        inside = band & (pos >= 0) & (pos < rows * count) if i else band
        bias[i] = jnp.where(inside, 0.0, masked_score)

    pltpu.make_async_copy(w_in, w_in, w_sem.at[0]).wait()
    for copy in weights[3:]:
        copy.wait()
    project_input(t, True)
    project_grad(t, True)
    to_partner[0].wait_recv()
    project_input(partner)
    to_partner[1].wait_recv()
    project_grad(partner)
    to_across[0].wait_recv()
    relay[0].start()
    send_columns(0, (0,))
    project_input(across)
    relay[0].wait_recv()
    project_input(diag)
    for b in range(per_slot):
        span = slice(b * block_cols, (b + 1) * block_cols)

        @pl.when(t * per_slot + b == s)
        def _():
            for a in range(2):
                cols[a, s] = xg[t, a, :, span]


    def own_rows(block):
        return pl.ds(pl.multiple_of(WINDOW + block * rows, 32), rows)

    def item(i, block):
        return acts.at[i - 1, block] if i else kvs.at[own_rows(block)]

    def z_copy(i, block, way):
        dev = (z + 1 - 2 * way + depth) % depth * 2 + x
        ref = item(i, block)
        return remote(ref, ref, z_sem.at[way, block // 2], acts_recv.at[i, block], dev, t)

    def cross_copy(i, block):
        ref = item(i, block)
        return remote(
            ref, ref, cross_sem.at[block // 2], acts_recv.at[i, block], z * 2 + (1 - x), t
        )

    def goes_on(way):
        return jnp.where(way == 0, z < depth - 1, z > 0)

    def send_own(i):
        cross_copy(i, s).start()
        for way in range(2):

            @pl.when(goes_on(way))
            def _():
                z_copy(i, s, way).start()

    def level_at(d, way):
        level = z - d * (1 - 2 * way)
        return level, (level >= 0) & (level < depth)

    def crosses(i, level):
        return (i < 2) | ((level > 0) & (level < depth - 1)) | (level == z)

    def end_copy(way):
        block = (depth - 1) * way * 2 + (1 - x)
        dev = (z + 1 - 2 * way + depth) % depth * 2 + x
        ref = item(2, block)
        return remote(ref, ref, end_sem.at[way], acts_recv.at[2, block], dev, t)

    def forward_end(d, allowed=True):
        for way in range(2):
            level, there = level_at(d, way)
            there = there & allowed

            @pl.when(there & (level == (depth - 1) * way))
            def _():
                end_copy(way).wait_recv()

                @pl.when(goes_on(way))
                def _():
                    end_copy(way).start()

    def forward_way(i, d, way, allowed=True):
        level, there = level_at(d, way)

        @pl.when(there & allowed)
        def _():
            block = level * 2 + x
            z_copy(i, block, way).wait_recv()

            @pl.when(crosses(i, level))
            def _():
                cross_copy(i, block).start()

            @pl.when(goes_on(way))
            def _():
                z_copy(i, block, way).start()

    early, late = 1 - y, y

    def forward(i, d, allowed=True):
        forward_way(i, d, early, allowed)
        forward_way(i, d, late, allowed)

    kvs[own_rows(s)] = acc[:, q_cols:in_cols].astype(bf16)
    send_own(0)
    acts[0, s] = acc[:, :q_cols].astype(bf16)
    send_own(1)
    send_columns(0, (1,))

    to_across[1].wait_recv()
    relay[1].start()
    project_grad(across)
    relay[1].wait_recv()
    project_grad(diag)
    acts[1, s] = acc[:, in_cols:].astype(bf16)
    send_own(2)

    straight = [(source, a) for source in near for a in range(2)] + [(source, 1) for source in far]
    around = [(source, 0) for source in far]

    def pass_direct(here, items):
        @pl.when(here)
        def _():
            for source, a in items:

                @pl.when(source != s)
                def _():
                    column_arrival(a, source).wait_recv()

                y_copy(a, source).start()
                chip_copy(a, source).start()

    def pass_second(here, items):
        @pl.when(here)
        def _():
            for source, a in items:
                y_copy(a, source).wait_recv()
                chip_copy(a, source).start()

    def last_arrivals(sources):
        @pl.when(is_last)
        def _():
            for source in sources:
                for a in range(2):
                    chip_copy(a, source).wait_recv()

    def attend_block(block):
        jobs = [(half_at, kh) for half_at in range(2) for kh in range(key_heads)]
        each = range(len(jobs))
        head_at = lax.broadcasted_iota(jnp.int32, (tall, 1), 0) // part_rows

        def at(half_at):
            start = block * rows + half_at * part_rows
            return pl.ds(pl.multiple_of(start, 16), part_keys)

        def stacked(i, half_at, kh):
            span = slice(half_at * part_rows, (half_at + 1) * part_rows)
            heads = [kh * group + g for g in range(group)]
            return jnp.concatenate(
                [acts[i, block, span, h * HEAD : (h + 1) * HEAD] for h in heads], axis=0
            )

        def k_lanes(kh):
            return slice(kh * HEAD, (kh + 1) * HEAD)

        def v_lanes(kh):
            return slice(k_cols + kh * HEAD, k_cols + (kh + 1) * HEAD)

        which = []
        for half_at, _ in jobs:
            part_at = block * 2 + half_at
            late = part_at - (parts - edges)
            which.append(
                jnp.where(part_at < edges, 1 + part_at, jnp.where(late >= 0, 1 + edges + late, 0))
            )
        q = [stacked(0, *job) for job in jobs]
        do = [stacked(1, *job) for job in jobs]
        keys = [kvs[at(half_at), k_lanes(kh)] for half_at, kh in jobs]
        values = [kvs[at(half_at), v_lanes(kh)] for half_at, kh in jobs]
        scores = [contract_cols(q[i], keys[i]) for i in each]
        prob_grads = [contract_cols(do[i], values[i]) for i in each]
        scores = [scores[i] * (scaling * LOG2E) + bias[which[i]] for i in each]
        sink = []
        for _, kh in jobs:
            column = jnp.full((tall, 1), sink_ref[0, kh * group], f32)
            for g in range(1, group):
                column = jnp.where(head_at == g, sink_ref[0, kh * group + g], column)
            sink.append(column * LOG2E)
        top = [jnp.maximum(jnp.max(scores[i], axis=1, keepdims=True), sink[i]) for i in each]
        e = [jnp.exp2(scores[i] - top[i]) for i in each]
        sink_e = [jnp.exp2(sink[i] - top[i]) for i in each]
        inverse = [1.0 / (jnp.sum(e[i], axis=1, keepdims=True) + sink_e[i]) for i in each]
        p = [e[i] * inverse[i] for i in each]
        p_low = [p[i].astype(bf16) for i in each]
        attended = [dot_nn(p_low[i], values[i]).astype(bf16) for i in each]
        dots = [
            jnp.sum(do[i].astype(f32) * attended[i].astype(f32), axis=1, keepdims=True)
            for i in each
        ]
        dv = [contract_rows(p_low[i], do[i]) for i in each]
        ds = [(p[i] * (prob_grads[i] - dots[i])).astype(bf16) for i in each]
        dq = [(dot_nn(ds[i], keys[i]) * scaling).astype(bf16) for i in each]
        dk = [contract_rows(ds[i], q[i]) for i in each]
        lane_at = lax.broadcasted_iota(jnp.int32, (8, LANES), 1)
        sink_row = sinks[...]
        for i, (half_at, kh) in enumerate(jobs):
            span = slice(half_at * part_rows, (half_at + 1) * part_rows)
            sink_terms = sink_e[i] * inverse[i] * dots[i]
            for g in range(group):
                h = kh * group + g
                lanes, piece = slice(h * HEAD, (h + 1) * HEAD), slice(g * part_rows, (g + 1) * part_rows)
                att[block, span, lanes] = attended[i][piece]
                dqs[block, span, lanes] = dq[i][piece]
                total = jnp.sum(sink_terms[piece], axis=0, keepdims=True)
                sink_row = jnp.where(lane_at == h, sink_row - total, sink_row)
            dkv[at(half_at), k_lanes(kh)] += dk[i]
            dkv[at(half_at), v_lanes(kh)] += dv[i]
        sinks[...] = sink_row

    def cross_arrived(i, level):
        cross_copy(i, level * 2 + (1 - x)).wait_recv()

    def attend_own():
        for i in range(3):
            cross_arrived(i, z)
        for way in range(2):

            @pl.when(z == (depth - 1) * way)
            def _():
                end_copy(way).start()

        @pl.when((z == 0) | (z == depth - 1))
        def _():
            block = jnp.where(z == 0, 0, count - 1)
            attend_block(block)

    def attend(d, way, span=None):
        level, there = level_at(d, way)
        cross = level * 2 + (1 - x)
        extra = jnp.where(jnp.where(way == 0, level == 0, level == depth - 1), 1, 0)
        stop = 2 + extra
        nearest = jnp.where(way == 0, 2 * level + 2, 2 * level - 1)
        step = jnp.where(way == 0, -1, 1)
        inside = (x == way) | (extra == 1)
        key_at = jnp.where(x == way, 0, 1)

        def one(k, _):
            is_end = k == stop - 1
            block = nearest + step * k
            passed = jnp.where(way == 0, block <= cross, block >= cross)
            block = jnp.where(inside & passed, block + step, block)
            block = jnp.where(inside & is_end, cross, block)

            @pl.when(k == key_at)
            def _():
                cross_arrived(0, level)

            @pl.when(is_end)
            def _():
                cross_arrived(1, level)

            @pl.when(is_end & (extra == 0))
            def _():
                cross_arrived(2, level)

            attend_block(block)
            return 0

        begin, end = (0, stop) if span is None else span(stop)
        lax.fori_loop(begin, jnp.where(there, end, begin), one, 0)

    def attend_both(d, span=None):
        def one(way, _):
            attend(d, way, None if span is None else functools.partial(span, way))
            return 0

        lax.fori_loop(0, 2, one, 0)

    is_end = (z == 0) | (z == depth - 1)
    is_mid = jnp.logical_not(is_end)
    waits_late = is_mid & ((2 * z < depth) == (y == 1))
    waits_little = is_mid & jnp.logical_not(waits_late)
    pass_direct(is_home, straight)
    forward_way(0, 1, early)
    forward_way(1, 1, early)
    forward_way(0, 1, late)
    forward_way(2, 1, early, is_mid)
    forward_way(1, 1, late)
    attend_own()
    forward_way(2, 1, early, is_end)
    forward_way(2, 1, late)
    forward_end(1)
    pass_direct(is_across, around)
    attend(1, 1 - y, lambda stop: (0, jnp.where(waits_late, stop, 0)))
    forward(0, 2)
    forward(1, 2)
    attend(1, 1 - y, lambda stop: (jnp.where(waits_late, stop, 0), stop))
    forward(2, 2, waits_little)
    forward_end(2, waits_little)
    pass_second(is_across, straight)
    attend(1, y)
    own_dkv = dkv[own_rows(s)]
    own_grads = jnp.concatenate(
        [
            dqs[s],
            (own_dkv[:, :k_cols] * scaling).astype(bf16),
            own_dkv[:, k_cols:].astype(bf16),
        ],
        axis=1,
    )

    def partial_for(slot):
        span = pl.ds(pl.multiple_of(slot * feats, feats), feats)
        return contract_cols(own_grads, w_in[span, :])

    rs_copies = [
        remote(part.at[i], rs_in.at[i], rs_send.at[i], rs_recv.at[i], s, peer)
        for i, peer in enumerate((partner, partner, across))
    ]
    part[0] = partial_for(diag).astype(bf16)
    rs_copies[0].start()
    acc[:, :feats] = partial_for(across)
    forward(2, 2, jnp.logical_not(waits_little))
    forward_end(2, jnp.logical_not(waits_little))
    def weight_grads():
        last_arrivals(near)
        blocks = pl.ds(here_half, half)
        seq = pl.ds(pl.multiple_of(WINDOW + here_half * rows, WINDOW), half * rows)

        def flat(value):
            return value.reshape(half * rows, value.shape[-1])

        left = flat(cols[0, blocks])
        pieces = (
            (go_ref, contract_rows(flat(att[blocks]), flat(cols[1, blocks]))),
            (gq_ref, contract_rows(left, flat(dqs[blocks]))),
            (gk_ref, contract_rows(left, (dkv[seq, :k_cols] * scaling).astype(bf16))),
            (gv_ref, contract_rows(left, dkv[seq, k_cols:].astype(bf16))),
        )
        for ref, value in pieces:
            ref[...] = value

    @pl.when(jnp.logical_not(is_end) & (core == 1))
    def _():
        weight_grads()

    rs_copies[0].wait_recv()
    part[2] = (acc[:, :feats] + rs_in[0].astype(f32)).astype(bf16)
    rs_copies[2].start()
    part[1] = partial_for(partner).astype(bf16)
    rs_copies[1].start()
    acc[:, :feats] = partial_for(t)

    @pl.when(jnp.logical_not(is_end) & (core == 0))
    def _():
        weight_grads()

    for d in range(3, depth):
        forward(0, d)
        forward(1, d)
    attend_both(2)
    @pl.when(is_end)
    def _():
        weight_grads()

    for d in range(3, depth):
        attend_both(d, lambda way, stop: (0, 1))
    for d in range(3, depth):
        forward(2, d)
        attend_both(d, lambda way, stop: (1, stop - 1))
    pass_second(is_home, around)
    last_arrivals(far)
    far_cols[...] = cols[:, pl.ds(half - here_half, half)]
    for d in range(3, depth):
        forward_end(d)
        attend_both(d, lambda way, stop: (stop - 1, stop))
    sg_ref[...] = sinks[...]
    for copy in rs_copies[1:]:
        copy.wait_recv()
    ig_ref[...] = (
        acc[:, :feats] + rs_in[1].astype(f32) + rs_in[2].astype(f32)
    ).astype(bf16)

    def sent(ref, sem):
        remote(ref, ref, sem, rs_recv.at[0], (s + 1) % count, t).wait_send()

    for i in range(3):
        sent(xg.at[t], ag_send.at[i])
    for copy in rs_copies:
        copy.wait_send()
    for kind in range(3):
        each_column(kind, lambda copy: copy.wait_send())

    @pl.when(is_home)
    def _():
        sent(cols.at[0, pl.ds(here_half, half)], y_send.at[0])
        sent(cols.at[1], y_send.at[1])

    @pl.when(is_across)
    def _():
        sent(cols.at[0, pl.ds(half - here_half, half)], y_send.at[0])

    @pl.when(jnp.logical_not(is_last))
    def _():
        sent(cols, chip_send.at[0])

    for level in range(depth):
        for way in range(2):
            came = jnp.where(way == 0, level <= z, level >= z)

            @pl.when(came & goes_on(way))
            def _():
                sent(acts.at[0, pl.ds(0, 3)], z_sem.at[way, level])

        all_cross = crosses(2, level)

        @pl.when(all_cross)
        def _():
            sent(acts.at[0, pl.ds(0, 3)], cross_sem.at[level])

        @pl.when(jnp.logical_not(all_cross))
        def _():
            sent(acts.at[0, pl.ds(0, 2)], cross_sem.at[level])

    for way in range(2):

        @pl.when(goes_on(way))
        def _():
            end_copy(way).wait_send()


def store_kernel(
    ig_in, gq_in, gk_in, gv_in, go_in, sink_in, att, dqs, dkv, far_cols,
    ig_out, gq_out, gk_out, gv_out, go_out, sink_out, gq, gk, gv, go, sem,
):
    bf16 = jnp.bfloat16
    count = lax.axis_size("sp")
    half = count // 2
    begin = half - lax.axis_index("sp") // half * half
    rows = att.shape[1]
    k_cols = gk.shape[1]
    blocks = pl.ds(begin, half)
    seq = pl.ds(pl.multiple_of(WINDOW + begin * rows, WINDOW), half * rows)

    def flat(value):
        return value.reshape(half * rows, value.shape[-1])

    def send(i, held, out):
        copy = pltpu.make_async_copy(held, out, sem.at[i])
        copy.start()
        return copy

    copies = [send(0, ig_in, ig_out)]
    sink_out[...] = sink_in[0:1, : sink_out.shape[1]]
    left = flat(far_cols[0])
    go[...] = go_in[...] + contract_rows(flat(att[blocks]), flat(far_cols[1]))
    copies.append(send(1, go, go_out))
    gq[...] = gq_in[...] + contract_rows(left, flat(dqs[blocks]))
    copies.append(send(2, gq, gq_out))
    gk[...] = gk_in[...] + contract_rows(left, (dkv[seq, :k_cols] * HEAD**-0.5).astype(bf16))
    copies.append(send(3, gk, gk_out))
    gv[...] = gv_in[...] + contract_rows(left, dkv[seq, k_cols:].astype(bf16))
    copies.append(send(4, gv, gv_out))
    for copy in copies:
        copy.wait()


def fused_device(
    layer_input, output_grad, query_weight, key_weight, value_weight, out_weight, sink_logit
):
    bf16, f32 = jnp.bfloat16, jnp.float32
    count, tps = lax.axis_size("sp"), lax.axis_size("tp")
    rows, feats = layer_input.shape
    width = query_weight.shape[0]
    q_cols, k_cols = query_weight.shape[1], key_weight.shape[1]
    block_cols = width // count
    vmem = pl.BlockSpec(memory_space=pltpu.VMEM)
    hbm = pl.BlockSpec(memory_space=pltpu.HBM)
    dma = pltpu.SemaphoreType.DMA
    outs = pl.pallas_call(
        layer_kernel,
        out_shape=(
            jax.ShapeDtypeStruct((rows, feats), bf16),
            jax.ShapeDtypeStruct((block_cols, q_cols), f32),
            jax.ShapeDtypeStruct((block_cols, k_cols), f32),
            jax.ShapeDtypeStruct((block_cols, k_cols), f32),
            jax.ShapeDtypeStruct((q_cols, block_cols), f32),
            jax.ShapeDtypeStruct((8, LANES), f32),
            jax.ShapeDtypeStruct((count, rows, q_cols), bf16),
            jax.ShapeDtypeStruct((count, rows, q_cols), bf16),
            jax.ShapeDtypeStruct((count * rows + 2 * WINDOW, 2 * k_cols), f32),
            jax.ShapeDtypeStruct((2, count // 2, rows, block_cols), bf16),
        ),
        in_specs=[hbm] * 7,
        out_specs=(vmem,) * 10,
        scratch_shapes=[
            pltpu.VMEM((width, q_cols + 2 * k_cols), bf16),
            pltpu.VMEM(out_weight.shape, bf16),
            pltpu.VMEM((tps, 2, rows, feats), bf16),
            pltpu.VMEM((rows, 2 * q_cols + 2 * k_cols), f32),
            pltpu.VMEM((count * rows + 2 * WINDOW, 2 * k_cols), bf16),
            pltpu.VMEM((2, count, rows, q_cols), bf16),
            pltpu.VMEM((2, count, rows, block_cols), bf16),
            pltpu.VMEM((1 + 2 * (-(-2 * WINDOW // rows)), q_cols // k_cols * rows // 2, rows // 2 + 2 * WINDOW), f32),
            pltpu.VMEM((8, LANES), f32),
            pltpu.VMEM((3, rows, feats), bf16),
            pltpu.VMEM((3, rows, feats), bf16),
            pltpu.SMEM((1, sink_logit.shape[0]), f32),
            dma((5,)), dma((3,)), dma((3, 2)),
            dma((3, feats // block_cols)), dma((2, count)), dma((2,)), dma((1,)),
            dma((2, count // 2)), dma((count // 2,)), dma((2,)), dma((3, count)), dma((3,)), dma((3,)),
        ],
        compiler_params=pltpu.CompilerParams(
            collective_id=0, has_side_effects=True, vmem_limit_bytes=VMEM_BYTES
        ),
        name="layer",
    )(
        *(
            pltpu.with_memory_space_constraint(array, pltpu.HBM)
            for array in (
                layer_input, output_grad, query_weight, key_weight, value_weight, out_weight,
                sink_logit.reshape(1, -1),
            )
        ),
    )
    kept = [jax.ShapeDtypeStruct(out.shape, out.dtype) for out in outs[:5]]
    stored = pl.pallas_call(
        store_kernel,
        out_shape=(*kept, jax.ShapeDtypeStruct((1, sink_logit.shape[0]), f32)),
        in_specs=[vmem] * 10,
        out_specs=(hbm,) * 5 + (vmem,),
        scratch_shapes=[pltpu.VMEM(out.shape, f32) for out in outs[1:5]] + [dma((5,))],
        compiler_params=pltpu.CompilerParams(vmem_limit_bytes=STORE_BYTES),
        name="store",
    )(*outs)
    return tuple(stored[:5]) + (stored[5].reshape(-1),)


def fits_kernel(mesh, layer_width):
    count, tps = mesh.shape["sp"], mesh.shape["tp"]
    return tps == 4 and count == 8 and layer_width == count * tps * LANES and HEADS == 2 * KV_HEADS


def solution(mesh):
    placed = (
        P("sp", "tp"),
        P("sp", "tp"),
        P(None, "tp"),
        P(None, "tp"),
        P(None, "tp"),
        P("tp", None),
        P("tp"),
    )

    def sharded(*arrays):
        width = arrays[0].shape[1]
        body = fused_device if fits_kernel(mesh, width) else per_device
        return jax.shard_map(
            body,
            mesh=mesh,
            in_specs=placed,
            out_specs=(
                P("sp", "tp"),
                P("sp", "tp"),
                P("sp", "tp"),
                P("sp", "tp"),
                P("tp", "sp"),
                P("tp"),
            ),
            check_vma=False,
        )(*arrays)

    return sharded
```

```python
import functools

import jax
import jax.numpy as jnp
from jax import lax
from jax.experimental import pallas as pl
from jax.experimental.pallas import tpu as pltpu
from jax.sharding import PartitionSpec as P

HEADS = 16
KV_HEADS = 8
HEAD = 128
WINDOW = 128


masked_score = -1e30


def extended(cells, sides, width):
    for axis, dim in sides:
        count = lax.axis_size(axis)
        ends = count - 1
        head = lax.slice_in_dim(cells, 0, width, axis=dim)
        tail = lax.slice_in_dim(cells, cells.shape[dim] - width, cells.shape[dim], axis=dim)
        cells = jnp.concatenate(
            [
                lax.ppermute(tail, axis, [(i, (i + 1) % count) for i in range(ends)]),
                cells,
                lax.ppermute(head, axis, [((i + 1) % count, i) for i in range(ends)]),
            ],
            axis=dim,
        )
    return cells


def passed_along(value, axis, steps):
    count = lax.axis_size(axis)
    initial, last = (max(0, -steps), min(count, count - steps))
    return lax.ppermute(value, axis, [(source, source + steps) for source in range(initial, last)])


def contract_rows(left, right):
    return lax.dot_general(
        left, right, (((0,), (0,)), ((), ())), preferred_element_type=jnp.float32
    )


def contract_cols(left, right):
    return lax.dot_general(
        left, right, (((1,), (1,)), ((), ())), preferred_element_type=jnp.float32
    )


def per_device(
    layer_input, output_grad, query_weight, key_weight, value_weight, out_weight, sink_logit
):
    whole_input, whole_grad = (
        lax.all_gather(layer_input, "tp", axis=1, tiled=True),
        lax.all_gather(output_grad, "tp", axis=1, tiled=True),
    )
    tok_rows = whole_input.shape[0]
    query_cols = query_weight.shape[1]
    key_cols = key_weight.shape[1]
    key_heads = key_cols // HEAD
    group_size = HEADS // KV_HEADS
    scaling = HEAD ** (-0.5)
    queries = jnp.dot(whole_input, query_weight, preferred_element_type=jnp.float32).astype(
        jnp.bfloat16
    )
    key_rows = jnp.dot(whole_input, key_weight, preferred_element_type=jnp.float32).astype(
        jnp.bfloat16
    )
    value_rows = jnp.dot(whole_input, value_weight, preferred_element_type=jnp.float32).astype(
        jnp.bfloat16
    )
    out_rows_grad = contract_cols(whole_grad, out_weight).astype(jnp.bfloat16)
    joined = jnp.concatenate([key_rows, value_rows], axis=1)
    band = extended(joined, (("sp", 0),), WINDOW)
    band_rows = band.shape[0]
    band_keys = band[:, :key_cols].reshape(band_rows, key_heads, HEAD)
    band_values = band[:, key_cols:].reshape(band_rows, key_heads, HEAD)
    shard_index = lax.axis_index("sp")
    seq_total = tok_rows * lax.axis_size("sp")
    query_pos = shard_index * tok_rows + jnp.arange(tok_rows, dtype=jnp.int32)
    key_pos = shard_index * tok_rows - WINDOW + jnp.arange(band_rows, dtype=jnp.int32)
    in_window = (
        (jnp.abs(query_pos[:, None] - key_pos[None, :]) <= WINDOW)
        & (key_pos[None, :] >= 0)
        & (key_pos[None, :] < seq_total)
    )
    query_heads = queries.reshape(tok_rows, key_heads, group_size, HEAD)
    grad_heads = out_rows_grad.reshape(tok_rows, key_heads, group_size, HEAD)
    scores = (
        jnp.einsum("qkgd,skd->kgqs", query_heads, band_keys, preferred_element_type=jnp.float32)
        * scaling
    )
    scores = jnp.where(in_window[None, None], scores, masked_score)
    sink_column = sink_logit.reshape(key_heads, group_size)[:, :, None]
    row_max = jnp.maximum(jnp.max(scores, axis=-1), sink_column)
    row_total = jnp.sum(jnp.exp(scores - row_max[..., None]), axis=-1) + jnp.exp(
        sink_column - row_max
    )
    log_total = row_max + jnp.log(row_total)
    soft_weights = jnp.exp(scores - log_total[..., None])
    soft_rounded = soft_weights.astype(jnp.bfloat16)
    attended = jnp.einsum(
        "kgqs,skd->qkgd", soft_rounded, band_values, preferred_element_type=jnp.float32
    ).astype(jnp.bfloat16)
    row_dots = jnp.sum(
        grad_heads.astype(jnp.float32) * attended.astype(jnp.float32), axis=-1
    ).transpose(1, 2, 0)
    prob_grads = jnp.einsum(
        "qkgd,skd->kgqs", grad_heads, band_values, preferred_element_type=jnp.float32
    )
    score_grads = (soft_weights * (prob_grads - row_dots[..., None])).astype(jnp.bfloat16)
    query_grads = (
        jnp.einsum("kgqs,skd->qkgd", score_grads, band_keys, preferred_element_type=jnp.float32)
        * scaling
    )
    query_grads = query_grads.astype(jnp.bfloat16).reshape(tok_rows, query_cols)
    band_key_grads = (
        jnp.einsum("kgqs,qkgd->skd", score_grads, query_heads, preferred_element_type=jnp.float32)
        * scaling
    )
    band_value_grads = jnp.einsum(
        "kgqs,qkgd->skd", soft_rounded, grad_heads, preferred_element_type=jnp.float32
    )
    band_grads = jnp.concatenate(
        [
            band_key_grads.reshape(band_rows, key_cols),
            band_value_grads.reshape(band_rows, key_cols),
        ],
        axis=1,
    )
    sink_part = -jnp.sum(jnp.exp(sink_column - log_total) * row_dots, axis=-1).reshape(-1)
    sink_grad = lax.psum(sink_part, "sp")
    attended_rows = attended.reshape(tok_rows, query_cols)
    input_block = lax.all_to_all(whole_input, "sp", 1, 0, tiled=True)
    grad_block = lax.all_to_all(whole_grad, "sp", 1, 0, tiled=True)
    early_rows = lax.all_gather(
        jnp.concatenate([query_grads, attended_rows], axis=1), "sp", axis=0, tiled=True
    )
    query_part = contract_rows(input_block, early_rows[:, :query_cols])
    out_part = contract_rows(early_rows[:, query_cols:], grad_block)
    returned_low = passed_along(band_grads[:WINDOW].astype(jnp.bfloat16), "sp", -1).astype(
        jnp.float32
    )
    returned_high = passed_along(
        band_grads[band_rows - WINDOW :].astype(jnp.bfloat16), "sp", 1
    ).astype(jnp.float32)
    own_rows = band_grads[WINDOW : WINDOW + tok_rows]
    own_rows = own_rows.at[tok_rows - WINDOW :].add(returned_low)
    own_rows = own_rows.at[:WINDOW].add(returned_high)
    key_grads = own_rows[:, :key_cols].astype(jnp.bfloat16)
    value_grads = own_rows[:, key_cols:].astype(jnp.bfloat16)
    late_rows = lax.all_gather(
        jnp.concatenate([key_grads, value_grads], axis=1), "sp", axis=0, tiled=True
    )
    key_part = contract_rows(input_block, late_rows[:, :key_cols])
    value_part = contract_rows(input_block, late_rows[:, key_cols:])
    partials = (
        contract_cols(query_grads, query_weight)
        + contract_cols(key_grads, key_weight)
        + contract_cols(value_grads, value_weight)
    )
    input_grad = lax.psum_scatter(
        partials.astype(jnp.bfloat16), "tp", scatter_dimension=1, tiled=True
    )
    return (input_grad, query_part, key_part, value_part, out_part, sink_grad)


LANES = 128
LOG2E = 1.4426950408889634
MESH = pl.DeviceIdType.MESH
VMEM_BYTES = 40 * 1024 * 1024
STORE_BYTES = 12 * 1024 * 1024


def dot_nn(a, b):
    return jnp.dot(a, b, preferred_element_type=jnp.float32)


def layer_kernel(
    x_hbm, g_hbm, wq_hbm, wk_hbm, wv_hbm, wo_hbm, sink_hbm,
    ig_ref, gq_ref, gk_ref, gv_ref, go_ref, sg_ref, att, dqs, dkv, far_cols,
    w_in, wo, xg, acc, kvs, acts, cols, bias, sinks, part, rs_in, sink_ref,
    w_sem, ag_send, ag_recv, col_send, col_recv, y_send, chip_send,
    z_sem, cross_sem, end_sem, acts_recv, rs_send, rs_recv,
):
    bf16, f32 = jnp.bfloat16, jnp.float32
    count, tps = lax.axis_size("sp"), lax.axis_size("tp")
    depth = count // 2
    s, t = lax.axis_index("sp"), lax.axis_index("tp")
    z, x = s // 2, s % 2
    y, core = t // 2, t % 2
    partner = y * 2 + (1 - core)
    across = (1 - y) * 2 + core
    diag = (1 - y) * 2 + (1 - core)
    rows, feats = x_hbm.shape
    q_cols, k_cols = wq_hbm.shape[1], wk_hbm.shape[1]
    in_cols = q_cols + 2 * k_cols
    block_cols = gq_ref.shape[0]
    per_slot = feats // block_cols
    key_heads = k_cols // HEAD
    group = q_cols // k_cols
    scaling = HEAD**-0.5

    def remote(src, dst, send, recv, dev_s, dev_t):
        return pltpu.make_async_remote_copy(
            src_ref=src, dst_ref=dst, send_sem=send, recv_sem=recv,
            device_id=(dev_s, dev_t), device_id_type=MESH,
        )

    own = [
        pltpu.make_async_copy(src, xg.at[t, a], w_sem.at[3 + a])
        for a, src in enumerate((x_hbm, g_hbm))
    ]
    for copy in own:
        copy.start()
    weights, at = [], 0
    for src in (wq_hbm, wk_hbm, wv_hbm):
        span = pl.ds(at, src.shape[1])
        weights.append(pltpu.make_async_copy(src, w_in.at[:, span], w_sem.at[0]))
        at += src.shape[1]
    weights.append(pltpu.make_async_copy(wo_hbm, wo, w_sem.at[1]))
    weights.append(pltpu.make_async_copy(sink_hbm, sink_ref, w_sem.at[2]))
    for copy in weights:
        copy.start()

    barrier = pltpu.get_barrier_semaphore()
    for peer in (partner, across, diag):
        pl.semaphore_signal(barrier, inc=1, device_id=(s, peer), device_id_type=MESH)
    for d in range(1, count):
        pl.semaphore_signal(
            barrier, inc=1, device_id=((s + d) % count, t), device_id_type=MESH
        )
    pl.semaphore_wait(barrier, 3 + count - 1)

    sources = (xg.at[t, 0], xg.at[t, 1])
    for copy in own:
        copy.wait()
    to_across = [
        remote(sources[a], xg.at[t, a], ag_send.at[0], ag_recv.at[0, a], s, across)
        for a in range(2)
    ]
    to_partner = [
        remote(sources[a], xg.at[t, a], ag_send.at[1], ag_recv.at[1, a], s, partner)
        for a in range(2)
    ]
    relay = [
        remote(xg.at[across, a], xg.at[across, a], ag_send.at[2], ag_recv.at[2, a], s, partner)
        for a in range(2)
    ]
    for copy in to_across + to_partner:
        copy.start()

    is_home = s // per_slot == t
    is_across = s // per_slot == across
    is_last = jnp.logical_not(is_home | is_across)

    half = count // 2
    here_half = s // half * half
    near = [here_half + i for i in range(half)]
    far = [half - here_half + i for i in range(half)]
    sends_near = s // half == t * per_slot // half

    def column_copy(kind, b):
        a, slot = kind % 2, t if kind else across
        return remote(
            xg.at[slot, a, :, pl.ds(b * block_cols, block_cols)], cols.at[a, s],
            col_send.at[kind, b], col_recv.at[a, s], slot * per_slot + b, t,
        )

    def column_arrival(a, source):
        ref = cols.at[a, source]
        return remote(ref, ref, col_send.at[a, 0], col_recv.at[a, source], (s + 1) % count, t)

    def y_copy(a, source):
        ref = cols.at[a, source]
        return remote(ref, ref, y_send.at[a], col_recv.at[a, source], s, across)

    def chip_copy(a, source):
        ref = cols.at[a, source]
        return remote(ref, ref, chip_send.at[0], col_recv.at[a, source], s, partner)

    def each_column(kind, act, which=None):
        slot = t if kind else across
        for b in range(per_slot) if which is None else which:
            sent = slot * per_slot + b != s

            @pl.when(sent if kind == 1 else sent & sends_near)
            def _():
                act(column_copy(kind, b))

    def send_columns(kind, which=None):
        each_column(kind, lambda copy: copy.start(), which)

    send_columns(1)
    send_columns(2)

    def project_input(slot, first=False):
        cells = xg[slot, 0]
        span = pl.ds(pl.multiple_of(slot * feats, feats), feats)
        term = dot_nn(cells, w_in[span, :])
        acc[:, :in_cols] = term if first else acc[:, :in_cols] + term

    def project_grad(slot, first=False):
        cells = xg[slot, 1]
        span = pl.ds(pl.multiple_of(slot * feats, feats), feats)
        term = contract_cols(cells, wo[:, span])
        acc[:, in_cols:] = term if first else acc[:, in_cols:] + term

    for edge in (0, WINDOW + count * rows):
        kvs[edge : edge + WINDOW] = jnp.zeros((WINDOW, 2 * k_cols), bf16)
    dkv[...] = jnp.zeros_like(dkv)
    sinks[...] = jnp.zeros_like(sinks)
    part_rows = rows // 2
    part_keys = part_rows + 2 * WINDOW
    tall = group * part_rows
    edges = -(-WINDOW // part_rows)
    parts = rows * count // part_rows
    q_at = lax.rem(lax.broadcasted_iota(jnp.int32, (tall, part_keys), 0), part_rows)
    k_at = lax.broadcasted_iota(jnp.int32, (tall, part_keys), 1)
    band = (k_at >= q_at) & (k_at - q_at <= 2 * WINDOW)
    starts = [edges] + list(range(edges)) + [parts - edges + i for i in range(edges)]
    for i, start in enumerate(starts):
        pos = k_at + (start * part_rows - WINDOW)
        inside = band & (pos >= 0) & (pos < rows * count) if i else band
        bias[i] = jnp.where(inside, 0.0, masked_score)

    pltpu.make_async_copy(w_in, w_in, w_sem.at[0]).wait()
    for copy in weights[3:]:
        copy.wait()
    project_input(t, True)
    project_grad(t, True)
    to_partner[0].wait_recv()
    project_input(partner)
    to_partner[1].wait_recv()
    project_grad(partner)
    to_across[0].wait_recv()
    relay[0].start()
    send_columns(0, (0,))
    project_input(across)
    relay[0].wait_recv()
    project_input(diag)
    for b in range(per_slot):
        span = slice(b * block_cols, (b + 1) * block_cols)

        @pl.when(t * per_slot + b == s)
        def _():
            for a in range(2):
                cols[a, s] = xg[t, a, :, span]


    def own_rows(block):
        return pl.ds(pl.multiple_of(WINDOW + block * rows, 32), rows)

    def item(i, block):
        return acts.at[i - 1, block] if i else kvs.at[own_rows(block)]

    def z_copy(i, block, way):
        dev = (z + 1 - 2 * way + depth) % depth * 2 + x
        ref = item(i, block)
        return remote(ref, ref, z_sem.at[way, block // 2], acts_recv.at[i, block], dev, t)

    def cross_copy(i, block):
        ref = item(i, block)
        return remote(
            ref, ref, cross_sem.at[block // 2], acts_recv.at[i, block], z * 2 + (1 - x), t
        )

    def goes_on(way):
        return jnp.where(way == 0, z < depth - 1, z > 0)

    def send_own(i):
        cross_copy(i, s).start()
        for way in range(2):

            @pl.when(goes_on(way))
            def _():
                z_copy(i, s, way).start()

    def level_at(d, way):
        level = z - d * (1 - 2 * way)
        return level, (level >= 0) & (level < depth)

    def crosses(i, level):
        return (i < 2) | ((level > 0) & (level < depth - 1)) | (level == z)

    def end_copy(way):
        block = (depth - 1) * way * 2 + (1 - x)
        dev = (z + 1 - 2 * way + depth) % depth * 2 + x
        ref = item(2, block)
        return remote(ref, ref, end_sem.at[way], acts_recv.at[2, block], dev, t)

    def forward_end(d, allowed=True):
        for way in range(2):
            level, there = level_at(d, way)
            there = there & allowed

            @pl.when(there & (level == (depth - 1) * way))
            def _():
                end_copy(way).wait_recv()

                @pl.when(goes_on(way))
                def _():
                    end_copy(way).start()

    def forward_way(i, d, way, allowed=True):
        level, there = level_at(d, way)

        @pl.when(there & allowed)
        def _():
            block = level * 2 + x
            z_copy(i, block, way).wait_recv()

            @pl.when(crosses(i, level))
            def _():
                cross_copy(i, block).start()

            @pl.when(goes_on(way))
            def _():
                z_copy(i, block, way).start()

    early, late = 1 - y, y

    def forward(i, d, allowed=True):
        forward_way(i, d, early, allowed)
        forward_way(i, d, late, allowed)

    kvs[own_rows(s)] = acc[:, q_cols:in_cols].astype(bf16)
    send_own(0)
    acts[0, s] = acc[:, :q_cols].astype(bf16)
    send_own(1)
    send_columns(0, (1,))

    to_across[1].wait_recv()
    relay[1].start()
    project_grad(across)
    relay[1].wait_recv()
    project_grad(diag)
    acts[1, s] = acc[:, in_cols:].astype(bf16)
    send_own(2)

    straight = [(source, a) for source in near for a in range(2)] + [(source, 1) for source in far]
    around = [(source, 0) for source in far]

    def pass_direct(here, items):
        @pl.when(here)
        def _():
            for source, a in items:

                @pl.when(source != s)
                def _():
                    column_arrival(a, source).wait_recv()

                y_copy(a, source).start()
                chip_copy(a, source).start()

    def pass_second(here, items):
        @pl.when(here)
        def _():
            for source, a in items:
                y_copy(a, source).wait_recv()
                chip_copy(a, source).start()

    def last_arrivals(sources):
        @pl.when(is_last)
        def _():
            for source in sources:
                for a in range(2):
                    chip_copy(a, source).wait_recv()

    def attend_block(block):
        jobs = [(half_at, kh) for half_at in range(2) for kh in range(key_heads)]
        each = range(len(jobs))
        head_at = lax.broadcasted_iota(jnp.int32, (tall, 1), 0) // part_rows

        def at(half_at):
            start = block * rows + half_at * part_rows
            return pl.ds(pl.multiple_of(start, 16), part_keys)

        def stacked(i, half_at, kh):
            span = slice(half_at * part_rows, (half_at + 1) * part_rows)
            heads = [kh * group + g for g in range(group)]
            return jnp.concatenate(
                [acts[i, block, span, h * HEAD : (h + 1) * HEAD] for h in heads], axis=0
            )

        def k_lanes(kh):
            return slice(kh * HEAD, (kh + 1) * HEAD)

        def v_lanes(kh):
            return slice(k_cols + kh * HEAD, k_cols + (kh + 1) * HEAD)

        which = []
        for half_at, _ in jobs:
            part_at = block * 2 + half_at
            late = part_at - (parts - edges)
            which.append(
                jnp.where(part_at < edges, 1 + part_at, jnp.where(late >= 0, 1 + edges + late, 0))
            )
        q = [stacked(0, *job) for job in jobs]
        do = [stacked(1, *job) for job in jobs]
        keys = [kvs[at(half_at), k_lanes(kh)] for half_at, kh in jobs]
        values = [kvs[at(half_at), v_lanes(kh)] for half_at, kh in jobs]
        scores = [contract_cols(q[i], keys[i]) for i in each]
        prob_grads = [contract_cols(do[i], values[i]) for i in each]
        scores = [scores[i] * (scaling * LOG2E) + bias[which[i]] for i in each]
        sink = []
        for _, kh in jobs:
            column = jnp.full((tall, 1), sink_ref[0, kh * group], f32)
            for g in range(1, group):
                column = jnp.where(head_at == g, sink_ref[0, kh * group + g], column)
            sink.append(column * LOG2E)
        top = [jnp.maximum(jnp.max(scores[i], axis=1, keepdims=True), sink[i]) for i in each]
        e = [jnp.exp2(scores[i] - top[i]) for i in each]
        sink_e = [jnp.exp2(sink[i] - top[i]) for i in each]
        inverse = [1.0 / (jnp.sum(e[i], axis=1, keepdims=True) + sink_e[i]) for i in each]
        p = [e[i] * inverse[i] for i in each]
        p_low = [p[i].astype(bf16) for i in each]
        attended = [dot_nn(p_low[i], values[i]).astype(bf16) for i in each]
        dots = [
            jnp.sum(do[i].astype(f32) * attended[i].astype(f32), axis=1, keepdims=True)
            for i in each
        ]
        dv = [contract_rows(p_low[i], do[i]) for i in each]
        ds = [(p[i] * (prob_grads[i] - dots[i])).astype(bf16) for i in each]
        dq = [(dot_nn(ds[i], keys[i]) * scaling).astype(bf16) for i in each]
        dk = [contract_rows(ds[i], q[i]) for i in each]
        lane_at = lax.broadcasted_iota(jnp.int32, (8, LANES), 1)
        sink_row = sinks[...]
        for i, (half_at, kh) in enumerate(jobs):
            span = slice(half_at * part_rows, (half_at + 1) * part_rows)
            sink_terms = sink_e[i] * inverse[i] * dots[i]
            for g in range(group):
                h = kh * group + g
                lanes, piece = slice(h * HEAD, (h + 1) * HEAD), slice(g * part_rows, (g + 1) * part_rows)
                att[block, span, lanes] = attended[i][piece]
                dqs[block, span, lanes] = dq[i][piece]
                total = jnp.sum(sink_terms[piece], axis=0, keepdims=True)
                sink_row = jnp.where(lane_at == h, sink_row - total, sink_row)
            dkv[at(half_at), k_lanes(kh)] += dk[i]
            dkv[at(half_at), v_lanes(kh)] += dv[i]
        sinks[...] = sink_row

    def cross_arrived(i, level):
        cross_copy(i, level * 2 + (1 - x)).wait_recv()

    def attend_own():
        for i in range(3):
            cross_arrived(i, z)
        for way in range(2):

            @pl.when(z == (depth - 1) * way)
            def _():
                end_copy(way).start()

        @pl.when((z == 0) | (z == depth - 1))
        def _():
            block = jnp.where(z == 0, 0, count - 1)
            attend_block(block)

    def attend(d, way, span=None):
        level, there = level_at(d, way)
        cross = level * 2 + (1 - x)
        extra = jnp.where(jnp.where(way == 0, level == 0, level == depth - 1), 1, 0)
        stop = 2 + extra
        nearest = jnp.where(way == 0, 2 * level + 2, 2 * level - 1)
        step = jnp.where(way == 0, -1, 1)
        inside = (x == way) | (extra == 1)
        key_at = jnp.where(x == way, 0, 1)

        def one(k, _):
            is_end = k == stop - 1
            block = nearest + step * k
            passed = jnp.where(way == 0, block <= cross, block >= cross)
            block = jnp.where(inside & passed, block + step, block)
            block = jnp.where(inside & is_end, cross, block)

            @pl.when(k == key_at)
            def _():
                cross_arrived(0, level)

            @pl.when(is_end)
            def _():
                cross_arrived(1, level)

            @pl.when(is_end & (extra == 0))
            def _():
                cross_arrived(2, level)

            attend_block(block)
            return 0

        begin, end = (0, stop) if span is None else span(stop)
        lax.fori_loop(begin, jnp.where(there, end, begin), one, 0)

    def attend_both(d, span=None):
        def one(way, _):
            attend(d, way, None if span is None else functools.partial(span, way))
            return 0

        lax.fori_loop(0, 2, one, 0)

    is_end = (z == 0) | (z == depth - 1)
    is_mid = jnp.logical_not(is_end)
    waits_late = is_mid & ((2 * z < depth) == (y == 1))
    waits_little = is_mid & jnp.logical_not(waits_late)
    pass_direct(is_home, straight)
    forward_way(0, 1, early)
    forward_way(1, 1, early)
    forward_way(0, 1, late)
    forward_way(2, 1, early, is_mid)
    forward_way(1, 1, late)
    attend_own()
    forward_way(2, 1, early, is_end)
    forward_way(2, 1, late)
    forward_end(1)
    pass_direct(is_across, around)
    attend(1, 1 - y, lambda stop: (0, jnp.where(waits_late, stop, 0)))
    forward(0, 2)
    forward(1, 2)
    attend(1, 1 - y, lambda stop: (jnp.where(waits_late, stop, 0), stop))
    forward(2, 2, waits_little)
    forward_end(2, waits_little)
    pass_second(is_across, straight)
    attend(1, y)
    own_dkv = dkv[own_rows(s)]
    own_grads = jnp.concatenate(
        [
            dqs[s],
            (own_dkv[:, :k_cols] * scaling).astype(bf16),
            own_dkv[:, k_cols:].astype(bf16),
        ],
        axis=1,
    )

    def partial_for(slot):
        span = pl.ds(pl.multiple_of(slot * feats, feats), feats)
        return contract_cols(own_grads, w_in[span, :])

    rs_copies = [
        remote(part.at[i], rs_in.at[i], rs_send.at[i], rs_recv.at[i], s, peer)
        for i, peer in enumerate((partner, partner, across))
    ]
    part[0] = partial_for(diag).astype(bf16)
    rs_copies[0].start()
    acc[:, :feats] = partial_for(across)
    forward(2, 2, jnp.logical_not(waits_little))
    forward_end(2, jnp.logical_not(waits_little))
    def weight_grads():
        last_arrivals(near)
        blocks = pl.ds(here_half, half)
        seq = pl.ds(pl.multiple_of(WINDOW + here_half * rows, WINDOW), half * rows)

        def flat(value):
            return value.reshape(half * rows, value.shape[-1])

        left = flat(cols[0, blocks])
        pieces = (
            (go_ref, contract_rows(flat(att[blocks]), flat(cols[1, blocks]))),
            (gq_ref, contract_rows(left, flat(dqs[blocks]))),
            (gk_ref, contract_rows(left, (dkv[seq, :k_cols] * scaling).astype(bf16))),
            (gv_ref, contract_rows(left, dkv[seq, k_cols:].astype(bf16))),
        )
        for ref, value in pieces:
            ref[...] = value

    for d in range(3, depth):
        forward(0, d)
    @pl.when(jnp.logical_not(is_end) & (core == 1))
    def _():
        weight_grads()

    rs_copies[0].wait_recv()
    part[2] = (acc[:, :feats] + rs_in[0].astype(f32)).astype(bf16)
    rs_copies[2].start()
    part[1] = partial_for(partner).astype(bf16)
    rs_copies[1].start()
    acc[:, :feats] = partial_for(t)

    @pl.when(jnp.logical_not(is_end) & (core == 0))
    def _():
        weight_grads()

    for d in range(3, depth):
        forward(1, d)
    attend_both(2)
    pass_second(is_home, around)
    @pl.when(is_end)
    def _():
        weight_grads()

    for d in range(3, depth):
        attend_both(d, lambda way, stop: (0, 1))
    for d in range(3, depth):
        forward(2, d)
        attend_both(d, lambda way, stop: (1, stop - 1))
    last_arrivals(far)
    far_cols[...] = cols[:, pl.ds(half - here_half, half)]
    for d in range(3, depth):
        forward_end(d)
        attend_both(d, lambda way, stop: (stop - 1, stop))
    sg_ref[...] = sinks[...]
    for copy in rs_copies[1:]:
        copy.wait_recv()
    ig_ref[...] = (
        acc[:, :feats] + rs_in[1].astype(f32) + rs_in[2].astype(f32)
    ).astype(bf16)

    def sent(ref, sem):
        remote(ref, ref, sem, rs_recv.at[0], (s + 1) % count, t).wait_send()

    for i in range(3):
        sent(xg.at[t], ag_send.at[i])
    for copy in rs_copies:
        copy.wait_send()
    for kind in range(3):
        each_column(kind, lambda copy: copy.wait_send())

    @pl.when(is_home)
    def _():
        sent(cols.at[0, pl.ds(here_half, half)], y_send.at[0])
        sent(cols.at[1], y_send.at[1])

    @pl.when(is_across)
    def _():
        sent(cols.at[0, pl.ds(half - here_half, half)], y_send.at[0])

    @pl.when(jnp.logical_not(is_last))
    def _():
        sent(cols, chip_send.at[0])

    for level in range(depth):
        for way in range(2):
            came = jnp.where(way == 0, level <= z, level >= z)

            @pl.when(came & goes_on(way))
            def _():
                sent(acts.at[0, pl.ds(0, 3)], z_sem.at[way, level])

        all_cross = crosses(2, level)

        @pl.when(all_cross)
        def _():
            sent(acts.at[0, pl.ds(0, 3)], cross_sem.at[level])

        @pl.when(jnp.logical_not(all_cross))
        def _():
            sent(acts.at[0, pl.ds(0, 2)], cross_sem.at[level])

    for way in range(2):

        @pl.when(goes_on(way))
        def _():
            end_copy(way).wait_send()


def store_kernel(
    ig_in, gq_in, gk_in, gv_in, go_in, sink_in, att, dqs, dkv, far_cols,
    ig_out, gq_out, gk_out, gv_out, go_out, sink_out, gq, gk, gv, go, sem,
):
    bf16 = jnp.bfloat16
    count = lax.axis_size("sp")
    half = count // 2
    begin = half - lax.axis_index("sp") // half * half
    rows = att.shape[1]
    k_cols = gk.shape[1]
    blocks = pl.ds(begin, half)
    seq = pl.ds(pl.multiple_of(WINDOW + begin * rows, WINDOW), half * rows)

    def flat(value):
        return value.reshape(half * rows, value.shape[-1])

    def send(i, held, out):
        copy = pltpu.make_async_copy(held, out, sem.at[i])
        copy.start()
        return copy

    copies = [send(0, ig_in, ig_out)]
    sink_out[...] = sink_in[0:1, : sink_out.shape[1]]
    left = flat(far_cols[0])
    go[...] = go_in[...] + contract_rows(flat(att[blocks]), flat(far_cols[1]))
    copies.append(send(1, go, go_out))
    gq[...] = gq_in[...] + contract_rows(left, flat(dqs[blocks]))
    copies.append(send(2, gq, gq_out))
    gk[...] = gk_in[...] + contract_rows(left, (dkv[seq, :k_cols] * HEAD**-0.5).astype(bf16))
    copies.append(send(3, gk, gk_out))
    gv[...] = gv_in[...] + contract_rows(left, dkv[seq, k_cols:].astype(bf16))
    copies.append(send(4, gv, gv_out))
    for copy in copies:
        copy.wait()


def fused_device(
    layer_input, output_grad, query_weight, key_weight, value_weight, out_weight, sink_logit
):
    bf16, f32 = jnp.bfloat16, jnp.float32
    count, tps = lax.axis_size("sp"), lax.axis_size("tp")
    rows, feats = layer_input.shape
    width = query_weight.shape[0]
    q_cols, k_cols = query_weight.shape[1], key_weight.shape[1]
    block_cols = width // count
    vmem = pl.BlockSpec(memory_space=pltpu.VMEM)
    hbm = pl.BlockSpec(memory_space=pltpu.HBM)
    dma = pltpu.SemaphoreType.DMA
    outs = pl.pallas_call(
        layer_kernel,
        out_shape=(
            jax.ShapeDtypeStruct((rows, feats), bf16),
            jax.ShapeDtypeStruct((block_cols, q_cols), f32),
            jax.ShapeDtypeStruct((block_cols, k_cols), f32),
            jax.ShapeDtypeStruct((block_cols, k_cols), f32),
            jax.ShapeDtypeStruct((q_cols, block_cols), f32),
            jax.ShapeDtypeStruct((8, LANES), f32),
            jax.ShapeDtypeStruct((count, rows, q_cols), bf16),
            jax.ShapeDtypeStruct((count, rows, q_cols), bf16),
            jax.ShapeDtypeStruct((count * rows + 2 * WINDOW, 2 * k_cols), f32),
            jax.ShapeDtypeStruct((2, count // 2, rows, block_cols), bf16),
        ),
        in_specs=[hbm] * 7,
        out_specs=(vmem,) * 10,
        scratch_shapes=[
            pltpu.VMEM((width, q_cols + 2 * k_cols), bf16),
            pltpu.VMEM(out_weight.shape, bf16),
            pltpu.VMEM((tps, 2, rows, feats), bf16),
            pltpu.VMEM((rows, 2 * q_cols + 2 * k_cols), f32),
            pltpu.VMEM((count * rows + 2 * WINDOW, 2 * k_cols), bf16),
            pltpu.VMEM((2, count, rows, q_cols), bf16),
            pltpu.VMEM((2, count, rows, block_cols), bf16),
            pltpu.VMEM((1 + 2 * (-(-2 * WINDOW // rows)), q_cols // k_cols * rows // 2, rows // 2 + 2 * WINDOW), f32),
            pltpu.VMEM((8, LANES), f32),
            pltpu.VMEM((3, rows, feats), bf16),
            pltpu.VMEM((3, rows, feats), bf16),
            pltpu.SMEM((1, sink_logit.shape[0]), f32),
            dma((5,)), dma((3,)), dma((3, 2)),
            dma((3, feats // block_cols)), dma((2, count)), dma((2,)), dma((1,)),
            dma((2, count // 2)), dma((count // 2,)), dma((2,)), dma((3, count)), dma((3,)), dma((3,)),
        ],
        compiler_params=pltpu.CompilerParams(
            collective_id=0, has_side_effects=True, vmem_limit_bytes=VMEM_BYTES
        ),
        name="layer",
    )(
        *(
            pltpu.with_memory_space_constraint(array, pltpu.HBM)
            for array in (
                layer_input, output_grad, query_weight, key_weight, value_weight, out_weight,
                sink_logit.reshape(1, -1),
            )
        ),
    )
    kept = [jax.ShapeDtypeStruct(out.shape, out.dtype) for out in outs[:5]]
    stored = pl.pallas_call(
        store_kernel,
        out_shape=(*kept, jax.ShapeDtypeStruct((1, sink_logit.shape[0]), f32)),
        in_specs=[vmem] * 10,
        out_specs=(hbm,) * 5 + (vmem,),
        scratch_shapes=[pltpu.VMEM(out.shape, f32) for out in outs[1:5]] + [dma((5,))],
        compiler_params=pltpu.CompilerParams(vmem_limit_bytes=STORE_BYTES),
        name="store",
    )(*outs)
    return tuple(stored[:5]) + (stored[5].reshape(-1),)


def fits_kernel(mesh, layer_width):
    count, tps = mesh.shape["sp"], mesh.shape["tp"]
    return tps == 4 and count == 8 and layer_width == count * tps * LANES and HEADS == 2 * KV_HEADS


def solution(mesh):
    placed = (
        P("sp", "tp"),
        P("sp", "tp"),
        P(None, "tp"),
        P(None, "tp"),
        P(None, "tp"),
        P("tp", None),
        P("tp"),
    )

    def sharded(*arrays):
        width = arrays[0].shape[1]
        body = fused_device if fits_kernel(mesh, width) else per_device
        return jax.shard_map(
            body,
            mesh=mesh,
            in_specs=placed,
            out_specs=(
                P("sp", "tp"),
                P("sp", "tp"),
                P("sp", "tp"),
                P("sp", "tp"),
                P("tp", "sp"),
                P("tp"),
            ),
            check_vma=False,
        )(*arrays)

    return sharded
```
